128 devices in a mesh: tp: 16 (over z, y), dp: 8 (over x, core).
Axes of the slice: x: 4, y: 4, z: 4, core: 2. Of those that a mesh axis runs over, the one named last changes fastest.
Arguments:
- tokens: bfloat16 [256, 4096], P('dp', 'tp'), may hold values from -6 to 6
- lengths: int32 [256], P('dp'), may hold values from 1 to 96, 6144 in all
- norm_gain: float32 [2, 4096], replicated, may hold values from 0.1 to 1.9
- w_recept: bfloat16 [2, 4096, 4096], P(None, None, ('tp', 'dp')), may hold values from -0.09375 to 0.09375
- w_key: bfloat16 [2, 4096, 4096], P(None, None, ('tp', 'dp')), may hold values from -0.09375 to 0.09375
- w_value: bfloat16 [2, 4096, 4096], P(None, None, ('tp', 'dp')), may hold values from -0.09375 to 0.09375
- w_decay: bfloat16 [2, 4096, 4096], P(None, None, ('tp', 'dp')), may hold values from -0.09375 to 0.09375
- w_rate: bfloat16 [2, 4096, 4096], P(None, None, ('tp', 'dp')), may hold values from -0.09375 to 0.09375
- w_gate: bfloat16 [2, 4096, 4096], P(None, None, ('tp', 'dp')), may hold values from -0.09375 to 0.09375
- w_out: bfloat16 [2, 4096, 4096], P(None, None, ('tp', 'dp')), may hold values from -0.09375 to 0.09375
- decay_base: float32 [2, 4096], P(None, 'tp'), may hold values from -3 to 1
- rate_base: float32 [2, 4096], P(None, 'tp'), may hold values from -3 to 3
- group_gain: float32 [2, 4096], P(None, 'tp'), may hold values from 0.1 to 1.9
- state: float32 [2, 256, 64, 64, 64], P(None, 'dp', 'tp'), may hold values from -6 to 6
Outputs:
- mixed: bfloat16 [256, 4096], P('dp', 'tp')
- new_state: float32 [2, 256, 64, 64, 64], P(None, 'dp', 'tp')
The draws below stay inside these ranges and needn't reach their ends.
Inputs may be any that keep to these rules, and one draw needn't show every extreme that they name: Each sequence's live length lies between 1 and 96, some sequences reach 96, and the lengths sum to 6144.
All inputs are finite; a program needn't handle non-finite values.
Results may differ from the reference program's by a relative error of at most 0.025.
Values may be sent and summed in bfloat16 or wider, within the bound.
A program may use at most 128 MiB of HBM per device.

```python
import math
import jax
import jax.numpy as jnp
import numpy as np
from jax import lax

D = 4096
HEAD = 64
STEP = 16
BATCH = 256


def steps_of(key, extent, cuts, least, high):
    gain, own = 1.0, jax.random.fold_in(key, 6)
    for dim, blocks in cuts:
        heights = jnp.exp(jax.random.uniform(jax.random.fold_in(own, dim), (blocks,), jnp.float32, least / len(cuts), high / len(cuts)))
        gain = gain * jnp.repeat(heights, extent[dim] // blocks).reshape([-1 if axis == dim else 1 for axis in range(len(extent))])
    return gain


def profile(amount, total, reach, slope):
    loads = [(1 << 20) // math.isqrt(grade ** slope) + 1 for grade in range(2, amount + 1)]
    surplus, given = total - reach - (amount - 1), [1] * (amount - 1)
    while surplus > 0:
        candidates = [i for i in range(amount - 1) if given[i] < reach]
        pool, left = sum([loads[i] for i in candidates]), surplus
        for i in candidates:
            addition = min(reach - given[i], max(1, left * loads[i] // pool), surplus)
            given[i] = given[i] + addition
            surplus = surplus - addition
    return np.array([reach] + given)


def uneven_parts(key, amount, total, limit, slope):
    if amount == 2:
        one = jax.random.randint(key, (), max(1, total - limit), min(limit, total - 1) + 1)
        return jnp.stack([one, total - one])
    sizes = jnp.asarray(profile(amount, total, limit, slope), jnp.int32)
    couples = (amount - 1) // 2
    donor, receiver = sizes[1:1 + 2 * couples:2], sizes[2:2 + 2 * couples:2]
    room = jnp.minimum(donor - 1, limit - receiver)
    moved = jax.random.randint(jax.random.fold_in(key, 1), (couples,), 0, 1 << 20) % (room + 1)
    sizes = sizes.at[1:1 + 2 * couples:2].set(donor - moved).at[2:2 + 2 * couples:2].set(receiver + moved)
    return sizes[jax.random.permutation(jax.random.fold_in(key, 2), amount)]


def scatter_about(rng, dims, width, reach, pieces=(), dtype=jnp.bfloat16):
    level = steps_of(rng, dims, pieces, -0.22, 0.18) if pieces else 1.0
    values = jax.random.normal(rng, dims, jnp.float32) * width * level
    return jnp.minimum(jnp.maximum(values, -reach), reach).astype(dtype)


def setup_inputs(seed: int = 0) -> dict:
    splits = jax.random.split(jax.random.key(seed), 15)
    tokens = scatter_about(splits[0], (BATCH, D), 1.0, 6.0, ((0, 8), (1, 16)))
    lengths = uneven_parts(splits[1], BATCH, 24 * BATCH, 96, 2).astype(jnp.int32)
    norm_gain = jnp.clip(1.0 + 0.18 * jax.random.normal(splits[2], (2, D), jnp.float32), 0.1, 1.9)
    w_recept = scatter_about(splits[3], (2, D, D), D ** -0.5, 0.09375, ((2, 128),))
    w_key = scatter_about(splits[4], (2, D, D), D ** -0.5, 0.09375, ((2, 128),))
    w_value = scatter_about(splits[5], (2, D, D), D ** -0.5, 0.09375, ((2, 128),))
    w_decay = scatter_about(splits[6], (2, D, D), D ** -0.5, 0.09375, ((2, 128),))
    w_rate = scatter_about(splits[7], (2, D, D), D ** -0.5, 0.09375, ((2, 128),))
    w_gate = scatter_about(splits[8], (2, D, D), D ** -0.5, 0.09375, ((2, 128),))
    w_out = scatter_about(splits[9], (2, D, D), D ** -0.5, 0.09375, ((2, 128),))
    decay_base = jnp.clip(-3.0 + 4.0 * jax.random.uniform(splits[10], (2, D), jnp.float32) ** steps_of(splits[10], (2, D), ((1, 16),), -0.2, 0.2), -3.0, 1.0)
    rate_base = scatter_about(splits[11], (2, D), 0.5, 3.0, ((1, 16),), jnp.float32)
    group_gain = jnp.clip(1.0 + 0.18 * jax.random.normal(splits[12], (2, D), jnp.float32), 0.1, 1.9)
    state = scatter_about(splits[13], (2, BATCH, D // HEAD, HEAD, HEAD), 1.0, 6.0, ((1, 8), (2, 16)), jnp.float32)
    return dict(tokens=tokens, lengths=lengths, norm_gain=norm_gain, w_recept=w_recept, w_key=w_key, w_value=w_value, w_decay=w_decay, w_rate=w_rate, w_gate=w_gate, w_out=w_out, decay_base=decay_base, rate_base=rate_base, group_gain=group_gain, state=state)


RMS_EPS = 1e-06
GROUP_EPS = 0.00064

def stored(matrix, weight):
    product = jnp.dot(matrix, weight, preferred_element_type=jnp.float32)
    return lax.optimization_barrier(product.astype(jnp.bfloat16)).astype(jnp.float32)

def recur(state_old, recept, key_vec, value_vec, decay_rate, learn_rate, active, head_size):
    split = (recept.shape[0], -1, head_size)
    recept_h = recept.reshape(split)
    key_h = key_vec.reshape(split)
    value_h = value_vec.reshape(split)
    decay_h = decay_rate.reshape(split)
    rate_h = learn_rate.reshape(split)
    key_len = jnp.sqrt(lax.optimization_barrier(jnp.sum(key_h * key_h, axis=-1, keepdims=True)))
    key_unit = key_h / jnp.maximum(key_len, 1e-12)
    state_a = jnp.einsum('bhij,bhj->bhi', state_old, -key_unit, precision=lax.Precision.HIGHEST)
    updated = state_old * decay_h[:, :, None, :] + state_a[:, :, :, None] * (key_unit * rate_h)[:, :, None, :] + value_h[:, :, :, None] * (key_h * rate_h)[:, :, None, :]
    updated = jnp.where(active[:, None, None, None], updated, state_old)
    readout = jnp.einsum('bhij,bhj->bhi', updated, recept_h, precision=lax.Precision.HIGHEST)
    centre = lax.optimization_barrier(jnp.mean(readout, axis=-1, keepdims=True))
    spread = lax.optimization_barrier(jnp.mean(jnp.square(readout - centre), axis=-1, keepdims=True))
    normal_out = ((readout - centre) * lax.rsqrt(spread + GROUP_EPS)).reshape(recept.shape[0], -1)
    return (updated, normal_out)

def reference(tokens, lengths, norm_gain, w_recept, w_key, w_value, w_decay, w_rate, w_gate, w_out, decay_base, rate_base, group_gain, state):
    active = lengths > STEP
    current = tokens
    updated_states = []
    for layer_idx in range(2):
        values = current.astype(jnp.float32)
        factor = lax.rsqrt(lax.optimization_barrier(jnp.mean(values * values, axis=1, keepdims=True)) + RMS_EPS)
        normed = (values * factor * norm_gain[layer_idx]).astype(jnp.bfloat16)
        recept = stored(normed, w_recept[layer_idx])
        key_vec = stored(normed, w_key[layer_idx])
        value_vec = stored(normed, w_value[layer_idx])
        decay_pre = stored(normed, w_decay[layer_idx])
        rate_pre = stored(normed, w_rate[layer_idx])
        gate_pre = stored(normed, w_gate[layer_idx])
        decay_rate = jnp.exp(-jnp.exp(-jax.nn.softplus(-(decay_base[layer_idx] + decay_pre)) - 0.5))
        learn_rate = jax.nn.sigmoid(rate_base[layer_idx] + rate_pre)
        gate_open = jax.nn.sigmoid(gate_pre)
        updated, normal_out = recur(state[layer_idx], recept, key_vec, value_vec, decay_rate, learn_rate, active, HEAD)
        updated_states.append(updated)
        mixed_rows = jnp.where(active[:, None], normal_out * group_gain[layer_idx] * gate_open, 0.0).astype(jnp.bfloat16)
        current = jnp.dot(mixed_rows, w_out[layer_idx], preferred_element_type=jnp.float32).astype(jnp.bfloat16)
    return (current, jnp.stack(updated_states))
```

```python
import functools

import jax
import jax.numpy as jnp
from jax import lax
from jax.experimental import pallas as pl
from jax.experimental.pallas import tpu as pltpu
from jax.sharding import PartitionSpec as P

STEP = 16
RMS_EPS = 1e-06
GROUP_EPS = 0.00064
VMEM_LIMIT = 56 * 1024 * 1024
MESH = pl.DeviceIdType.MESH


def dot_t(a, b):
    return lax.dot_general(a, b, (((1,), (1,)), ((), ())), preferred_element_type=jnp.float32)


def plane_offsets(tp):
    ny = 4 if tp == 16 else tp
    nz = tp // ny
    hops = lambda k, n: min(k, n - k)
    offs = [(dz, dy) for dz in range(nz) for dy in range(ny)]
    offs.sort(key=lambda o: (hops(o[0], nz) + hops(o[1], ny), o))
    return ny, nz, offs


def step_body(
    tok, lens, gain, base, rate, ggain, wr, wk, wv, wd, wa, wg, wo, state,
    mixed_ref, rows_ref,
    xg, wcat, wot, vg, mg, pieces, st, acc, square,
    ag_send, a1_recv, b1_recv, fin_recv, ex_send, ex_recv, mg_send, mg_recv,
    wo_send, wo_recv, wc_send, wc_recv, own_sem, st_sem,
    *, tp, dp,
):
    t, d = lax.axis_index("tp"), lax.axis_index("dp")
    nx = dp // 2
    x, core = d // 2, lax.rem(d, 2)
    sibling = d + 1 - 2 * core
    ny, nz, offs = plane_offsets(tp)
    z, y = t // ny, lax.rem(t, ny)
    rows, width = tok.shape
    slim = width // dp
    feat = tp * width
    half = rows // 2
    weights = (wr, wk, wv, wd, wa, wg)

    def plane(off):
        return lax.rem(z + off[0], nz) * ny + lax.rem(y + off[1], ny)

    def xpeer(k):
        return lax.rem(x + k + nx, nx)

    def remote(src, dst, ssem, rsem, tt, dd):
        return pltpu.make_async_remote_copy(
            src_ref=src, dst_ref=dst, send_sem=ssem, recv_sem=rsem,
            device_id=(tt, dd), device_id_type=MESH,
        )

    def arrived(ref, sem):
        remote(ref, ref, ag_send.at[0], sem, t, sibling).wait_recv()

    peers = [plane(o) for o in offs[1:]]
    far = peers[::-1]
    ks = [1, nx - 1] + list(range(2, nx - 1))
    xs = [xpeer(k) for k in ks]

    local = []

    def fetch(src, dst, sem):
        copy = pltpu.make_async_copy(src, dst, sem)
        copy.start()
        return copy

    def wrow(q):
        return pl.ds(pl.multiple_of(q * 2 * slim + core * slim, slim), slim)

    def worow(dd, start=0, count=None):
        return pl.ds(pl.multiple_of(dd * slim + start, slim // 2), slim if count is None else count)

    own_w = [[fetch(weights[q].at[l], wcat.at[l, wrow(q)], own_sem.at[l, q]) for q in range(6)] for l in range(2)]
    own_o = [fetch(wo.at[l], wot.at[l, worow(d)], own_sem.at[l, 6]) for l in range(2)]
    own_s = [fetch(state.at[l], st.at[l], st_sem.at[l]) for l in range(2)]

    barrier = pltpu.get_barrier_semaphore()
    everyone = [(p, d) for p in far] + [(t, 2 * o + core) for o in xs] + [(t, sibling)]
    for p in everyone:
        pl.semaphore_signal(barrier, inc=1, device_id=p, device_id_type=MESH)
    pl.semaphore_wait(barrier, len(everyone))

    def own_rows(h, xx):
        return pl.ds(pl.multiple_of(xx * rows + h * half, half), half)

    def gather_start(l, source):
        sent = []

        def send(src, dst, rsem, tt, dd):
            copy = remote(src, dst, ag_send.at[len(sent)], rsem, tt, dd)
            copy.start()
            sent.append(copy)

        a_dst, b_dst = xg.at[l, t, own_rows(0, x)], xg.at[l, t, own_rows(1, x)]
        for o in xs:
            send(source(0), a_dst, a1_recv.at[l, x], t, 2 * o + core)
        for p in far:
            send(source(1), b_dst, b1_recv.at[l, t], p, d)
        for p in far:
            send(source(0), a_dst, fin_recv.at[l, t], p, d)
        for o in xs:
            send(source(1), b_dst, fin_recv.at[l, t], t, 2 * o + core)
        return sent, send

    def gather_relay(l, send):
        for o in xs:
            block = xg.at[l, t, own_rows(0, o)]
            arrived(block, a1_recv.at[l, o])
            for p in far:
                send(block, block, fin_recv.at[l, t], p, d)
        for p in peers:
            block = xg.at[l, p, own_rows(1, x)]
            arrived(block, b1_recv.at[l, p])
            for o in xs:
                send(block, block, fin_recv.at[l, p], t, 2 * o + core)

    def prepare(l):
        for q in range(6):
            own_w[l][q].wait()
        for q in range(6):
            other = pl.ds(pl.multiple_of(q * 2 * slim + (1 - core) * slim, slim), slim)
            arrived(wcat.at[l, other], wc_recv.at[l, q])
        line = gain[l : l + 1, :]

        def one(i, carry):
            part = pl.ds(pl.multiple_of(i * 16, 16), 16)
            wcat[l, part, :] = (wcat[l, part, :].astype(jnp.float32) * line).astype(jnp.bfloat16)
            return carry

        lax.fori_loop(0, 12 * slim // 16, one, 0)

    def project(l):
        acc[...] = jnp.zeros_like(acc)
        square[...] = jnp.zeros_like(square)
        for o in offs:
            tt = plane(o)
            count = (nx - 1) * half if o == (0, 0) else (2 * nx - 1) * half
            arrived(xg.at[l, tt, pl.ds(0, count)], fin_recv.at[l, tt])
            block = xg[l, tt]
            cols = pl.ds(pl.multiple_of(tt * width, width), width)
            acc[...] += dot_t(block, wcat[l, :, cols])
            values = block.astype(jnp.float32)
            values = values * values
            total = values[:, :128]
            for j in range(1, width // 128):
                total += values[:, j * 128 : (j + 1) * 128]
            square[...] += total
        factor = lax.rsqrt(jnp.sum(square[...], axis=1, keepdims=True) / feat + RMS_EPS)
        done = (acc[...] * factor).astype(jnp.bfloat16)
        for j in range(nx):
            pieces[l, j] = done[j * rows : (j + 1) * rows]
        sent = []
        for i, o in enumerate(xs):
            copy = remote(pieces.at[l, o], vg.at[l, x], ex_send.at[l, i], ex_recv.at[l, x], t, 2 * o + core)
            copy.start()
            sent.append(copy)
        vg[l, x] = pieces[l, x]
        return sent

    def out_slot(l, xx, cc, start=0, count=None):
        return wot.at[l, worow(2 * xx + cc, start, count)]

    def out_start(l):
        own_o[l].wait()
        up, down = xpeer(1), xpeer(-1)
        block = out_slot(l, x, core)
        sent = [
            remote(block, block, wo_send.at[l, 0], wo_recv.at[l, 0], t, 2 * up + core),
            remote(block, block, wo_send.at[l, 1], wo_recv.at[l, 1], t, 2 * down + core),
            remote(block, block, wo_send.at[l, 2], wo_recv.at[l, 4], t, sibling),
        ]
        for copy in sent:
            copy.start()
        return sent

    def out_relay(l, sent):
        up, down, across = xpeer(1), xpeer(-1), xpeer(2)
        part = slim // 2
        below, above = out_slot(l, down, core), out_slot(l, up, core)
        arrived(below, wo_recv.at[l, 0])
        first = out_slot(l, down, core, 0, part)
        one = remote(first, first, wo_send.at[l, 3], wo_recv.at[l, 2], t, 2 * up + core)
        one.start()
        two = remote(below, below, wo_send.at[l, 4], wo_recv.at[l, 5], t, sibling)
        two.start()
        arrived(above, wo_recv.at[l, 1])
        second = out_slot(l, up, core, part, part)
        three = remote(second, second, wo_send.at[l, 5], wo_recv.at[l, 3], t, 2 * down + core)
        three.start()
        four = remote(above, above, wo_send.at[l, 6], wo_recv.at[l, 6], t, sibling)
        four.start()
        sent += [one, two, three, four]

    def out_finish(l, sent):
        up, down, across = xpeer(1), xpeer(-1), xpeer(2)
        part = slim // 2
        arrived(out_slot(l, across, core, 0, part), wo_recv.at[l, 2])
        arrived(out_slot(l, across, core, part, part), wo_recv.at[l, 3])
        block = out_slot(l, across, core)
        copy = remote(block, block, wo_send.at[l, 7], wo_recv.at[l, 7], t, sibling)
        copy.start()
        sent.append(copy)
        for i, xx in enumerate((x, down, up, across)):
            arrived(out_slot(l, xx, 1 - core), wo_recv.at[l, 4 + i])

    size = 2 * slim
    sub = lax.broadcasted_iota(jnp.int32, (rows, rows), 0)
    lane = lax.broadcasted_iota(jnp.int32, (rows, rows), 1)
    spread = jnp.where(sub == lane, lens[...].astype(jnp.float32), 0.0)
    live = jnp.sum(spread, axis=1, keepdims=True) > STEP
    eight = lax.broadcasted_iota(jnp.int32, (8, size), 0)

    def recur(l):
        for o in xs:
            arrived(vg.at[l, o], ex_recv.at[l, o])
        own_s[l].wait()
        looks, extras, gates = [], [], []
        for h in range(nx):
            part = slice(h * size, (h + 1) * size)
            recept, key, value, decay_pre, rate_pre, gate_pre = [
                vg[l, h, :, q * size : (q + 1) * size].astype(jnp.float32) for q in range(6)
            ]
            decay = jnp.exp(-jnp.exp(-jax.nn.softplus(-(base[l : l + 1, part] + decay_pre)) - 0.5))
            learn = jax.nn.sigmoid(rate[l : l + 1, part] + rate_pre)
            length = jnp.maximum(jnp.sqrt(jnp.sum(key * key, axis=1, keepdims=True)), 1e-12)
            unit = key / length
            rated = unit * learn
            held = value * length
            rho = jnp.sum(rated * recept, axis=1, keepdims=True)
            rows_ref[l, 0, h] = jnp.where(live, -unit, 0.0)
            rows_ref[l, 1, h] = jnp.where(live, held, 0.0)
            rows_ref[l, 2, h] = jnp.where(live, decay, 1.0)
            rows_ref[l, 3, h] = rated
            looks.append(decay * recept - rho * unit)
            extras.append(rho * held)
            gates.append(jax.nn.sigmoid(gate_pre) * ggain[l : l + 1, part])
        sent = []
        for g in range(2):
            outs = []
            for h in range(nx):
                reads = []
                for k in range(half // 8):
                    low = g * half + k * 8
                    look = looks[h][low : low + 8]
                    read = extras[h][low : low + 8]
                    for b in range(8):
                        got = dot_t(look, st[l, low + b, h])
                        read += jnp.where(eight == b, got, 0.0)
                    reads.append(read)
                read = jnp.concatenate(reads, axis=0)
                span = slice(g * half, (g + 1) * half)
                centre = jnp.mean(read, axis=1, keepdims=True)
                apart = read - centre
                var = jnp.mean(apart * apart, axis=1, keepdims=True)
                normal = apart * lax.rsqrt(var + GROUP_EPS) * gates[h][span]
                outs.append(jnp.where(live[span], normal, 0.0).astype(jnp.bfloat16))
            span = pl.ds(g * half, half)
            mg[l, t, span, :] = jnp.concatenate(outs, axis=1)
            block = mg.at[l, t, span]
            for i, p in enumerate(far):
                copy = remote(block, block, mg_send.at[l, g * (tp - 1) + i], mg_recv.at[l, t], p, d)
                copy.start()
                sent.append(copy)
        return sent

    def fold(l):
        total = jnp.zeros((rows, width), jnp.float32)
        for o in offs:
            tt = plane(o)
            if o != (0, 0):
                arrived(mg.at[l, tt], mg_recv.at[l, tt])
            cols = pl.ds(pl.multiple_of(tt * width, width), width)
            total += dot_t(mg[l, tt], wot[l, :, cols])
        return total.astype(jnp.bfloat16)

    mine = pl.ds(pl.multiple_of(x * rows, rows), rows)
    for l in range(2):
        if l == 0:
            sent, send = gather_start(0, lambda h: tok.at[pl.ds(h * half, half)])
            xg[0, t, mine, :] = tok[...]
            shared = []
            for ll in range(2):
                for q in range(6):
                    copy = remote(
                        weights[q].at[ll], wcat.at[ll, wrow(q)],
                        wc_send.at[ll, q], wc_recv.at[ll, q], t, sibling,
                    )
                    copy.start()
                    shared.append(copy)
        else:
            xg[1, t, mine, :] = current
            sent, send = gather_start(1, lambda h: xg.at[1, t, own_rows(h, x)])
        gather_relay(l, send)
        if l == 0:
            prepare(0)
        traded = project(l)
        folded = out_start(l)
        for copy in sent:
            copy.wait_send()
        mixed = recur(l)
        out_relay(l, folded)
        if l == 0:
            prepare(1)
        out_finish(l, folded)
        current = fold(l)
        for copy in traded + folded + mixed:
            copy.wait_send()
    mixed_ref[...] = current
    for copy in shared:
        copy.wait_send()


def step(tok, lens, gain, base, rate, ggain, weights, wo, state, tp, dp):
    rows, width = tok.shape
    slim = width // dp
    nx = dp // 2
    feat = tp * width
    bf = jnp.bfloat16
    vmem, any_ = pl.BlockSpec(memory_space=pltpu.VMEM), pl.BlockSpec(memory_space=pl.ANY)
    dma = pltpu.SemaphoreType.DMA
    half = rows // 2
    return pl.pallas_call(
        functools.partial(step_body, tp=tp, dp=dp),
        out_shape=(
            jax.ShapeDtypeStruct((rows, width), bf),
            jax.ShapeDtypeStruct((2, 4, nx, rows, 2 * slim), jnp.float32),
        ),
        in_specs=[vmem] * 6 + [any_] * 8,
        out_specs=(vmem, vmem),
        scratch_shapes=[
            pltpu.VMEM((2, tp, nx * rows, width), bf),
            pltpu.VMEM((2, 12 * slim, feat), bf),
            pltpu.VMEM((2, width, feat), bf),
            pltpu.VMEM((2, nx, rows, 12 * slim), bf),
            pltpu.VMEM((2, tp, rows, width), bf),
            pltpu.VMEM((2, nx, rows, 12 * slim), bf),
            pltpu.VMEM(state.shape, state.dtype),
            pltpu.VMEM((nx * rows, 12 * slim), jnp.float32),
            pltpu.VMEM((nx * rows, 128), jnp.float32),
            dma(((nx - 1) * (tp + 1) + (tp - 1) * (nx + 1),)),
            dma((2, nx)),
            dma((2, tp)),
            dma((2, tp)),
            dma((2, nx)),
            dma((2, nx)),
            dma((2, 2 * tp)),
            dma((2, tp)),
            dma((2, 8)),
            dma((2, 8)),
            dma((2, 6)),
            dma((2, 6)),
            dma((2, 7)),
            dma((2,)),
        ],
        compiler_params=pltpu.CompilerParams(
            collective_id=0, has_side_effects=True, vmem_limit_bytes=VMEM_LIMIT
        ),
        name="step",
    )(tok, lens, gain, base, rate, ggain, *weights, wo, state)


def renew_body(rows_ref, mixed_ref, state_ref, new_ref, out_ref):
    group, heads, size = state_ref.shape[1:4]
    across = lax.broadcasted_iota(jnp.int32, (size, size), 0)
    along = lax.broadcasted_iota(jnp.int32, (size, size), 1)
    eye = across == along

    @pl.when((pl.program_id(0) == 0) & (pl.program_id(1) == 0))
    def _():
        out_ref[...] = mixed_ref[...]

    for b in range(group):
        for h in range(heads):
            neg, held, decay, rated = [rows_ref[0, q, h, b : b + 1, :] for q in range(4)]
            old = state_ref[0, b, h]
            weight = jnp.sum(old * neg + jnp.where(eye, held, 0.0), axis=1, keepdims=True)
            new_ref[0, b, h] = old * decay + weight * rated


def renew(rows, mixed, state):
    group = 8
    heads, size = state.shape[2:4]
    block = pl.BlockSpec((1, group, heads, size, size), lambda l, i: (l, i, 0, 0, 0))
    whole = pl.BlockSpec(mixed.shape, lambda l, i: (0, 0))
    return pl.pallas_call(
        renew_body,
        grid=(2, state.shape[1] // group),
        out_shape=(
            jax.ShapeDtypeStruct(state.shape, state.dtype),
            jax.ShapeDtypeStruct(mixed.shape, mixed.dtype),
        ),
        in_specs=[
            pl.BlockSpec((1, 4, heads, group, size), lambda l, i: (l, 0, 0, i, 0)),
            whole,
            block,
        ],
        out_specs=(block, whole),
        compiler_params=pltpu.CompilerParams(vmem_limit_bytes=VMEM_LIMIT),
        name="renew",
    )(rows, mixed, state)


def on_device(
    tokens,
    lengths,
    norm_gain,
    w_recept,
    w_key,
    w_value,
    w_decay,
    w_rate,
    w_gate,
    w_out,
    decay_base,
    rate_base,
    group_gain,
    state,
):
    tp, dp = lax.axis_size("tp"), lax.axis_size("dp")
    weights = [w.transpose(0, 2, 1) for w in (w_recept, w_key, w_value, w_decay, w_rate, w_gate)]
    mixed, rows = step(
        tokens, lengths.reshape(1, -1), norm_gain, decay_base, rate_base, group_gain,
        weights, w_out.transpose(0, 2, 1), state, tp, dp,
    )
    states, mixed = renew(rows, mixed, state)
    return (mixed, states)


def solution(mesh):
    columns = P(None, None, ("tp", "dp"))
    in_specs = (
        (P("dp", "tp"), P("dp"), P())
        + (columns,) * 7
        + (P(None, "tp"),) * 3
        + (P(None, "dp", "tp", None, None),)
    )
    out_specs = (P("dp", "tp"), P(None, "dp", "tp", None, None))
    return jax.shard_map(
        on_device, mesh=mesh, in_specs=in_specs, out_specs=out_specs, check_vma=False
    )
```

```python
import contextlib
import functools

import jax
import jax.numpy as jnp
from jax import lax
from jax.experimental import pallas as pl
from jax.experimental.pallas import tpu as pltpu
from jax.sharding import PartitionSpec as P

STEP = 16
RMS_EPS = 1e-06
GROUP_EPS = 0.00064
VMEM_LIMIT = 55_000_000
MESH = pl.DeviceIdType.MESH


def scope(name):
    return contextlib.nullcontext()


def dot_t(a, b):
    return lax.dot_general(a, b, (((1,), (1,)), ((), ())), preferred_element_type=jnp.float32)


def plane_offsets(tp):
    ny = 4 if tp == 16 else tp
    nz = tp // ny
    hops = lambda k, n: min(k, n - k)
    offs = [(dz, dy) for dz in range(nz) for dy in range(ny)]
    offs.sort(key=lambda o: (hops(o[0], nz) + hops(o[1], ny), o))
    return ny, nz, offs


def step_body(
    tok, lens_hbm, gain_hbm, base_hbm, rate_hbm, ggain_hbm, wr, wk, wv, wd, wa, wg, wo, state,
    mixed_ref, st,
    xg, wcat, wot, vg, mg, pieces, turned, rows_ref, acc, square,
    lens, gain, base, rate, ggain,
    ag_send, a1_recv, b1_recv, fin_recv, ex_send, ex_recv, mg_send, mg_recv,
    wo_send, wo_recv, wc_send, wc_recv, own_sem, st_sem, small_sem,
    *, tp, dp,
):
    t, d = lax.axis_index("tp"), lax.axis_index("dp")
    nx = dp // 2
    x, core = d // 2, lax.rem(d, 2)
    sibling = d + 1 - 2 * core
    ny, nz, offs = plane_offsets(tp)
    z, y = t // ny, lax.rem(t, ny)
    rows, width = tok.shape
    slim = width // dp
    feat = tp * width
    half = rows // 2
    weights = (wr, wk, wv, wd, wa, wg)

    def plane(off):
        return lax.rem(z + off[0], nz) * ny + lax.rem(y + off[1], ny)

    def xpeer(k):
        return lax.rem(x + k + nx, nx)

    def remote(src, dst, ssem, rsem, tt, dd):
        return pltpu.make_async_remote_copy(
            src_ref=src, dst_ref=dst, send_sem=ssem, recv_sem=rsem,
            device_id=(tt, dd), device_id_type=MESH,
        )

    def arrived(ref, sem):
        remote(ref, ref, ag_send.at[0], sem, t, sibling).wait_recv()

    peers = [plane(o) for o in offs[1:]]
    far = peers[::-1]
    ks = [1, nx - 1] + list(range(2, nx - 1))
    xs = [xpeer(k) for k in ks]

    local = []

    def fetch(src, dst, sem):
        copy = pltpu.make_async_copy(src, dst, sem)
        copy.start()
        return copy

    def wrow(q):
        return pl.ds(pl.multiple_of(q * 2 * slim + core * slim, slim), slim)

    def worow(dd, start=0, count=None):
        return pl.ds(pl.multiple_of(dd * slim + start, slim // 2), slim if count is None else count)

    mine = pl.ds(pl.multiple_of(x * rows, rows), rows)
    own_tok = fetch(tok, xg.at[0, t, mine], small_sem.at[5])
    small = [
        fetch(src, dst, small_sem.at[i])
        for i, (src, dst) in enumerate(
            [(lens_hbm, lens), (gain_hbm, gain), (base_hbm, base), (rate_hbm, rate), (ggain_hbm, ggain)]
        )
    ]
    own_s = [fetch(state.at[0], st.at[0], st_sem.at[0])]
    own_w = [[fetch(weights[q].at[l], wcat.at[l, wrow(q)], own_sem.at[l, q]) for q in range(6)] for l in range(2)]
    own_o = [fetch(wo.at[l], wot.at[l, worow(d)], own_sem.at[l, 6]) for l in range(2)]
    own_s.append(fetch(state.at[1], st.at[1], st_sem.at[1]))

    barrier = pltpu.get_barrier_semaphore()
    everyone = [(p, d) for p in far] + [(t, 2 * o + core) for o in xs] + [(t, sibling)]
    for p in everyone:
        pl.semaphore_signal(barrier, inc=1, device_id=p, device_id_type=MESH)

    def turn(l):
        own_s[l].wait()

        def one(i, carry):
            for k in range(4):
                for p in range(nx // 2):
                    both = jnp.concatenate([st[l, i * 4 + k, 2 * p], st[l, i * 4 + k, 2 * p + 1]], axis=0)
                    turned[l, i * 4 + k, :, p * 128 : (p + 1) * 128] = both.T.astype(jnp.bfloat16)
            return carry

        lax.fori_loop(0, rows // 4, one, 0)

    with scope("turn0"):
        turn(0)
    with scope("barrier"):
        pl.semaphore_wait(barrier, len(everyone))
    with scope("small"):
        for copy in small:
            copy.wait()
        own_tok.wait()

    def own_rows(h, xx):
        return pl.ds(pl.multiple_of(xx * rows + h * half, half), half)

    def gather_start(l, source):
        sent = []

        def send(src, dst, rsem, tt, dd):
            copy = remote(src, dst, ag_send.at[len(sent)], rsem, tt, dd)
            copy.start()
            sent.append(copy)

        a_dst, b_dst = xg.at[l, t, own_rows(0, x)], xg.at[l, t, own_rows(1, x)]
        for o in xs:
            send(source(0), a_dst, a1_recv.at[l, x], t, 2 * o + core)
        for p in far:
            send(source(1), b_dst, b1_recv.at[l, t], p, d)
        for p in far:
            send(source(0), a_dst, fin_recv.at[l, t], p, d)
        for o in xs:
            send(source(1), b_dst, fin_recv.at[l, t], t, 2 * o + core)
        return sent, send

    def gather_relay(l, send):
        for i, o in enumerate(xs):
            with scope(f"a{l}_{i}"):
                block = xg.at[l, t, own_rows(0, o)]
                arrived(block, a1_recv.at[l, o])
                for p in far:
                    send(block, block, fin_recv.at[l, t], p, d)
        for i, p in enumerate(peers):
            with scope(f"b{l}_{i}"):
                block = xg.at[l, p, own_rows(1, x)]
                arrived(block, b1_recv.at[l, p])
                for o in xs:
                    send(block, block, fin_recv.at[l, p], t, 2 * o + core)

    def prepare(l):
        for q in range(6):
            own_w[l][q].wait()
        for q in range(6):
            other = pl.ds(pl.multiple_of(q * 2 * slim + (1 - core) * slim, slim), slim)
            arrived(wcat.at[l, other], wc_recv.at[l, q])
        line = gain[l : l + 1, :]

        def one(i, carry):
            part = pl.ds(pl.multiple_of(i * 16, 16), 16)
            wcat[l, part, :] = (wcat[l, part, :].astype(jnp.float32) * line).astype(jnp.bfloat16)
            return carry

        lax.fori_loop(0, 12 * slim // 16, one, 0)

    def project(l):
        acc[...] = jnp.zeros_like(acc)
        square[...] = jnp.zeros_like(square)
        for o in offs:
            tt = plane(o)
            count = (nx - 1) * half if o == (0, 0) else (2 * nx - 1) * half
            with scope(f"x{l}_{o[0]}_{o[1]}"):
                arrived(xg.at[l, tt, pl.ds(0, count)], fin_recv.at[l, tt])
            block = xg[l, tt]
            cols = pl.ds(pl.multiple_of(tt * width, width), width)
            acc[...] += dot_t(block, wcat[l, :, cols])
            values = block.astype(jnp.float32)
            values = values * values
            total = values[:, :128]
            for j in range(1, width // 128):
                total += values[:, j * 128 : (j + 1) * 128]
            square[...] += total
        factor = lax.rsqrt(jnp.sum(square[...], axis=1, keepdims=True) / feat + RMS_EPS)
        done = (acc[...] * factor).astype(jnp.bfloat16)
        for j in range(nx):
            pieces[l, j] = done[j * rows : (j + 1) * rows]
        sent = []
        for i, o in enumerate(xs):
            copy = remote(pieces.at[l, o], vg.at[l, x], ex_send.at[l, i], ex_recv.at[l, x], t, 2 * o + core)
            copy.start()
            sent.append(copy)
        vg[l, x] = pieces[l, x]
        return sent

    def out_slot(l, xx, cc, start=0, count=None):
        return wot.at[l, worow(2 * xx + cc, start, count)]

    def out_start(l):
        own_o[l].wait()
        up, down = xpeer(1), xpeer(-1)
        block = out_slot(l, x, core)
        sent = [
            remote(block, block, wo_send.at[l, 0], wo_recv.at[l, 0], t, 2 * up + core),
            remote(block, block, wo_send.at[l, 1], wo_recv.at[l, 1], t, 2 * down + core),
            remote(block, block, wo_send.at[l, 2], wo_recv.at[l, 4], t, sibling),
        ]
        for copy in sent:
            copy.start()
        return sent

    def out_relay(l, sent):
        up, down, across = xpeer(1), xpeer(-1), xpeer(2)
        part = slim // 2
        below, above = out_slot(l, down, core), out_slot(l, up, core)
        arrived(below, wo_recv.at[l, 0])
        first = out_slot(l, down, core, 0, part)
        one = remote(first, first, wo_send.at[l, 3], wo_recv.at[l, 2], t, 2 * up + core)
        one.start()
        two = remote(below, below, wo_send.at[l, 4], wo_recv.at[l, 5], t, sibling)
        two.start()
        arrived(above, wo_recv.at[l, 1])
        second = out_slot(l, up, core, part, part)
        three = remote(second, second, wo_send.at[l, 5], wo_recv.at[l, 3], t, 2 * down + core)
        three.start()
        four = remote(above, above, wo_send.at[l, 6], wo_recv.at[l, 6], t, sibling)
        four.start()
        sent += [one, two, three, four]

    def out_finish(l, sent):
        up, down, across = xpeer(1), xpeer(-1), xpeer(2)
        part = slim // 2
        arrived(out_slot(l, across, core, 0, part), wo_recv.at[l, 2])
        arrived(out_slot(l, across, core, part, part), wo_recv.at[l, 3])
        block = out_slot(l, across, core)
        copy = remote(block, block, wo_send.at[l, 7], wo_recv.at[l, 7], t, sibling)
        copy.start()
        sent.append(copy)
        for i, xx in enumerate((x, down, up, across)):
            arrived(out_slot(l, xx, 1 - core), wo_recv.at[l, 4 + i])

    size = 2 * slim
    sub = lax.broadcasted_iota(jnp.int32, (rows, rows), 0)
    lane = lax.broadcasted_iota(jnp.int32, (rows, rows), 1)
    spread = jnp.where(sub == lane, lens[...].astype(jnp.float32), 0.0)
    live = jnp.sum(spread, axis=1, keepdims=True) > STEP
    eight = lax.broadcasted_iota(jnp.int32, (8, 2 * size), 0)
    left = lax.broadcasted_iota(jnp.int32, (8, 2 * size), 1) < size
    left_half = lax.broadcasted_iota(jnp.int32, (half, 2 * size), 1) < size

    def paired(parts, p):
        return jnp.concatenate([parts[2 * p], parts[2 * p + 1]], axis=1)

    def by_head(values):
        one = jnp.sum(jnp.where(left_half, values, 0.0), axis=1, keepdims=True)
        two = jnp.sum(jnp.where(left_half, 0.0, values), axis=1, keepdims=True)
        return jnp.where(left_half, one, two) / size

    def recur(l):
        with scope(f"exchange{l}"):
            for o in xs:
                arrived(vg.at[l, o], ex_recv.at[l, o])
        looks, extras, gates = [], [], []
        for h in range(nx):
            part = slice(h * size, (h + 1) * size)
            recept, key, value, decay_pre, rate_pre, gate_pre = [
                vg[l, h, :, q * size : (q + 1) * size].astype(jnp.float32) for q in range(6)
            ]
            decay = jnp.exp(-jnp.exp(-jax.nn.softplus(-(base[l : l + 1, part] + decay_pre)) - 0.5))
            learn = jax.nn.sigmoid(rate[l : l + 1, part] + rate_pre)
            length = jnp.maximum(jnp.sqrt(jnp.sum(key * key, axis=1, keepdims=True)), 1e-12)
            blend = jnp.sum(key * learn * recept, axis=1, keepdims=True)
            unit = key / length
            held = value * length
            rows_ref[l, 0, h] = jnp.where(live, -unit, 0.0)
            rows_ref[l, 1, h] = jnp.where(live, held, 0.0)
            rows_ref[l, 2, h] = jnp.where(live, decay, 1.0)
            rows_ref[l, 3, h] = unit * learn
            looks.append(decay * recept - (blend / length) * unit)
            extras.append(blend * value)
            gates.append(jax.nn.sigmoid(gate_pre) * ggain[l : l + 1, part])
        gates = [paired(gates, p) for p in range(nx // 2)]
        extras = [paired(extras, p) for p in range(nx // 2)]
        sent = []
        for g in range(2):
            reads = [[] for p in range(nx // 2)]
            for k in range(half // 8):
                low = g * half + k * 8
                look = jnp.concatenate([v[low : low + 8] for v in looks], axis=0).astype(jnp.bfloat16)
                sums = [extras[p][low : low + 8] for p in range(nx // 2)]
                for b in range(8):
                    got = jnp.dot(look, turned[l, low + b], preferred_element_type=jnp.float32)
                    for h in range(nx):
                        p = h // 2
                        side = left if h % 2 == 0 else jnp.logical_not(left)
                        piece = got[h * 8 : (h + 1) * 8, p * 128 : (p + 1) * 128]
                        sums[p] += jnp.where((eight == b) & side, piece, 0.0)
                for p in range(nx // 2):
                    reads[p].append(sums[p])
            span = slice(g * half, (g + 1) * half)
            outs = []
            for p in range(nx // 2):
                read = jnp.concatenate(reads[p], axis=0)
                apart = read - by_head(read)
                normal = apart * lax.rsqrt(by_head(apart * apart) + GROUP_EPS) * gates[p][span]
                outs.append(jnp.where(live[span], normal, 0.0).astype(jnp.bfloat16))
            span = pl.ds(g * half, half)
            mg[l, t, span, :] = jnp.concatenate(outs, axis=1)
            block = mg.at[l, t, span]
            for i, p in enumerate(far):
                copy = remote(block, block, mg_send.at[l, g * (tp - 1) + i], mg_recv.at[l, t], p, d)
                copy.start()
                sent.append(copy)
        return sent

    eye = lax.broadcasted_iota(jnp.int32, (size, size), 0) == lax.broadcasted_iota(jnp.int32, (size, size), 1)

    def update(l):
        def one(i, carry):
            for k in range(4):
                b = i * 4 + k
                for h in range(nx):
                    neg, held, decay, rated = [rows_ref[l, q, h, pl.ds(b, 1), :] for q in range(4)]
                    old = st[l, b, h]
                    weight = jnp.sum(old * neg + jnp.where(eye, held, 0.0), axis=1, keepdims=True)
                    st[l, b, h] = old * decay + weight * rated
            return carry

        lax.fori_loop(0, rows // 4, one, 0)

    def fold(l):
        total = jnp.zeros((rows, width), jnp.float32)
        for o in offs:
            tt = plane(o)
            if o != (0, 0):
                with scope(f"m{l}_{o[0]}_{o[1]}"):
                    arrived(mg.at[l, tt], mg_recv.at[l, tt])
            cols = pl.ds(pl.multiple_of(tt * width, width), width)
            total += dot_t(mg[l, tt], wot[l, :, cols])
        return total.astype(jnp.bfloat16)

    for l in range(2):
        with scope(f"start{l}"):
            if l == 1:
                xg[1, t, mine, :] = current
            sent, send = gather_start(l, lambda h: xg.at[l, t, own_rows(h, x)])
            if l == 0:
                shared = []
                for ll in range(2):
                    for q in range(6):
                        copy = remote(
                            weights[q].at[ll], wcat.at[ll, wrow(q)],
                            wc_send.at[ll, q], wc_recv.at[ll, q], t, sibling,
                        )
                        copy.start()
                        shared.append(copy)
        gather_relay(l, send)
        if l == 0:
            with scope("prepare0"):
                prepare(0)
        else:
            with scope("update0"):
                update(0)
        with scope(f"project{l}"):
            traded = project(l)
            folded = out_start(l)
            for copy in sent:
                copy.wait_send()
        with scope(f"recur{l}"):
            mixed = recur(l)
        with scope(f"outrelay{l}"):
            out_relay(l, folded)
        if l == 0:
            with scope("prepare1"):
                prepare(1)
                turn(1)
        else:
            with scope("update1"):
                update(1)
        with scope(f"outfinish{l}"):
            out_finish(l, folded)
        with scope(f"fold{l}"):
            current = fold(l)
        for copy in traded + folded + mixed:
            copy.wait_send()
    mixed_ref[...] = current
    for copy in shared:
        copy.wait_send()


def step(tok, lens, gain, base, rate, ggain, weights, wo, state, tp, dp):
    rows, width = tok.shape
    slim = width // dp
    nx = dp // 2
    feat = tp * width
    bf = jnp.bfloat16
    vmem, hbm = pl.BlockSpec(memory_space=pltpu.VMEM), pl.BlockSpec(memory_space=pltpu.HBM)
    dma = pltpu.SemaphoreType.DMA
    half = rows // 2
    return pl.pallas_call(
        functools.partial(step_body, tp=tp, dp=dp),
        out_shape=(
            pltpu.VMEM((rows, width), bf),
            pltpu.VMEM(state.shape, state.dtype),
        ),
        in_specs=[hbm] * 14,
        out_specs=(vmem, vmem),
        scratch_shapes=[
            pltpu.VMEM((2, tp, nx * rows, width), bf),
            pltpu.VMEM((2, 12 * slim, feat), bf),
            pltpu.VMEM((2, width, feat), bf),
            pltpu.VMEM((2, nx, rows, 12 * slim), bf),
            pltpu.VMEM((2, tp, rows, width), bf),
            pltpu.VMEM((2, nx, rows, 12 * slim), bf),
            pltpu.VMEM((2, rows, 2 * slim, nx * 2 * slim), bf),
            pltpu.VMEM((2, 4, nx, rows, 2 * slim), jnp.float32),
            pltpu.VMEM((nx * rows, 12 * slim), jnp.float32),
            pltpu.VMEM((nx * rows, 128), jnp.float32),
            pltpu.VMEM(lens.shape, lens.dtype),
            pltpu.VMEM(gain.shape, gain.dtype),
            pltpu.VMEM(base.shape, base.dtype),
            pltpu.VMEM(rate.shape, rate.dtype),
            pltpu.VMEM(ggain.shape, ggain.dtype),
            dma(((nx - 1) * (tp + 1) + (tp - 1) * (nx + 1),)),
            dma((2, nx)),
            dma((2, tp)),
            dma((2, tp)),
            dma((2, nx)),
            dma((2, nx)),
            dma((2, 2 * tp)),
            dma((2, tp)),
            dma((2, 8)),
            dma((2, 8)),
            dma((2, 6)),
            dma((2, 6)),
            dma((2, 7)),
            dma((2,)),
            dma((6,)),
        ],
        compiler_params=pltpu.CompilerParams(
            collective_id=0, has_side_effects=True, vmem_limit_bytes=VMEM_LIMIT
        ),
        name="step",
    )(tok, lens, gain, base, rate, ggain, *weights, wo, state)


def put_body(mixed_ref, state_ref, out_ref, new_ref, sem):
    count = state_ref.shape[0] * 4
    part = state_ref.shape[1] // 4
    copies = [pltpu.make_async_copy(mixed_ref, out_ref, sem.at[count])]
    for i in range(count):
        span = pl.ds(i % 4 * part, part)
        copies.append(
            pltpu.make_async_copy(state_ref.at[i // 4, span], new_ref.at[i // 4, span], sem.at[i])
        )
    for copy in copies:
        copy.start()
    for copy in copies:
        copy.wait()


def put(mixed, state):
    vmem, hbm = pl.BlockSpec(memory_space=pltpu.VMEM), pl.BlockSpec(memory_space=pltpu.HBM)
    return pl.pallas_call(
        put_body,
        out_shape=(
            jax.ShapeDtypeStruct(mixed.shape, mixed.dtype),
            jax.ShapeDtypeStruct(state.shape, state.dtype),
        ),
        in_specs=[vmem, vmem],
        out_specs=(hbm, hbm),
        scratch_shapes=[pltpu.SemaphoreType.DMA((state.shape[0] * 4 + 1,))],
        compiler_params=pltpu.CompilerParams(vmem_limit_bytes=4 * 1024 * 1024),
        name="put",
    )(mixed, state)


def on_device(
    tokens,
    lengths,
    norm_gain,
    w_recept,
    w_key,
    w_value,
    w_decay,
    w_rate,
    w_gate,
    w_out,
    decay_base,
    rate_base,
    group_gain,
    state,
):
    tp, dp = lax.axis_size("tp"), lax.axis_size("dp")
    weights = [w.transpose(0, 2, 1) for w in (w_recept, w_key, w_value, w_decay, w_rate, w_gate)]
    mixed, states = step(
        tokens, lengths.reshape(1, -1), norm_gain, decay_base, rate_base, group_gain,
        weights, w_out.transpose(0, 2, 1), state, tp, dp,
    )
    return put(mixed, states)


def solution(mesh):
    columns = P(None, None, ("tp", "dp"))
    in_specs = (
        (P("dp", "tp"), P("dp"), P())
        + (columns,) * 7
        + (P(None, "tp"),) * 3
        + (P(None, "dp", "tp", None, None),)
    )
    out_specs = (P("dp", "tp"), P(None, "dp", "tp", None, None))
    return jax.shard_map(
        on_device, mesh=mesh, in_specs=in_specs, out_specs=out_specs, check_vma=False
    )
```

```python
import contextlib
import functools

import jax
import jax.numpy as jnp
from jax import lax
from jax.experimental import pallas as pl
from jax.experimental.pallas import tpu as pltpu
from jax.sharding import PartitionSpec as P

STEP = 16
RMS_EPS = 1e-06
GROUP_EPS = 0.00064
VMEM_LIMIT = 55_000_000
MESH = pl.DeviceIdType.MESH


def scope(name):
    return contextlib.nullcontext()


def dot_t(a, b):
    return lax.dot_general(a, b, (((1,), (1,)), ((), ())), preferred_element_type=jnp.float32)


def plane_offsets(tp):
    ny = 4 if tp == 16 else tp
    nz = tp // ny
    hops = lambda k, n: min(k, n - k)
    offs = [(dz, dy) for dz in range(nz) for dy in range(ny)]
    offs.sort(key=lambda o: (hops(o[0], nz) + hops(o[1], ny), o))
    return ny, nz, offs


def step_body(
    tok, lens_hbm, gain_hbm, base_hbm, rate_hbm, ggain_hbm, wr, wk, wv, wd, wa, wg, wo, state,
    mixed_ref, st,
    xg, wcat, wot, vg, mg, pieces, turned, rows_ref, acc, square,
    lens, gain, base, rate, ggain,
    ag_send, a1_recv, b1_recv, fin_recv, ex_send, ex_recv, mg_send, mg_recv,
    wo_send, wo_recv, wc_send, wc_recv, own_sem, st_sem, small_sem,
    *, tp, dp,
):
    t, d = lax.axis_index("tp"), lax.axis_index("dp")
    nx = dp // 2
    x, core = d // 2, lax.rem(d, 2)
    sibling = d + 1 - 2 * core
    ny, nz, offs = plane_offsets(tp)
    z, y = t // ny, lax.rem(t, ny)
    rows, width = tok.shape
    slim = width // dp
    feat = tp * width
    half = rows // 2
    weights = (wr, wk, wv, wd, wa, wg)

    def plane(off):
        return lax.rem(z + off[0], nz) * ny + lax.rem(y + off[1], ny)

    def xpeer(k):
        return lax.rem(x + k + nx, nx)

    def remote(src, dst, ssem, rsem, tt, dd):
        return pltpu.make_async_remote_copy(
            src_ref=src, dst_ref=dst, send_sem=ssem, recv_sem=rsem,
            device_id=(tt, dd), device_id_type=MESH,
        )

    def arrived(ref, sem):
        remote(ref, ref, ag_send.at[0], sem, t, sibling).wait_recv()

    peers = [plane(o) for o in offs[1:]]
    far = peers[::-1]
    ks = [1, nx - 1] + list(range(2, nx - 1))
    xs = [xpeer(k) for k in ks]


    def fetch(src, dst, sem):
        copy = pltpu.make_async_copy(src, dst, sem)
        copy.start()
        return copy

    def wrow(q):
        return pl.ds(pl.multiple_of(q * 2 * slim + core * slim, slim), slim)

    def worow(dd, start=0, count=None):
        return pl.ds(pl.multiple_of(dd * slim + start, slim // 2), slim if count is None else count)

    mine = pl.ds(pl.multiple_of(x * rows, rows), rows)
    own_tok = fetch(tok, xg.at[0, t, mine], small_sem.at[5])
    barrier = pltpu.get_barrier_semaphore()
    everyone = [(p, d) for p in far] + [(t, 2 * o + core) for o in xs] + [(t, sibling)]
    for p in everyone:
        pl.semaphore_signal(barrier, inc=1, device_id=p, device_id_type=MESH)
    small = [
        fetch(src, dst, small_sem.at[i])
        for i, (src, dst) in enumerate(
            [(lens_hbm, lens), (gain_hbm, gain), (base_hbm, base), (rate_hbm, rate), (ggain_hbm, ggain)]
        )
    ]
    own_s = [fetch(state.at[0], st.at[0], st_sem.at[0])]
    own_w = [[fetch(weights[q].at[l], wcat.at[l, wrow(q)], own_sem.at[l, q]) for q in range(6)] for l in range(2)]
    own_o = [fetch(wo.at[l], wot.at[l, worow(d)], own_sem.at[l, 6]) for l in range(2)]
    own_s.append(fetch(state.at[1], st.at[1], st_sem.at[1]))


    def turn(l):
        own_s[l].wait()

        def one(i, carry):
            for k in range(4):
                for p in range(nx // 2):
                    both = jnp.concatenate([st[l, i * 4 + k, 2 * p], st[l, i * 4 + k, 2 * p + 1]], axis=0)
                    turned[l, i * 4 + k, :, p * 128 : (p + 1) * 128] = both.T.astype(jnp.bfloat16)
            return carry

        lax.fori_loop(0, rows // 4, one, 0)

    with scope("barrier"):
        pl.semaphore_wait(barrier, len(everyone))
    with scope("small"):
        for copy in small:
            copy.wait()
        own_tok.wait()

    def own_rows(h, xx):
        return pl.ds(pl.multiple_of(xx * rows + h * half, half), half)

    def gather_start(l, source):
        sent = []

        def send(src, dst, rsem, tt, dd):
            copy = remote(src, dst, ag_send.at[len(sent)], rsem, tt, dd)
            copy.start()
            sent.append(copy)

        a_dst, b_dst = xg.at[l, t, own_rows(0, x)], xg.at[l, t, own_rows(1, x)]
        for o in xs:
            send(source(0), a_dst, a1_recv.at[l, x], t, 2 * o + core)
        for p in far:
            send(source(1), b_dst, b1_recv.at[l, t], p, d)
        for p in far:
            send(source(0), a_dst, fin_recv.at[l, t], p, d)
        for o in xs:
            send(source(1), b_dst, fin_recv.at[l, t], t, 2 * o + core)
        return sent, send

    def gather_relay(l, send):
        steps = [("a", o) for o in xs[:2]] + [("b", p) for p in peers[:4]]
        steps += [("a", o) for o in xs[2:]] + [("b", p) for p in peers[4:]]
        for i, (kind, o) in enumerate(steps):
            with scope(f"{kind}{l}_{i}"):
                if kind == "a":
                    block = xg.at[l, t, own_rows(0, o)]
                    arrived(block, a1_recv.at[l, o])
                    for p in far:
                        send(block, block, fin_recv.at[l, t], p, d)
                else:
                    block = xg.at[l, o, own_rows(1, x)]
                    arrived(block, b1_recv.at[l, o])
                    for p in xs:
                        send(block, block, fin_recv.at[l, o], t, 2 * p + core)

    def prepare(l):
        for q in range(6):
            own_w[l][q].wait()
        for q in range(6):
            other = pl.ds(pl.multiple_of(q * 2 * slim + (1 - core) * slim, slim), slim)
            arrived(wcat.at[l, other], wc_recv.at[l, q])
        line = gain[l : l + 1, :]

        def one(i, carry):
            part = pl.ds(pl.multiple_of(i * 16, 16), 16)
            wcat[l, part, :] = (wcat[l, part, :].astype(jnp.float32) * line).astype(jnp.bfloat16)
            return carry

        lax.fori_loop(0, 12 * slim // 16, one, 0)

    def project(l):
        acc[...] = jnp.zeros_like(acc)
        square[...] = jnp.zeros_like(square)
        for o in offs:
            tt = plane(o)
            count = (nx - 1) * half if o == (0, 0) else (2 * nx - 1) * half
            with scope(f"x{l}_{o[0]}_{o[1]}"):
                arrived(xg.at[l, tt, pl.ds(0, count)], fin_recv.at[l, tt])
            block = xg[l, tt]
            cols = pl.ds(pl.multiple_of(tt * width, width), width)
            acc[...] += dot_t(block, wcat[l, :, cols])
            values = block.astype(jnp.float32)
            values = values * values
            total = values[:, :128]
            for j in range(1, width // 128):
                total += values[:, j * 128 : (j + 1) * 128]
            square[...] += total
        factor = lax.rsqrt(jnp.sum(square[...], axis=1, keepdims=True) / feat + RMS_EPS)
        done = (acc[...] * factor).astype(jnp.bfloat16)
        for j in range(nx):
            pieces[l, j] = done[j * rows : (j + 1) * rows]
        sent = []
        for i, o in enumerate(xs):
            copy = remote(pieces.at[l, o], vg.at[l, x], ex_send.at[l, i], ex_recv.at[l, x], t, 2 * o + core)
            copy.start()
            sent.append(copy)
        vg[l, x] = pieces[l, x]
        return sent

    part = slim // 2
    up, down, across = xpeer(1), xpeer(-1), xpeer(2)

    def out_piece(l, xx, cc, piece):
        start, count = (0, slim) if piece is None else (piece * part, part)
        return wot.at[l, worow(2 * xx + cc, start, count)]

    def out_send(l, sent, n, xx, piece, to_x, to_core):
        block = out_piece(l, xx, core, piece)
        copy = remote(block, block, wo_send.at[l, n], wo_recv.at[l, n], t, 2 * to_x + to_core)
        copy.start()
        sent.append(copy)

    def out_arrived(l, n, xx, piece, cc=None):
        arrived(out_piece(l, xx, core if cc is None else cc, piece), wo_recv.at[l, n])

    def out_first(l):
        own_o[l].wait()
        sent = []
        out_send(l, sent, 0, x, 0, up, core)
        out_send(l, sent, 1, x, 1, down, core)
        out_send(l, sent, 6, x, None, x, 1 - core)
        return sent

    def out_second(l, sent):
        out_arrived(l, 0, down, 0)
        out_send(l, sent, 4, down, 0, up, core)
        out_send(l, sent, 7, down, 0, x, 1 - core)
        out_arrived(l, 1, up, 1)
        out_send(l, sent, 5, up, 1, down, core)
        out_send(l, sent, 8, up, 1, x, 1 - core)

    def out_third(l, sent):
        out_send(l, sent, 2, x, 1, up, core)
        out_send(l, sent, 3, x, 0, down, core)

    def out_fourth(l, sent):
        out_arrived(l, 4, across, 0)
        out_arrived(l, 5, across, 1)
        out_send(l, sent, 11, across, None, x, 1 - core)
        out_arrived(l, 2, down, 1)
        out_send(l, sent, 9, down, 1, x, 1 - core)
        out_arrived(l, 3, up, 0)
        out_send(l, sent, 10, up, 0, x, 1 - core)

    def out_finish(l):
        for n, xx, piece in ((6, x, None), (7, down, 0), (8, up, 1), (9, down, 1), (10, up, 0), (11, across, None)):
            out_arrived(l, n, xx, piece, 1 - core)

    size = 2 * slim
    sub = lax.broadcasted_iota(jnp.int32, (rows, rows), 0)
    lane = lax.broadcasted_iota(jnp.int32, (rows, rows), 1)
    spread = jnp.where(sub == lane, lens[...].astype(jnp.float32), 0.0)
    live = jnp.sum(spread, axis=1, keepdims=True) > STEP
    eight = lax.broadcasted_iota(jnp.int32, (8, 2 * size), 0)
    left = lax.broadcasted_iota(jnp.int32, (8, 2 * size), 1) < size
    left_half = lax.broadcasted_iota(jnp.int32, (half, 2 * size), 1) < size

    def paired(parts, p):
        return jnp.concatenate([parts[2 * p], parts[2 * p + 1]], axis=1)

    def by_head(values):
        one = jnp.sum(jnp.where(left_half, values, 0.0), axis=1, keepdims=True)
        two = jnp.sum(jnp.where(left_half, 0.0, values), axis=1, keepdims=True)
        return jnp.where(left_half, one, two) / size

    def recur(l):
        with scope(f"exchange{l}"):
            for o in xs:
                arrived(vg.at[l, o], ex_recv.at[l, o])
        looks, extras, gates = [], [], []
        for h in range(nx):
            part = slice(h * size, (h + 1) * size)
            recept, key, value, decay_pre, rate_pre, gate_pre = [
                vg[l, h, :, q * size : (q + 1) * size].astype(jnp.float32) for q in range(6)
            ]
            decay = jnp.exp(-jnp.exp(-jax.nn.softplus(-(base[l : l + 1, part] + decay_pre)) - 0.5))
            learn = jax.nn.sigmoid(rate[l : l + 1, part] + rate_pre)
            length = jnp.maximum(jnp.sqrt(jnp.sum(key * key, axis=1, keepdims=True)), 1e-12)
            blend = jnp.sum(key * learn * recept, axis=1, keepdims=True)
            unit = key / length
            held = value * length
            rows_ref[l, 0, h] = jnp.where(live, -unit, 0.0)
            rows_ref[l, 1, h] = jnp.where(live, held, 0.0)
            rows_ref[l, 2, h] = jnp.where(live, decay, 1.0)
            rows_ref[l, 3, h] = unit * learn
            looks.append(decay * recept - (blend / length) * unit)
            extras.append(blend * value)
            gates.append(jax.nn.sigmoid(gate_pre) * ggain[l : l + 1, part])
        gates = [paired(gates, p) for p in range(nx // 2)]
        extras = [paired(extras, p) for p in range(nx // 2)]
        sent = []
        for g in range(2):
            reads = [[] for p in range(nx // 2)]
            for k in range(half // 8):
                low = g * half + k * 8
                look = jnp.concatenate([v[low : low + 8] for v in looks], axis=0).astype(jnp.bfloat16)
                sums = [extras[p][low : low + 8] for p in range(nx // 2)]
                for b in range(8):
                    got = jnp.dot(look, turned[l, low + b], preferred_element_type=jnp.float32)
                    for h in range(nx):
                        p = h // 2
                        side = left if h % 2 == 0 else jnp.logical_not(left)
                        piece = got[h * 8 : (h + 1) * 8, p * 128 : (p + 1) * 128]
                        sums[p] += jnp.where((eight == b) & side, piece, 0.0)
                for p in range(nx // 2):
                    reads[p].append(sums[p])
            span = slice(g * half, (g + 1) * half)
            outs = []
            for p in range(nx // 2):
                read = jnp.concatenate(reads[p], axis=0)
                apart = read - by_head(read)
                normal = apart * lax.rsqrt(by_head(apart * apart) + GROUP_EPS) * gates[p][span]
                outs.append(jnp.where(live[span], normal, 0.0).astype(jnp.bfloat16))
            span = pl.ds(g * half, half)
            mg[l, t, span, :] = jnp.concatenate(outs, axis=1)
            block = mg.at[l, t, span]
            for i, p in enumerate(far):
                copy = remote(block, block, mg_send.at[l, g * (tp - 1) + i], mg_recv.at[l, t], p, d)
                copy.start()
                sent.append(copy)
        return sent

    eye = lax.broadcasted_iota(jnp.int32, (size, size), 0) == lax.broadcasted_iota(jnp.int32, (size, size), 1)

    def update(l):
        def one(i, carry):
            for k in range(4):
                b = i * 4 + k
                for h in range(nx):
                    neg, held, decay, rated = [rows_ref[l, q, h, pl.ds(b, 1), :] for q in range(4)]
                    old = st[l, b, h]
                    weight = jnp.sum(old * neg + jnp.where(eye, held, 0.0), axis=1, keepdims=True)
                    st[l, b, h] = old * decay + weight * rated
            return carry

        lax.fori_loop(0, rows // 4, one, 0)

    def fold(l):
        total = jnp.zeros((rows, width), jnp.float32)
        for o in offs:
            tt = plane(o)
            if o != (0, 0):
                with scope(f"m{l}_{o[0]}_{o[1]}"):
                    arrived(mg.at[l, tt], mg_recv.at[l, tt])
            cols = pl.ds(pl.multiple_of(tt * width, width), width)
            total += dot_t(mg[l, tt], wot[l, :, cols])
        return total.astype(jnp.bfloat16)

    for l in range(2):
        with scope(f"start{l}"):
            if l == 1:
                xg[1, t, mine, :] = current
            sent, send = gather_start(l, lambda h: xg.at[l, t, own_rows(h, x)])
            if l == 0:
                shared = []
                for ll in range(2):
                    for q in range(6):
                        copy = remote(
                            weights[q].at[ll], wcat.at[ll, wrow(q)],
                            wc_send.at[ll, q], wc_recv.at[ll, q], t, sibling,
                        )
                        copy.start()
                        shared.append(copy)
            folded = out_first(l)
        if l == 0:
            with scope("turn0"):
                turn(0)
        gather_relay(l, send)
        with scope(f"outsecond{l}"):
            out_second(l, folded)
        if l == 0:
            with scope("prepare0"):
                prepare(0)
        else:
            with scope("update0"):
                update(0)
        with scope(f"project{l}"):
            traded = project(l)
            out_third(l, folded)
            for copy in sent:
                copy.wait_send()
        with scope(f"recur{l}"):
            mixed = recur(l)
        if l == 0:
            with scope("prepare1"):
                prepare(1)
                turn(1)
        else:
            with scope("update1"):
                update(1)
        with scope(f"outfourth{l}"):
            out_fourth(l, folded)
        with scope(f"outfinish{l}"):
            out_finish(l)
        with scope(f"fold{l}"):
            current = fold(l)
        for copy in traded + folded + mixed:
            copy.wait_send()
    mixed_ref[...] = current
    for copy in shared:
        copy.wait_send()


def step(tok, lens, gain, base, rate, ggain, weights, wo, state, tp, dp):
    rows, width = tok.shape
    slim = width // dp
    nx = dp // 2
    feat = tp * width
    bf = jnp.bfloat16
    vmem, hbm = pl.BlockSpec(memory_space=pltpu.VMEM), pl.BlockSpec(memory_space=pltpu.HBM)
    dma = pltpu.SemaphoreType.DMA
    half = rows // 2
    return pl.pallas_call(
        functools.partial(step_body, tp=tp, dp=dp),
        out_shape=(
            pltpu.VMEM((rows, width), bf),
            pltpu.VMEM(state.shape, state.dtype),
        ),
        in_specs=[hbm] * 14,
        out_specs=(vmem, vmem),
        scratch_shapes=[
            pltpu.VMEM((2, tp, nx * rows, width), bf),
            pltpu.VMEM((2, 12 * slim, feat), bf),
            pltpu.VMEM((2, width, feat), bf),
            pltpu.VMEM((2, nx, rows, 12 * slim), bf),
            pltpu.VMEM((2, tp, rows, width), bf),
            pltpu.VMEM((2, nx, rows, 12 * slim), bf),
            pltpu.VMEM((2, rows, 2 * slim, nx * 2 * slim), bf),
            pltpu.VMEM((2, 4, nx, rows, 2 * slim), jnp.float32),
            pltpu.VMEM((nx * rows, 12 * slim), jnp.float32),
            pltpu.VMEM((nx * rows, 128), jnp.float32),
            pltpu.VMEM(lens.shape, lens.dtype),
            pltpu.VMEM(gain.shape, gain.dtype),
            pltpu.VMEM(base.shape, base.dtype),
            pltpu.VMEM(rate.shape, rate.dtype),
            pltpu.VMEM(ggain.shape, ggain.dtype),
            dma(((nx - 1) * (tp + 1) + (tp - 1) * (nx + 1),)),
            dma((2, nx)),
            dma((2, tp)),
            dma((2, tp)),
            dma((2, nx)),
            dma((2, nx)),
            dma((2, 2 * tp)),
            dma((2, tp)),
            dma((2, 12)),
            dma((2, 12)),
            dma((2, 6)),
            dma((2, 6)),
            dma((2, 7)),
            dma((2,)),
            dma((6,)),
        ],
        compiler_params=pltpu.CompilerParams(
            collective_id=0, has_side_effects=True, vmem_limit_bytes=VMEM_LIMIT
        ),
        name="step",
    )(tok, lens, gain, base, rate, ggain, *weights, wo, state)


def put_body(mixed_ref, state_ref, out_ref, new_ref, sem):
    count = state_ref.shape[0] * 4
    part = state_ref.shape[1] // 4
    copies = [pltpu.make_async_copy(mixed_ref, out_ref, sem.at[count])]
    for i in range(count):
        span = pl.ds(i % 4 * part, part)
        copies.append(
            pltpu.make_async_copy(state_ref.at[i // 4, span], new_ref.at[i // 4, span], sem.at[i])
        )
    for copy in copies:
        copy.start()
    for copy in copies:
        copy.wait()


def put(mixed, state):
    vmem, hbm = pl.BlockSpec(memory_space=pltpu.VMEM), pl.BlockSpec(memory_space=pltpu.HBM)
    return pl.pallas_call(
        put_body,
        out_shape=(
            jax.ShapeDtypeStruct(mixed.shape, mixed.dtype),
            jax.ShapeDtypeStruct(state.shape, state.dtype),
        ),
        in_specs=[vmem, vmem],
        out_specs=(hbm, hbm),
        scratch_shapes=[pltpu.SemaphoreType.DMA((state.shape[0] * 4 + 1,))],
        compiler_params=pltpu.CompilerParams(vmem_limit_bytes=4 * 1024 * 1024),
        name="put",
    )(mixed, state)


def on_device(
    tokens,
    lengths,
    norm_gain,
    w_recept,
    w_key,
    w_value,
    w_decay,
    w_rate,
    w_gate,
    w_out,
    decay_base,
    rate_base,
    group_gain,
    state,
):
    tp, dp = lax.axis_size("tp"), lax.axis_size("dp")
    weights = [w.transpose(0, 2, 1) for w in (w_recept, w_key, w_value, w_decay, w_rate, w_gate)]
    mixed, states = step(
        tokens, lengths.reshape(1, -1), norm_gain, decay_base, rate_base, group_gain,
        weights, w_out.transpose(0, 2, 1), state, tp, dp,
    )
    return put(mixed, states)


def solution(mesh):
    columns = P(None, None, ("tp", "dp"))
    in_specs = (
        (P("dp", "tp"), P("dp"), P())
        + (columns,) * 7
        + (P(None, "tp"),) * 3
        + (P(None, "dp", "tp", None, None),)
    )
    out_specs = (P("dp", "tp"), P(None, "dp", "tp", None, None))
    return jax.shard_map(
        on_device, mesh=mesh, in_specs=in_specs, out_specs=out_specs, check_vma=False
    )
```

```python
import contextlib
import functools

import jax
import jax.numpy as jnp
from jax import lax
from jax.experimental import pallas as pl
from jax.experimental.pallas import tpu as pltpu
from jax.sharding import PartitionSpec as P

STEP = 16
RMS_EPS = 1e-06
GROUP_EPS = 0.00064
VMEM_LIMIT = 55_000_000
MESH = pl.DeviceIdType.MESH


def scope(name):
    return contextlib.nullcontext()


def dot_t(a, b):
    return lax.dot_general(a, b, (((1,), (1,)), ((), ())), preferred_element_type=jnp.float32)


def plane_offsets(tp):
    ny = 4 if tp == 16 else tp
    nz = tp // ny
    hops = lambda k, n: min(k, n - k)
    offs = [(dz, dy) for dz in range(nz) for dy in range(ny)]
    offs.sort(key=lambda o: (hops(o[0], nz) + hops(o[1], ny), o))
    return ny, nz, offs


def step_body(
    tok, lens_hbm, gain_hbm, base_hbm, rate_hbm, ggain_hbm, wr, wk, wv, wd, wa, wg, wo, state,
    mixed_ref, st,
    xg, wcat, wot, vg, mg, pieces, turned, rows_ref, acc, square,
    lens, gain, base, rate, ggain,
    ag_send, a1_recv, b1_recv, fin_recv, ex_send, ex_recv, mg_send, mg_recv,
    wo_send, wo_recv, wc_send, wc_recv, own_sem, st_sem, small_sem,
    *, tp, dp,
):
    t, d = lax.axis_index("tp"), lax.axis_index("dp")
    nx = dp // 2
    x, core = d // 2, lax.rem(d, 2)
    sibling = d + 1 - 2 * core
    ny, nz, offs = plane_offsets(tp)
    z, y = t // ny, lax.rem(t, ny)
    rows, width = tok.shape
    slim = width // dp
    feat = tp * width
    half = rows // 2
    weights = (wr, wk, wv, wd, wa, wg)

    def plane(off):
        return lax.rem(z + off[0], nz) * ny + lax.rem(y + off[1], ny)

    def xpeer(k):
        return lax.rem(x + k + nx, nx)

    def remote(src, dst, ssem, rsem, tt, dd):
        return pltpu.make_async_remote_copy(
            src_ref=src, dst_ref=dst, send_sem=ssem, recv_sem=rsem,
            device_id=(tt, dd), device_id_type=MESH,
        )

    def arrived(ref, sem):
        remote(ref, ref, ag_send.at[0], sem, t, sibling).wait_recv()

    peers = [plane(o) for o in offs[1:]]
    far = peers[::-1]
    ks = [1, nx - 1] + list(range(2, nx - 1))
    xs = [xpeer(k) for k in ks]


    def fetch(src, dst, sem):
        copy = pltpu.make_async_copy(src, dst, sem)
        copy.start()
        return copy

    def wrow(q):
        return pl.ds(pl.multiple_of(q * 2 * slim + core * slim, slim), slim)

    def worow(dd, start=0, count=None):
        return pl.ds(pl.multiple_of(dd * slim + start, slim // 2), slim if count is None else count)

    mine = pl.ds(pl.multiple_of(x * rows, rows), rows)
    own_tok = fetch(tok, xg.at[0, t, mine], small_sem.at[5])
    barrier = pltpu.get_barrier_semaphore()
    everyone = [(p, d) for p in far] + [(t, 2 * o + core) for o in xs] + [(t, sibling)]
    for p in everyone:
        pl.semaphore_signal(barrier, inc=1, device_id=p, device_id_type=MESH)
    small = [
        fetch(src, dst, small_sem.at[i])
        for i, (src, dst) in enumerate(
            [(lens_hbm, lens), (gain_hbm, gain), (base_hbm, base), (rate_hbm, rate), (ggain_hbm, ggain)]
        )
    ]
    own_s = [fetch(state.at[0], st.at[0], st_sem.at[0])]
    own_w = [[fetch(weights[q].at[l], wcat.at[l, wrow(q)], own_sem.at[l, q]) for q in range(6)] for l in range(2)]
    own_o = [fetch(wo.at[l], wot.at[l, worow(d)], own_sem.at[l, 6]) for l in range(2)]
    own_s.append(fetch(state.at[1], st.at[1], st_sem.at[1]))


    def turn(l):
        own_s[l].wait()

        def one(i, carry):
            for k in range(4):
                for p in range(nx // 2):
                    both = jnp.concatenate([st[l, i * 4 + k, 2 * p], st[l, i * 4 + k, 2 * p + 1]], axis=0)
                    turned[l, i * 4 + k, :, p * 128 : (p + 1) * 128] = both.T.astype(jnp.bfloat16)
            return carry

        lax.fori_loop(0, rows // 4, one, 0)

    with scope("barrier"):
        pl.semaphore_wait(barrier, len(everyone))
    with scope("small"):
        for copy in small:
            copy.wait()
        own_tok.wait()

    def own_rows(h, xx):
        return pl.ds(pl.multiple_of(xx * rows + h * half, half), half)

    def gather_start(l, source):
        sent = []

        def send(src, dst, rsem, tt, dd):
            copy = remote(src, dst, ag_send.at[len(sent)], rsem, tt, dd)
            copy.start()
            sent.append(copy)

        a_dst, b_dst = xg.at[l, t, own_rows(0, x)], xg.at[l, t, own_rows(1, x)]
        for o in xs:
            send(source(0), a_dst, a1_recv.at[l, x], t, 2 * o + core)
        for p in far:
            send(source(1), b_dst, b1_recv.at[l, t], p, d)
        for p in far:
            send(source(0), a_dst, fin_recv.at[l, t], p, d)
        for o in xs:
            send(source(1), b_dst, fin_recv.at[l, t], t, 2 * o + core)
        return sent, send

    def gather_relay(l, send):
        steps = [("a", o) for o in xs[:2]] + [("b", p) for p in peers[:4]]
        steps += [("a", o) for o in xs[2:]] + [("b", p) for p in peers[4:]]
        for i, (kind, o) in enumerate(steps):
            with scope(f"{kind}{l}_{i}"):
                if kind == "a":
                    block = xg.at[l, t, own_rows(0, o)]
                    arrived(block, a1_recv.at[l, o])
                    for p in far:
                        send(block, block, fin_recv.at[l, t], p, d)
                else:
                    block = xg.at[l, o, own_rows(1, x)]
                    arrived(block, b1_recv.at[l, o])
                    for p in xs:
                        send(block, block, fin_recv.at[l, o], t, 2 * p + core)

    def prepare(l):
        for q in range(6):
            own_w[l][q].wait()
        for q in range(6):
            other = pl.ds(pl.multiple_of(q * 2 * slim + (1 - core) * slim, slim), slim)
            arrived(wcat.at[l, other], wc_recv.at[l, q])
        line = gain[l : l + 1, :]

        def one(i, carry):
            part = pl.ds(pl.multiple_of(i * 16, 16), 16)
            wcat[l, part, :] = (wcat[l, part, :].astype(jnp.float32) * line).astype(jnp.bfloat16)
            return carry

        lax.fori_loop(0, 12 * slim // 16, one, 0)

    def project(l):
        acc[...] = jnp.zeros_like(acc)
        square[...] = jnp.zeros_like(square)
        for o in offs:
            tt = plane(o)
            count = (nx - 1) * half if o == (0, 0) else (2 * nx - 1) * half
            with scope(f"x{l}_{o[0]}_{o[1]}"):
                arrived(xg.at[l, tt, pl.ds(0, count)], fin_recv.at[l, tt])
            block = xg[l, tt]
            cols = pl.ds(pl.multiple_of(tt * width, width), width)
            acc[...] += dot_t(block, wcat[l, :, cols])
            values = block.astype(jnp.float32)
            values = values * values
            total = values[:, :128]
            for j in range(1, width // 128):
                total += values[:, j * 128 : (j + 1) * 128]
            square[...] += total
        factor = lax.rsqrt(jnp.sum(square[...], axis=1, keepdims=True) / feat + RMS_EPS)
        done = (acc[...] * factor).astype(jnp.bfloat16)
        for j in range(nx):
            pieces[l, j] = done[j * rows : (j + 1) * rows]
        sent = []
        for i, o in enumerate(xs):
            copy = remote(pieces.at[l, o], vg.at[l, x], ex_send.at[l, i], ex_recv.at[l, x], t, 2 * o + core)
            copy.start()
            sent.append(copy)
        vg[l, x] = pieces[l, x]
        return sent

    part = slim // 2
    up, down, across = xpeer(1), xpeer(-1), xpeer(2)

    def out_piece(l, xx, cc, piece):
        start, count = (0, slim) if piece is None else (piece * part, part)
        return wot.at[l, worow(2 * xx + cc, start, count)]

    def out_send(l, sent, n, xx, piece, to_x, to_core):
        block = out_piece(l, xx, core, piece)
        copy = remote(block, block, wo_send.at[l, n], wo_recv.at[l, n], t, 2 * to_x + to_core)
        copy.start()
        sent.append(copy)

    def out_arrived(l, n, xx, piece, cc=None):
        arrived(out_piece(l, xx, core if cc is None else cc, piece), wo_recv.at[l, n])

    def out_first(l):
        own_o[l].wait()
        sent = []
        out_send(l, sent, 0, x, 0, up, core)
        out_send(l, sent, 1, x, 1, down, core)
        out_send(l, sent, 6, x, None, x, 1 - core)
        return sent

    def out_second(l, sent):
        out_arrived(l, 0, down, 0)
        out_send(l, sent, 4, down, 0, up, core)
        out_send(l, sent, 7, down, 0, x, 1 - core)
        out_arrived(l, 1, up, 1)
        out_send(l, sent, 5, up, 1, down, core)
        out_send(l, sent, 8, up, 1, x, 1 - core)

    def out_third(l, sent):
        out_send(l, sent, 2, x, 1, up, core)
        out_send(l, sent, 3, x, 0, down, core)

    def out_fourth(l, sent):
        out_arrived(l, 2, down, 1)
        out_send(l, sent, 9, down, 1, x, 1 - core)
        out_arrived(l, 3, up, 0)
        out_send(l, sent, 10, up, 0, x, 1 - core)

    def out_fifth(l, sent):
        out_arrived(l, 4, across, 0)
        out_arrived(l, 5, across, 1)
        out_send(l, sent, 11, across, None, x, 1 - core)

    def out_finish(l):
        for n, xx, piece in ((6, x, None), (7, down, 0), (8, up, 1), (9, down, 1), (10, up, 0), (11, across, None)):
            out_arrived(l, n, xx, piece, 1 - core)

    size = 2 * slim
    sub = lax.broadcasted_iota(jnp.int32, (rows, rows), 0)
    lane = lax.broadcasted_iota(jnp.int32, (rows, rows), 1)
    spread = jnp.where(sub == lane, lens[...].astype(jnp.float32), 0.0)
    live = jnp.sum(spread, axis=1, keepdims=True) > STEP
    eight = lax.broadcasted_iota(jnp.int32, (8, 2 * size), 0)
    left = lax.broadcasted_iota(jnp.int32, (8, 2 * size), 1) < size
    left_half = lax.broadcasted_iota(jnp.int32, (half, 2 * size), 1) < size

    def paired(parts, p):
        return jnp.concatenate([parts[2 * p], parts[2 * p + 1]], axis=1)

    def by_head(values):
        one = jnp.sum(jnp.where(left_half, values, 0.0), axis=1, keepdims=True)
        two = jnp.sum(jnp.where(left_half, 0.0, values), axis=1, keepdims=True)
        return jnp.where(left_half, one, two) / size

    def recur(l):
        if l == 0:
            with scope("prepare1"):
                prepare(1)
                turn(1)
        else:
            with scope("update0"):
                update(0)
        with scope(f"exchange{l}"):
            for o in xs:
                arrived(vg.at[l, o], ex_recv.at[l, o])
        looks, extras, gates = [], [], []
        for h in range(nx):
            part = slice(h * size, (h + 1) * size)
            recept, key, value, decay_pre, rate_pre, gate_pre = [
                vg[l, h, :, q * size : (q + 1) * size].astype(jnp.float32) for q in range(6)
            ]
            decay = jnp.exp(-jnp.exp(-jax.nn.softplus(-(base[l : l + 1, part] + decay_pre)) - 0.5))
            learn = jax.nn.sigmoid(rate[l : l + 1, part] + rate_pre)
            length = jnp.maximum(jnp.sqrt(jnp.sum(key * key, axis=1, keepdims=True)), 1e-12)
            blend = jnp.sum(key * learn * recept, axis=1, keepdims=True)
            unit = key / length
            held = value * length
            rows_ref[l, 0, h] = jnp.where(live, -unit, 0.0)
            rows_ref[l, 1, h] = jnp.where(live, held, 0.0)
            rows_ref[l, 2, h] = jnp.where(live, decay, 1.0)
            rows_ref[l, 3, h] = unit * learn
            looks.append(decay * recept - (blend / length) * unit)
            extras.append(blend * value)
            gates.append(jax.nn.sigmoid(gate_pre) * ggain[l : l + 1, part])
        gates = [paired(gates, p) for p in range(nx // 2)]
        extras = [paired(extras, p) for p in range(nx // 2)]
        sent = []
        for g in range(2):
            reads = [[] for p in range(nx // 2)]
            for k in range(half // 8):
                low = g * half + k * 8
                look = jnp.concatenate([v[low : low + 8] for v in looks], axis=0).astype(jnp.bfloat16)
                sums = [extras[p][low : low + 8] for p in range(nx // 2)]
                for b in range(8):
                    got = jnp.dot(look, turned[l, low + b], preferred_element_type=jnp.float32)
                    for h in range(nx):
                        p = h // 2
                        side = left if h % 2 == 0 else jnp.logical_not(left)
                        piece = got[h * 8 : (h + 1) * 8, p * 128 : (p + 1) * 128]
                        sums[p] += jnp.where((eight == b) & side, piece, 0.0)
                for p in range(nx // 2):
                    reads[p].append(sums[p])
            span = slice(g * half, (g + 1) * half)
            outs = []
            for p in range(nx // 2):
                read = jnp.concatenate(reads[p], axis=0)
                apart = read - by_head(read)
                normal = apart * lax.rsqrt(by_head(apart * apart) + GROUP_EPS) * gates[p][span]
                outs.append(jnp.where(live[span], normal, 0.0).astype(jnp.bfloat16))
            span = pl.ds(g * half, half)
            mg[l, t, span, :] = jnp.concatenate(outs, axis=1)
            block = mg.at[l, t, span]
            for i, p in enumerate(far):
                copy = remote(block, block, mg_send.at[l, g * (tp - 1) + i], mg_recv.at[l, t], p, d)
                copy.start()
                sent.append(copy)
        return sent

    eye = lax.broadcasted_iota(jnp.int32, (size, size), 0) == lax.broadcasted_iota(jnp.int32, (size, size), 1)

    def update(l):
        def one(i, carry):
            for k in range(4):
                b = i * 4 + k
                for h in range(nx):
                    neg, held, decay, rated = [rows_ref[l, q, h, pl.ds(b, 1), :] for q in range(4)]
                    old = st[l, b, h]
                    weight = jnp.sum(old * neg + jnp.where(eye, held, 0.0), axis=1, keepdims=True)
                    st[l, b, h] = old * decay + weight * rated
            return carry

        lax.fori_loop(0, rows // 4, one, 0)

    def fold(l):
        total = jnp.zeros((rows, width), jnp.float32)
        for o in offs:
            tt = plane(o)
            if o != (0, 0):
                with scope(f"m{l}_{o[0]}_{o[1]}"):
                    arrived(mg.at[l, tt], mg_recv.at[l, tt])
            cols = pl.ds(pl.multiple_of(tt * width, width), width)
            total += dot_t(mg[l, tt], wot[l, :, cols])
        return total.astype(jnp.bfloat16)

    for l in range(2):
        with scope(f"start{l}"):
            if l == 1:
                xg[1, t, mine, :] = current
            sent, send = gather_start(l, lambda h: xg.at[l, t, own_rows(h, x)])
            if l == 0:
                shared = []
                for ll in range(2):
                    for q in range(6):
                        copy = remote(
                            weights[q].at[ll], wcat.at[ll, wrow(q)],
                            wc_send.at[ll, q], wc_recv.at[ll, q], t, sibling,
                        )
                        copy.start()
                        shared.append(copy)
            if l == 0:
                folded = [out_first(0)]
            else:
                out_second(1, folded[1])
        if l == 0:
            with scope("turn0"):
                turn(0)
        gather_relay(l, send)
        if l == 0:
            with scope("prepare0"):
                prepare(0)
        with scope(f"project{l}"):
            traded = project(l)
            out_third(l, folded[l])
            if l == 0:
                out_second(0, folded[0])
            for copy in sent:
                copy.wait_send()
        with scope(f"recur{l}"):
            mixed = recur(l)
        with scope(f"outfourth{l}"):
            out_fourth(l, folded[l])
            if l == 0:
                folded.append(out_first(1))
        with scope(f"outfifth{l}"):
            out_fifth(l, folded[l])
        if l == 1:
            with scope("update1"):
                update(1)
        with scope(f"outfinish{l}"):
            out_finish(l)
        with scope(f"fold{l}"):
            current = fold(l)
        for copy in traded + folded[l] + mixed:
            copy.wait_send()
    mixed_ref[...] = current
    for copy in shared:
        copy.wait_send()


def step(tok, lens, gain, base, rate, ggain, weights, wo, state, tp, dp):
    rows, width = tok.shape
    slim = width // dp
    nx = dp // 2
    feat = tp * width
    bf = jnp.bfloat16
    vmem, hbm = pl.BlockSpec(memory_space=pltpu.VMEM), pl.BlockSpec(memory_space=pltpu.HBM)
    dma = pltpu.SemaphoreType.DMA
    half = rows // 2
    return pl.pallas_call(
        functools.partial(step_body, tp=tp, dp=dp),
        out_shape=(
            pltpu.VMEM((rows, width), bf),
            pltpu.VMEM(state.shape, state.dtype),
        ),
        in_specs=[hbm] * 14,
        out_specs=(vmem, vmem),
        scratch_shapes=[
            pltpu.VMEM((2, tp, nx * rows, width), bf),
            pltpu.VMEM((2, 12 * slim, feat), bf),
            pltpu.VMEM((2, width, feat), bf),
            pltpu.VMEM((2, nx, rows, 12 * slim), bf),
            pltpu.VMEM((2, tp, rows, width), bf),
            pltpu.VMEM((2, nx, rows, 12 * slim), bf),
            pltpu.VMEM((2, rows, 2 * slim, nx * 2 * slim), bf),
            pltpu.VMEM((2, 4, nx, rows, 2 * slim), jnp.float32),
            pltpu.VMEM((nx * rows, 12 * slim), jnp.float32),
            pltpu.VMEM((nx * rows, 128), jnp.float32),
            pltpu.VMEM(lens.shape, lens.dtype),
            pltpu.VMEM(gain.shape, gain.dtype),
            pltpu.VMEM(base.shape, base.dtype),
            pltpu.VMEM(rate.shape, rate.dtype),
            pltpu.VMEM(ggain.shape, ggain.dtype),
            dma(((nx - 1) * (tp + 1) + (tp - 1) * (nx + 1),)),
            dma((2, nx)),
            dma((2, tp)),
            dma((2, tp)),
            dma((2, nx)),
            dma((2, nx)),
            dma((2, 2 * tp)),
            dma((2, tp)),
            dma((2, 12)),
            dma((2, 12)),
            dma((2, 6)),
            dma((2, 6)),
            dma((2, 7)),
            dma((2,)),
            dma((6,)),
        ],
        compiler_params=pltpu.CompilerParams(
            collective_id=0, has_side_effects=True, vmem_limit_bytes=VMEM_LIMIT
        ),
        name="step",
    )(tok, lens, gain, base, rate, ggain, *weights, wo, state)


def put_body(mixed_ref, state_ref, out_ref, new_ref, sem):
    count = state_ref.shape[0] * 4
    part = state_ref.shape[1] // 4
    copies = [pltpu.make_async_copy(mixed_ref, out_ref, sem.at[count])]
    for i in range(count):
        span = pl.ds(i % 4 * part, part)
        copies.append(
            pltpu.make_async_copy(state_ref.at[i // 4, span], new_ref.at[i // 4, span], sem.at[i])
        )
    for copy in copies:
        copy.start()
    for copy in copies:
        copy.wait()


def put(mixed, state):
    vmem, hbm = pl.BlockSpec(memory_space=pltpu.VMEM), pl.BlockSpec(memory_space=pltpu.HBM)
    return pl.pallas_call(
        put_body,
        out_shape=(
            jax.ShapeDtypeStruct(mixed.shape, mixed.dtype),
            jax.ShapeDtypeStruct(state.shape, state.dtype),
        ),
        in_specs=[vmem, vmem],
        out_specs=(hbm, hbm),
        scratch_shapes=[pltpu.SemaphoreType.DMA((state.shape[0] * 4 + 1,))],
        compiler_params=pltpu.CompilerParams(vmem_limit_bytes=4 * 1024 * 1024),
        name="put",
    )(mixed, state)


def on_device(
    tokens,
    lengths,
    norm_gain,
    w_recept,
    w_key,
    w_value,
    w_decay,
    w_rate,
    w_gate,
    w_out,
    decay_base,
    rate_base,
    group_gain,
    state,
):
    tp, dp = lax.axis_size("tp"), lax.axis_size("dp")
    weights = [w.transpose(0, 2, 1) for w in (w_recept, w_key, w_value, w_decay, w_rate, w_gate)]
    mixed, states = step(
        tokens, lengths.reshape(1, -1), norm_gain, decay_base, rate_base, group_gain,
        weights, w_out.transpose(0, 2, 1), state, tp, dp,
    )
    return put(mixed, states)


def solution(mesh):
    columns = P(None, None, ("tp", "dp"))
    in_specs = (
        (P("dp", "tp"), P("dp"), P())
        + (columns,) * 7
        + (P(None, "tp"),) * 3
        + (P(None, "dp", "tp", None, None),)
    )
    out_specs = (P("dp", "tp"), P(None, "dp", "tp", None, None))
    return jax.shard_map(
        on_device, mesh=mesh, in_specs=in_specs, out_specs=out_specs, check_vma=False
    )
```

```python
import contextlib
import functools

import jax
import jax.numpy as jnp
from jax import lax
from jax.experimental import pallas as pl
from jax.experimental.pallas import tpu as pltpu
from jax.sharding import PartitionSpec as P

STEP = 16
RMS_EPS = 1e-06
GROUP_EPS = 0.00064
VMEM_LIMIT = 55_000_000
MESH = pl.DeviceIdType.MESH


def scope(name):
    return contextlib.nullcontext()


def dot_t(a, b):
    return lax.dot_general(a, b, (((1,), (1,)), ((), ())), preferred_element_type=jnp.float32)


def plane_offsets(tp):
    ny = 4 if tp == 16 else tp
    nz = tp // ny
    hops = lambda k, n: min(k, n - k)
    offs = [(dz, dy) for dz in range(nz) for dy in range(ny)]
    offs.sort(key=lambda o: (hops(o[0], nz) + hops(o[1], ny), o))
    return ny, nz, offs


def step_body(
    tok, lens_hbm, gain_hbm, base_hbm, rate_hbm, ggain_hbm, wr, wk, wv, wd, wa, wg, wo, state,
    mixed_ref, st,
    xg, wcat, wot, vg, mg, pieces, turned, rows_ref, acc, square,
    lens, gain, base, rate, ggain,
    ag_send, a1_recv, b1_recv, fin_recv, ex_send, ex_recv, mg_send, mg_recv,
    wo_send, wo_recv, wc_send, wc_recv, own_sem, st_sem, small_sem,
    *, tp, dp,
):
    t, d = lax.axis_index("tp"), lax.axis_index("dp")
    nx = dp // 2
    x, core = d // 2, lax.rem(d, 2)
    sibling = d + 1 - 2 * core
    ny, nz, offs = plane_offsets(tp)
    z, y = t // ny, lax.rem(t, ny)
    rows, width = tok.shape
    slim = width // dp
    feat = tp * width
    half = rows // 2
    weights = (wr, wk, wv, wd, wa, wg)

    def plane(off):
        return lax.rem(z + off[0], nz) * ny + lax.rem(y + off[1], ny)

    def xpeer(k):
        return lax.rem(x + k + nx, nx)

    def remote(src, dst, ssem, rsem, tt, dd):
        return pltpu.make_async_remote_copy(
            src_ref=src, dst_ref=dst, send_sem=ssem, recv_sem=rsem,
            device_id=(tt, dd), device_id_type=MESH,
        )

    def arrived(ref, sem):
        remote(ref, ref, ag_send.at[0], sem, t, sibling).wait_recv()

    def fetched(ref, sem):
        pltpu.make_async_copy(ref, ref, sem).wait()

    peers = [plane(o) for o in offs[1:]]
    far = peers[::-1]
    ks = [1, nx - 1] + list(range(2, nx - 1))
    xs = [xpeer(k) for k in ks]


    def fetch(src, dst, sem):
        copy = pltpu.make_async_copy(src, dst, sem)
        copy.start()
        return copy

    def wrow(q):
        return pl.ds(pl.multiple_of(q * 2 * slim + core * slim, slim), slim)

    def worow(dd, start=0, count=None):
        return pl.ds(pl.multiple_of(dd * slim + start, slim // 2), slim if count is None else count)

    def slot(tt, xx, h, count=half):
        start = tt * (nx * rows) + xx * rows + h * half
        return pl.ds(pl.multiple_of(start, half), count)

    own_tok = fetch(tok, xg.at[0, slot(t, x, 0, rows)], small_sem.at[5])
    barrier = pltpu.get_barrier_semaphore()
    everyone = [(p, d) for p in far] + [(t, 2 * o + core) for o in xs] + [(t, sibling)]
    for p in everyone:
        pl.semaphore_signal(barrier, inc=1, device_id=p, device_id_type=MESH)
    small = [
        fetch(src, dst, small_sem.at[i])
        for i, (src, dst) in enumerate(
            [(lens_hbm, lens), (gain_hbm, gain), (base_hbm, base), (rate_hbm, rate), (ggain_hbm, ggain)]
        )
    ]
    own_s = [fetch(state.at[0], st.at[0], st_sem.at[0])]
    for l in range(2):
        for q in range(6):
            fetch(weights[q].at[l], wcat.at[l, wrow(q)], own_sem.at[l])
    own_o = [fetch(wo.at[l], wot.at[l, worow(d)], own_sem.at[2 + l]) for l in range(2)]
    own_s.append(fetch(state.at[1], st.at[1], st_sem.at[1]))


    def turn(l):
        own_s[l].wait()

        def one(i, carry):
            for k in range(4):
                for p in range(nx // 2):
                    both = jnp.concatenate([st[l, i * 4 + k, 2 * p], st[l, i * 4 + k, 2 * p + 1]], axis=0)
                    turned[l, i * 4 + k, :, p * 128 : (p + 1) * 128] = both.T.astype(jnp.bfloat16)
            return carry

        lax.fori_loop(0, rows // 4, one, 0)

    with scope("barrier"):
        pl.semaphore_wait(barrier, len(everyone))
    with scope("small"):
        for copy in small:
            copy.wait()
        own_tok.wait()

    def gather_start(l):
        def send(block, rsem, tt, dd):
            remote(block, block, ag_send.at[0], rsem, tt, dd).start()

        first, second = xg.at[l, slot(t, x, 0)], xg.at[l, slot(t, x, 1)]
        for o in xs:
            send(first, a1_recv.at[x], t, 2 * o + core)
        for p in far:
            send(second, b1_recv.at[t], p, d)
        for p in far:
            send(first, fin_recv.at[t], p, d)
        for o in xs:
            send(second, fin_recv.at[t], t, 2 * o + core)
        return send

    def gather_relay(l, send):
        steps = [("b", peers[0]), ("a", xs[0])]
        steps += [("b", peers[1]), ("a", xs[1])]
        steps += [("b", p) for p in peers[2:4]] + [("a", o) for o in xs[2:]]
        steps += [("b", p) for p in peers[4:]]
        for i, (kind, o) in enumerate(steps):
            with scope(f"{kind}{l}_{i}"):
                if kind == "a":
                    block = xg.at[l, slot(t, o, 0)]
                    arrived(block, a1_recv.at[o])
                    for p in far:
                        send(block, fin_recv.at[t], p, d)
                else:
                    block = xg.at[l, slot(o, x, 1)]
                    arrived(block, b1_recv.at[o])
                    for p in xs:
                        send(block, fin_recv.at[o], t, 2 * p + core)

    def sent_all(ref, sem):
        remote(ref, ref, sem, ex_recv.at[0], t, sibling).wait_send()

    def prepare(l):
        fetched(wcat.at[l, pl.ds(0, 6 * slim)], own_sem.at[l])
        arrived(wcat.at[l, pl.ds(0, 6 * slim)], wc_recv.at[l])
        line = gain[l : l + 1, :]

        def one(i, carry):
            part = pl.ds(pl.multiple_of(i * 16, 16), 16)
            wcat[l, part, :] = (wcat[l, part, :].astype(jnp.float32) * line).astype(jnp.bfloat16)
            return carry

        lax.fori_loop(0, 12 * slim // 16, one, 0)

    def project(l, after):
        acc[...] = jnp.zeros_like(acc)
        square[...] = jnp.zeros_like(square)
        for i, o in enumerate(offs):
            tt = plane(o)
            count = (nx - 1) * half if o == (0, 0) else (2 * nx - 1) * half
            with scope(f"x{l}_{o[0]}_{o[1]}"):
                arrived(xg.at[l, pl.ds(0, count)], fin_recv.at[tt])
            if i == 3:
                after()
            block = xg[l, slot(tt, 0, 0, nx * rows), :]
            cols = pl.ds(pl.multiple_of(tt * width, width), width)
            acc[...] += dot_t(block, wcat[l, :, cols])
            values = block.astype(jnp.float32)
            values = values * values
            total = values[:, :128]
            for j in range(1, width // 128):
                total += values[:, j * 128 : (j + 1) * 128]
            square[...] += total
        factor = lax.rsqrt(jnp.sum(square[...], axis=1, keepdims=True) / feat + RMS_EPS)
        done = (acc[...] * factor).astype(jnp.bfloat16)
        for j in range(nx):
            pieces[l, j] = done[j * rows : (j + 1) * rows]
        for o in xs:
            remote(pieces.at[l, o], vg.at[l, x], ex_send.at[0], ex_recv.at[x], t, 2 * o + core).start()
        vg[l, x] = pieces[l, x]

    part = slim // 2
    up, down, across = xpeer(1), xpeer(-1), xpeer(2)

    def out_piece(l, xx, cc, piece):
        start, count = (0, slim) if piece is None else (piece * part, part)
        return wot.at[l, worow(2 * xx + cc, start, count)]

    def out_send(l, n, xx, piece, to_x, to_core):
        block = out_piece(l, xx, core, piece)
        remote(block, block, wo_send.at[l], wo_recv.at[l, n], t, 2 * to_x + to_core).start()

    def out_arrived(l, n, xx, piece):
        arrived(out_piece(l, xx, core, piece), wo_recv.at[l, n])

    def out_first(l):
        own_o[l].wait()
        out_send(l, 0, x, 0, up, core)
        out_send(l, 1, x, 1, down, core)
        out_send(l, 6, x, None, x, 1 - core)

    def out_second(l):
        out_arrived(l, 0, down, 0)
        out_send(l, 4, down, 0, up, core)
        out_send(l, 6, down, 0, x, 1 - core)
        out_arrived(l, 1, up, 1)
        out_send(l, 5, up, 1, down, core)
        out_send(l, 6, up, 1, x, 1 - core)

    def out_third(l):
        out_send(l, 2, x, 1, up, core)
        out_send(l, 3, x, 0, down, core)

    def out_fourth(l):
        out_arrived(l, 2, down, 1)
        out_send(l, 6, down, 1, x, 1 - core)
        out_arrived(l, 3, up, 0)
        out_send(l, 6, up, 0, x, 1 - core)

    def out_fifth(l):
        out_arrived(l, 4, across, 0)
        out_arrived(l, 5, across, 1)
        out_send(l, 6, across, None, x, 1 - core)

    def out_finish(l):
        arrived(wot.at[l, pl.ds(0, nx * slim)], wo_recv.at[l, 6])

    size = 2 * slim
    sub = lax.broadcasted_iota(jnp.int32, (rows, rows), 0)
    lane = lax.broadcasted_iota(jnp.int32, (rows, rows), 1)
    spread = jnp.where(sub == lane, lens[...].astype(jnp.float32), 0.0)
    live = jnp.sum(spread, axis=1, keepdims=True) > STEP
    eight = lax.broadcasted_iota(jnp.int32, (8, 2 * size), 0)
    left = lax.broadcasted_iota(jnp.int32, (8, 2 * size), 1) < size
    left_half = lax.broadcasted_iota(jnp.int32, (half, 2 * size), 1) < size

    def paired(parts, p):
        return jnp.concatenate([parts[2 * p], parts[2 * p + 1]], axis=1)

    def by_head(values):
        one = jnp.sum(jnp.where(left_half, values, 0.0), axis=1, keepdims=True)
        two = jnp.sum(jnp.where(left_half, 0.0, values), axis=1, keepdims=True)
        return jnp.where(left_half, one, two) / size

    def recur(l):
        if l == 0:
            with scope("prepare1"):
                prepare(1)
                turn(1)
        else:
            with scope("update0"):
                update(0)
        with scope(f"exchange{l}"):
            for o in xs:
                arrived(vg.at[l, o], ex_recv.at[o])
        looks, extras, gates = [], [], []
        for h in range(nx):
            part = slice(h * size, (h + 1) * size)
            recept, key, value, decay_pre, rate_pre, gate_pre = [
                vg[l, h, :, q * size : (q + 1) * size].astype(jnp.float32) for q in range(6)
            ]
            decay = jnp.exp(-jnp.exp(-jax.nn.softplus(-(base[l : l + 1, part] + decay_pre)) - 0.5))
            learn = jax.nn.sigmoid(rate[l : l + 1, part] + rate_pre)
            length = jnp.maximum(jnp.sqrt(jnp.sum(key * key, axis=1, keepdims=True)), 1e-12)
            blend = jnp.sum(key * learn * recept, axis=1, keepdims=True)
            unit = key / length
            held = value * length
            rows_ref[l, 0, h] = jnp.where(live, -unit, 0.0)
            rows_ref[l, 1, h] = jnp.where(live, held, 0.0)
            rows_ref[l, 2, h] = jnp.where(live, decay, 1.0)
            rows_ref[l, 3, h] = unit * learn
            looks.append(decay * recept - (blend / length) * unit)
            extras.append(blend * value)
            gates.append(jax.nn.sigmoid(gate_pre) * ggain[l : l + 1, part])
        gates = [paired(gates, p) for p in range(nx // 2)]
        extras = [paired(extras, p) for p in range(nx // 2)]
        for g in range(2):
            reads = [[] for p in range(nx // 2)]
            for k in range(half // 8):
                low = g * half + k * 8
                look = jnp.concatenate([v[low : low + 8] for v in looks], axis=0).astype(jnp.bfloat16)
                sums = [extras[p][low : low + 8] for p in range(nx // 2)]
                for b in range(8):
                    got = jnp.dot(look, turned[l, low + b], preferred_element_type=jnp.float32)
                    for h in range(nx):
                        p = h // 2
                        side = left if h % 2 == 0 else jnp.logical_not(left)
                        piece = got[h * 8 : (h + 1) * 8, p * 128 : (p + 1) * 128]
                        sums[p] += jnp.where((eight == b) & side, piece, 0.0)
                for p in range(nx // 2):
                    reads[p].append(sums[p])
            span = slice(g * half, (g + 1) * half)
            outs = []
            for p in range(nx // 2):
                read = jnp.concatenate(reads[p], axis=0)
                apart = read - by_head(read)
                normal = apart * lax.rsqrt(by_head(apart * apart) + GROUP_EPS) * gates[p][span]
                outs.append(jnp.where(live[span], normal, 0.0).astype(jnp.bfloat16))
            span = pl.ds(pl.multiple_of(t * rows + g * half, half), half)
            mg[l, span, :] = jnp.concatenate(outs, axis=1)
            block = mg.at[l, span]
            for p in far:
                remote(block, block, mg_send.at[0], mg_recv.at[t], p, d).start()

    eye = lax.broadcasted_iota(jnp.int32, (size, size), 0) == lax.broadcasted_iota(jnp.int32, (size, size), 1)

    def update(l):
        def one(i, carry):
            for k in range(4):
                b = i * 4 + k
                for h in range(nx):
                    neg, held, decay, rated = [rows_ref[l, q, h, pl.ds(b, 1), :] for q in range(4)]
                    old = st[l, b, h]
                    weight = jnp.sum(old * neg + jnp.where(eye, held, 0.0), axis=1, keepdims=True)
                    st[l, b, h] = old * decay + weight * rated
            return carry

        lax.fori_loop(0, rows // 4, one, 0)

    def fold(l):
        total = jnp.zeros((rows, width), jnp.float32)
        for o in offs:
            tt = plane(o)
            span = pl.ds(pl.multiple_of(tt * rows, rows), rows)
            if o != (0, 0):
                with scope(f"m{l}_{o[0]}_{o[1]}"):
                    arrived(mg.at[l, span], mg_recv.at[tt])
            cols = pl.ds(pl.multiple_of(tt * width, width), width)
            total += dot_t(mg[l, span, :], wot[l, :, cols])
        return total.astype(jnp.bfloat16)

    for l in range(2):
        with scope(f"start{l}"):
            if l == 1:
                xg[1, slot(t, x, 0, rows), :] = current
            send = gather_start(l)
            if l == 0:
                for ll in range(2):
                    for q in range(6):
                        remote(
                            weights[q].at[ll], wcat.at[ll, wrow(q)], wc_send.at[0], wc_recv.at[ll], t, sibling
                        ).start()
                out_first(0)
            else:
                out_second(1)
        if l == 0:
            with scope("turn0"):
                turn(0)
        gather_relay(l, send)
        if l == 0:
            with scope("prepare0"):
                prepare(0)
        with scope(f"project{l}"):
            project(l, lambda: out_second(0) if l == 0 else None)
            out_third(l)
            sent_all(xg.at[l, pl.ds(0, ((nx - 1) * (tp + 1) + (tp - 1) * (nx + 1)) * half)], ag_send.at[0])
        with scope(f"recur{l}"):
            recur(l)
        with scope(f"outfourth{l}"):
            out_fourth(l)
            if l == 0:
                out_first(1)
            out_fifth(l)
        if l == 1:
            with scope("update1"):
                update(1)
        with scope(f"outfinish{l}"):
            out_finish(l)
        with scope(f"fold{l}"):
            current = fold(l)
        sent_all(pieces.at[l, pl.ds(0, nx - 1)], ex_send.at[0])
        sent_all(mg.at[l, pl.ds(0, (tp - 1) * rows)], mg_send.at[0])
        sent_all(wot.at[l, pl.ds(0, 7 * slim)], wo_send.at[l])
    mixed_ref[...] = current
    sent_all(wcat.at[0], wc_send.at[0])


def step(tok, lens, gain, base, rate, ggain, weights, wo, state, tp, dp):
    rows, width = tok.shape
    slim = width // dp
    nx = dp // 2
    feat = tp * width
    bf = jnp.bfloat16
    vmem, hbm = pl.BlockSpec(memory_space=pltpu.VMEM), pl.BlockSpec(memory_space=pltpu.HBM)
    dma = pltpu.SemaphoreType.DMA
    half = rows // 2
    return pl.pallas_call(
        functools.partial(step_body, tp=tp, dp=dp),
        out_shape=(
            pltpu.VMEM((rows, width), bf),
            pltpu.VMEM(state.shape, state.dtype),
        ),
        in_specs=[hbm] * 14,
        out_specs=(vmem, vmem),
        scratch_shapes=[
            pltpu.VMEM((2, tp * nx * rows, width), bf),
            pltpu.VMEM((2, 12 * slim, feat), bf),
            pltpu.VMEM((2, width, feat), bf),
            pltpu.VMEM((2, nx, rows, 12 * slim), bf),
            pltpu.VMEM((2, tp * rows, width), bf),
            pltpu.VMEM((2, nx, rows, 12 * slim), bf),
            pltpu.VMEM((2, rows, 2 * slim, nx * 2 * slim), bf),
            pltpu.VMEM((2, 4, nx, rows, 2 * slim), jnp.float32),
            pltpu.VMEM((nx * rows, 12 * slim), jnp.float32),
            pltpu.VMEM((nx * rows, 128), jnp.float32),
            pltpu.VMEM(lens.shape, lens.dtype),
            pltpu.VMEM(gain.shape, gain.dtype),
            pltpu.VMEM(base.shape, base.dtype),
            pltpu.VMEM(rate.shape, rate.dtype),
            pltpu.VMEM(ggain.shape, ggain.dtype),
            dma((1,)),
            dma((nx,)),
            dma((tp,)),
            dma((tp,)),
            dma((1,)),
            dma((nx,)),
            dma((1,)),
            dma((tp,)),
            dma((2,)),
            dma((2, 7)),
            dma((1,)),
            dma((2,)),
            dma((4,)),
            dma((2,)),
            dma((6,)),
        ],
        compiler_params=pltpu.CompilerParams(
            collective_id=0, has_side_effects=True, vmem_limit_bytes=VMEM_LIMIT
        ),
        name="step",
    )(tok, lens, gain, base, rate, ggain, *weights, wo, state)


def put_body(mixed_ref, state_ref, out_ref, new_ref, sem):
    count = state_ref.shape[0] * 4
    part = state_ref.shape[1] // 4
    copies = [pltpu.make_async_copy(mixed_ref, out_ref, sem.at[count])]
    for i in range(count):
        span = pl.ds(i % 4 * part, part)
        copies.append(
            pltpu.make_async_copy(state_ref.at[i // 4, span], new_ref.at[i // 4, span], sem.at[i])
        )
    for copy in copies:
        copy.start()
    for copy in copies:
        copy.wait()


def put(mixed, state):
    vmem, hbm = pl.BlockSpec(memory_space=pltpu.VMEM), pl.BlockSpec(memory_space=pltpu.HBM)
    return pl.pallas_call(
        put_body,
        out_shape=(
            jax.ShapeDtypeStruct(mixed.shape, mixed.dtype),
            jax.ShapeDtypeStruct(state.shape, state.dtype),
        ),
        in_specs=[vmem, vmem],
        out_specs=(hbm, hbm),
        scratch_shapes=[pltpu.SemaphoreType.DMA((state.shape[0] * 4 + 1,))],
        compiler_params=pltpu.CompilerParams(vmem_limit_bytes=4 * 1024 * 1024),
        name="put",
    )(mixed, state)


def on_device(
    tokens,
    lengths,
    norm_gain,
    w_recept,
    w_key,
    w_value,
    w_decay,
    w_rate,
    w_gate,
    w_out,
    decay_base,
    rate_base,
    group_gain,
    state,
):
    tp, dp = lax.axis_size("tp"), lax.axis_size("dp")
    weights = [w.transpose(0, 2, 1) for w in (w_recept, w_key, w_value, w_decay, w_rate, w_gate)]
    mixed, states = step(
        tokens, lengths.reshape(1, -1), norm_gain, decay_base, rate_base, group_gain,
        weights, w_out.transpose(0, 2, 1), state, tp, dp,
    )
    return put(mixed, states)


def solution(mesh):
    columns = P(None, None, ("tp", "dp"))
    in_specs = (
        (P("dp", "tp"), P("dp"), P())
        + (columns,) * 7
        + (P(None, "tp"),) * 3
        + (P(None, "dp", "tp", None, None),)
    )
    out_specs = (P("dp", "tp"), P(None, "dp", "tp", None, None))
    return jax.shard_map(
        on_device, mesh=mesh, in_specs=in_specs, out_specs=out_specs, check_vma=False
    )
```

```python
import contextlib
import functools

import jax
import jax.numpy as jnp
from jax import lax
from jax.experimental import pallas as pl
from jax.experimental.pallas import tpu as pltpu
from jax.sharding import PartitionSpec as P

STEP = 16
RMS_EPS = 1e-06
GROUP_EPS = 0.00064
VMEM_LIMIT = 55_000_000
MESH = pl.DeviceIdType.MESH


def scope(name):
    return contextlib.nullcontext()


def dot_t(a, b):
    return lax.dot_general(a, b, (((1,), (1,)), ((), ())), preferred_element_type=jnp.float32)


def plane_offsets(tp):
    ny = 4 if tp == 16 else tp
    nz = tp // ny
    hops = lambda k, n: min(k, n - k)
    offs = [(dz, dy) for dz in range(nz) for dy in range(ny)]
    offs.sort(key=lambda o: (hops(o[0], nz) + hops(o[1], ny), o))
    return ny, nz, offs


def step_body(
    tok, lens_hbm, gain_hbm, base_hbm, rate_hbm, ggain_hbm, wr, wk, wv, wd, wa, wg, wo, state,
    mixed_ref, st,
    xg, wcat, wot, vg, mg, pieces, turned, rows_ref, acc, square,
    lens, gain, base, rate, ggain,
    ag_send, a1_recv, b1_recv, fin_recv, ex_send, ex_recv, mg_send, mg_recv,
    wo_send, wo_recv, wc_send, wc_recv, own_sem, st_sem, small_sem,
    *, tp, dp,
):
    t, d = lax.axis_index("tp"), lax.axis_index("dp")
    nx = dp // 2
    x, core = d // 2, lax.rem(d, 2)
    sibling = d + 1 - 2 * core
    ny, nz, offs = plane_offsets(tp)
    z, y = t // ny, lax.rem(t, ny)
    rows, width = tok.shape
    slim = width // dp
    feat = tp * width
    half = rows // 2
    weights = (wr, wk, wv, wd, wa, wg)

    def plane(off):
        return lax.rem(z + off[0], nz) * ny + lax.rem(y + off[1], ny)

    def xpeer(k):
        return lax.rem(x + k + nx, nx)

    def remote(src, dst, ssem, rsem, tt, dd):
        return pltpu.make_async_remote_copy(
            src_ref=src, dst_ref=dst, send_sem=ssem, recv_sem=rsem,
            device_id=(tt, dd), device_id_type=MESH,
        )

    def arrived(ref, sem):
        remote(ref, ref, ag_send.at[0], sem, t, sibling).wait_recv()

    def fetched(ref, sem):
        pltpu.make_async_copy(ref, ref, sem).wait()

    peers = [plane(o) for o in offs[1:]]
    far = peers[::-1]
    ks = [1, nx - 1] + list(range(2, nx - 1))
    xs = [xpeer(k) for k in ks]


    def fetch(src, dst, sem):
        copy = pltpu.make_async_copy(src, dst, sem)
        copy.start()
        return copy

    def wrow(q):
        return pl.ds(pl.multiple_of(q * 2 * slim + core * slim, slim), slim)

    def slot(tt, xx, h, count=half):
        start = tt * (nx * rows) + xx * rows + h * half
        return pl.ds(pl.multiple_of(start, half), count)

    own_tok = fetch(tok, xg.at[0, slot(t, x, 0, rows)], small_sem.at[5])
    barrier = pltpu.get_barrier_semaphore()
    everyone = [(p, d) for p in far] + [(t, 2 * o + core) for o in xs] + [(t, sibling)]
    for p in everyone:
        pl.semaphore_signal(barrier, inc=1, device_id=p, device_id_type=MESH)
    own_tok.wait()
    small = [
        fetch(src, dst, small_sem.at[i])
        for i, (src, dst) in enumerate(
            [(lens_hbm, lens), (gain_hbm, gain), (base_hbm, base), (rate_hbm, rate), (ggain_hbm, ggain)]
        )
    ]
    own_s = [fetch(state.at[0], st.at[0], st_sem.at[0])]
    for l in range(2):
        for q in range(6):
            fetch(weights[q].at[l], wcat.at[l, wrow(q)], own_sem.at[l])
    own_o = [
        fetch(wo.at[l], wot.at[pl.ds(pl.multiple_of(l * width + d * slim, slim), slim)], own_sem.at[2 + l])
        for l in range(2)
    ]
    own_s.append(fetch(state.at[1], st.at[1], st_sem.at[1]))


    def turn(l):
        own_s[l].wait()

        def one(i, carry):
            for k in range(4):
                for p in range(nx // 2):
                    both = jnp.concatenate([st[l, i * 4 + k, 2 * p], st[l, i * 4 + k, 2 * p + 1]], axis=0)
                    turned[l, i * 4 + k, :, p * 128 : (p + 1) * 128] = both.T.astype(jnp.bfloat16)
            return carry

        lax.fori_loop(0, rows // 4, one, 0)

    with scope("barrier"):
        pl.semaphore_wait(barrier, len(everyone))

    def gather_start(l):
        def send(block, rsem, tt, dd):
            remote(block, block, ag_send.at[0], rsem, tt, dd).start()

        first, second = xg.at[l, slot(t, x, 0)], xg.at[l, slot(t, x, 1)]
        for o in xs:
            send(first, a1_recv.at[x], t, 2 * o + core)
        for p in far:
            send(second, b1_recv.at[t], p, d)
        for p in far:
            send(first, fin_recv.at[t], p, d)
        for o in xs:
            send(second, fin_recv.at[t], t, 2 * o + core)
        return send

    def gather_relay(l, send):
        steps = [("a", o) for o in xs[:2]] + [("b", p) for p in peers[:4]]
        steps += [("a", o) for o in xs[2:]] + [("b", p) for p in peers[4:]]
        for i, (kind, o) in enumerate(steps):
            if l == 0 and i == 4:
                out_first(0)
            with scope(f"{kind}{l}_{i}"):
                if kind == "a":
                    block = xg.at[l, slot(t, o, 0)]
                    arrived(block, a1_recv.at[o])
                    for p in far:
                        send(block, fin_recv.at[t], p, d)
                else:
                    block = xg.at[l, slot(o, x, 1)]
                    arrived(block, b1_recv.at[o])
                    for p in xs:
                        send(block, fin_recv.at[o], t, 2 * p + core)

    def sent_all(ref, sem):
        remote(ref, ref, sem, ex_recv.at[0], t, sibling).wait_send()

    def prepare(l):
        fetched(wcat.at[l, pl.ds(0, 6 * slim)], own_sem.at[l])
        arrived(wcat.at[l, pl.ds(0, 6 * slim)], wc_recv.at[l])
        line = gain[l : l + 1, :]

        def one(i, carry):
            part = pl.ds(pl.multiple_of(i * 16, 16), 16)
            wcat[l, part, :] = (wcat[l, part, :].astype(jnp.float32) * line).astype(jnp.bfloat16)
            return carry

        lax.fori_loop(0, 12 * slim // 16, one, 0)

    def project(l, after):
        acc[...] = jnp.zeros_like(acc)
        square[...] = jnp.zeros_like(square)
        for i, o in enumerate(offs[:1] + offs[:0:-1]):
            tt = plane(o)
            count = (nx - 1) * half if o == (0, 0) else (2 * nx - 1) * half
            with scope(f"x{l}_{o[0]}_{o[1]}"):
                arrived(xg.at[l, pl.ds(0, count)], fin_recv.at[tt])
            if i == 3:
                after()
            block = xg[l, slot(tt, 0, 0, nx * rows), :]
            cols = pl.ds(pl.multiple_of(tt * width, width), width)
            acc[...] += dot_t(block, wcat[l, :, cols])
            values = block.astype(jnp.float32)
            values = values * values
            total = values[:, :128]
            for j in range(1, width // 128):
                total += values[:, j * 128 : (j + 1) * 128]
            square[...] += total
        factor = lax.rsqrt(jnp.sum(square[...], axis=1, keepdims=True) / feat + RMS_EPS)
        done = (acc[...] * factor).astype(jnp.bfloat16)
        for j in range(nx):
            pieces[l, j] = done[j * rows : (j + 1) * rows]
        for o in xs:
            remote(pieces.at[l, o], vg.at[l, x], ex_send.at[0], ex_recv.at[x], t, 2 * o + core).start()
        vg[l, x] = pieces[l, x]

    up, down, across = xpeer(1), xpeer(-1), xpeer(2)

    def block_of(l, xx, cc):
        return wot.at[pl.ds(pl.multiple_of(l * width + (2 * xx + cc) * slim, slim), slim)]

    def out_send(l, n, xx, cc, to_x, to_core):
        block = block_of(l, xx, cc)
        remote(block, block, wo_send.at[l], wo_recv.at[l, n], t, 2 * to_x + to_core).start()

    def out_arrived(l, n, count=1):
        arrived(wot.at[pl.ds(0, count * slim)], wo_recv.at[l, n])

    def ring(body):
        pl.when(core == 1)(body)

    def out_first(l):
        own_o[l].wait()

        @ring
        def _():
            out_arrived(l, 6)
            out_send(l, 0, x, 0, up, 1)
            out_send(l, 1, x, 1, down, 1)

    def out_second(l):
        @ring
        def _():
            out_arrived(l, 0)
            out_send(l, 4, down, 0, up, 1)
            out_send(l, 6, down, 0, x, 0)
            out_arrived(l, 1)
            out_send(l, 5, up, 1, down, 1)
            out_send(l, 6, up, 1, x, 0)

    def out_third(l):
        @ring
        def _():
            out_send(l, 2, x, 1, up, 1)
            out_send(l, 3, x, 0, down, 1)

    def out_fourth(l):
        @ring
        def _():
            out_arrived(l, 4)
            out_send(l, 6, across, 0, x, 0)
            out_arrived(l, 5)
            out_send(l, 6, across, 1, x, 0)
            out_arrived(l, 2)
            out_send(l, 6, down, 1, x, 0)
            out_arrived(l, 3)
            out_send(l, 6, up, 0, x, 0)

    def out_finish(l):
        @pl.when(core == 0)
        def _():
            out_arrived(l, 6, 2 * nx - 1)

    def out_done(l):
        @ring
        def _():
            sent_all(wot.at[pl.ds(0, 13 * slim)], wo_send.at[l])

        @pl.when(core == 0)
        def _():
            sent_all(wot.at[pl.ds(0, slim)], wo_send.at[l])

    size = 2 * slim
    eight = lax.broadcasted_iota(jnp.int32, (8, 2 * size), 0)
    left = lax.broadcasted_iota(jnp.int32, (8, 2 * size), 1) < size
    left_half = lax.broadcasted_iota(jnp.int32, (half, 2 * size), 1) < size

    def paired(parts, p):
        return jnp.concatenate([parts[2 * p], parts[2 * p + 1]], axis=1)

    def by_head(values):
        one = jnp.sum(jnp.where(left_half, values, 0.0), axis=1, keepdims=True)
        two = jnp.sum(jnp.where(left_half, 0.0, values), axis=1, keepdims=True)
        return jnp.where(left_half, one, two) / size

    def recur(l):
        if l == 0:
            with scope("prepare1"):
                prepare(1)
                turn(1)
        else:
            with scope("update0"):
                update(0)
        with scope(f"exchange{l}"):
            for o in xs:
                arrived(vg.at[l, o], ex_recv.at[o])
        sub = lax.broadcasted_iota(jnp.int32, (rows, rows), 0)
        lane = lax.broadcasted_iota(jnp.int32, (rows, rows), 1)
        spread = jnp.where(sub == lane, lens[...].astype(jnp.float32), 0.0)
        live = jnp.sum(spread, axis=1, keepdims=True) > STEP
        looks, extras, gates = [], [], []
        for h in range(nx):
            part = slice(h * size, (h + 1) * size)
            recept, key, value, decay_pre, rate_pre, gate_pre = [
                vg[l, h, :, q * size : (q + 1) * size].astype(jnp.float32) for q in range(6)
            ]
            decay = jnp.exp(-jnp.exp(-jax.nn.softplus(-(base[l : l + 1, part] + decay_pre)) - 0.5))
            learn = jax.nn.sigmoid(rate[l : l + 1, part] + rate_pre)
            length = jnp.maximum(jnp.sqrt(jnp.sum(key * key, axis=1, keepdims=True)), 1e-12)
            blend = jnp.sum(key * learn * recept, axis=1, keepdims=True)
            unit = key / length
            held = value * length
            rows_ref[l, 0, h] = jnp.where(live, -unit, 0.0)
            rows_ref[l, 1, h] = jnp.where(live, held, 0.0)
            rows_ref[l, 2, h] = jnp.where(live, decay, 1.0)
            rows_ref[l, 3, h] = unit * learn
            looks.append(decay * recept - (blend / length) * unit)
            extras.append(blend * value)
            gates.append(jax.nn.sigmoid(gate_pre) * ggain[l : l + 1, part])
        gates = [paired(gates, p) for p in range(nx // 2)]
        extras = [paired(extras, p) for p in range(nx // 2)]
        for g in range(2):
            reads = [[] for p in range(nx // 2)]
            for k in range(half // 8):
                low = g * half + k * 8
                look = jnp.concatenate([v[low : low + 8] for v in looks], axis=0).astype(jnp.bfloat16)
                sums = [extras[p][low : low + 8] for p in range(nx // 2)]
                for b in range(8):
                    got = jnp.dot(look, turned[l, low + b], preferred_element_type=jnp.float32)
                    for h in range(nx):
                        p = h // 2
                        side = left if h % 2 == 0 else jnp.logical_not(left)
                        piece = got[h * 8 : (h + 1) * 8, p * 128 : (p + 1) * 128]
                        sums[p] += jnp.where((eight == b) & side, piece, 0.0)
                for p in range(nx // 2):
                    reads[p].append(sums[p])
            span = slice(g * half, (g + 1) * half)
            outs = []
            for p in range(nx // 2):
                read = jnp.concatenate(reads[p], axis=0)
                apart = read - by_head(read)
                normal = apart * lax.rsqrt(by_head(apart * apart) + GROUP_EPS) * gates[p][span]
                outs.append(jnp.where(live[span], normal, 0.0).astype(jnp.bfloat16))
            span = pl.ds(pl.multiple_of(t * rows + g * half, half), half)
            mg[l, span, :] = jnp.concatenate(outs, axis=1)
            block = mg.at[l, span]
            for p in far:
                remote(block, block, mg_send.at[0], mg_recv.at[t], p, d).start()

    eye = lax.broadcasted_iota(jnp.int32, (size, size), 0) == lax.broadcasted_iota(jnp.int32, (size, size), 1)

    def update(l):
        def one(i, carry):
            for k in range(4):
                b = i * 4 + k
                for h in range(nx):
                    neg, held, decay, rated = [rows_ref[l, q, h, pl.ds(b, 1), :] for q in range(4)]
                    old = st[l, b, h]
                    weight = jnp.sum(old * neg + jnp.where(eye, held, 0.0), axis=1, keepdims=True)
                    st[l, b, h] = old * decay + weight * rated
            return carry

        lax.fori_loop(0, rows // 4, one, 0)

    def fold(l):
        total = jnp.zeros((rows, width), jnp.float32)
        for o in offs[:1] + offs[:0:-1]:
            tt = plane(o)
            span = pl.ds(pl.multiple_of(tt * rows, rows), rows)
            if o != (0, 0):
                with scope(f"m{l}_{o[0]}_{o[1]}"):
                    arrived(mg.at[l, span], mg_recv.at[tt])
            cols = pl.ds(pl.multiple_of(tt * width, width), width)
            total += dot_t(mg[l, span, :], wot[pl.ds(l * width, width), cols])
        return total.astype(jnp.bfloat16)

    for l in range(2):
        with scope(f"start{l}"):
            if l == 1:
                xg[1, slot(t, x, 0, rows), :] = current
            send = gather_start(l)
            if l == 0:
                for ll in range(2):
                    remote(
                        wo.at[ll],
                        wot.at[pl.ds(pl.multiple_of(ll * width + d * slim, slim), slim)],
                        wo_send.at[ll], wo_recv.at[ll, 6], t, sibling,
                    ).start()
                    for q in range(6):
                        remote(
                            weights[q].at[ll], wcat.at[ll, wrow(q)], wc_send.at[0], wc_recv.at[ll], t, sibling
                        ).start()
            else:
                out_second(1)
        if l == 0:
            with scope("turn0"):
                turn(0)
        gather_relay(l, send)
        if l == 0:
            with scope("prepare0"):
                for copy in small:
                    copy.wait()
                prepare(0)
        with scope(f"project{l}"):
            project(l, lambda: out_second(0) if l == 0 else None)
            out_third(l)
            sent_all(xg.at[l, pl.ds(0, ((nx - 1) * (tp + 1) + (tp - 1) * (nx + 1)) * half)], ag_send.at[0])
        with scope(f"recur{l}"):
            recur(l)
        with scope(f"outfourth{l}"):
            out_fourth(l)
            if l == 0:
                out_first(1)
        if l == 1:
            with scope("update1"):
                update(1)
        with scope(f"outfinish{l}"):
            out_finish(l)
        with scope(f"fold{l}"):
            current = fold(l)
        sent_all(pieces.at[l, pl.ds(0, nx - 1)], ex_send.at[0])
        sent_all(mg.at[l, pl.ds(0, (tp - 1) * rows)], mg_send.at[0])
        out_done(l)
    mixed_ref[...] = current
    sent_all(wcat.at[0], wc_send.at[0])


def step(tok, lens, gain, base, rate, ggain, weights, wo, state, tp, dp):
    rows, width = tok.shape
    slim = width // dp
    nx = dp // 2
    feat = tp * width
    bf = jnp.bfloat16
    vmem, hbm = pl.BlockSpec(memory_space=pltpu.VMEM), pl.BlockSpec(memory_space=pltpu.HBM)
    dma = pltpu.SemaphoreType.DMA
    half = rows // 2
    return pl.pallas_call(
        functools.partial(step_body, tp=tp, dp=dp),
        out_shape=(
            pltpu.VMEM((rows, width), bf),
            pltpu.VMEM(state.shape, state.dtype),
        ),
        in_specs=[hbm] * 14,
        out_specs=(vmem, vmem),
        scratch_shapes=[
            pltpu.VMEM((2, tp * nx * rows, width), bf),
            pltpu.VMEM((2, 12 * slim, feat), bf),
            pltpu.VMEM((2 * width, feat), bf),
            pltpu.VMEM((2, nx, rows, 12 * slim), bf),
            pltpu.VMEM((2, tp * rows, width), bf),
            pltpu.VMEM((2, nx, rows, 12 * slim), bf),
            pltpu.VMEM((2, rows, 2 * slim, nx * 2 * slim), bf),
            pltpu.VMEM((2, 4, nx, rows, 2 * slim), jnp.float32),
            pltpu.VMEM((nx * rows, 12 * slim), jnp.float32),
            pltpu.VMEM((nx * rows, 128), jnp.float32),
            pltpu.VMEM(lens.shape, lens.dtype),
            pltpu.VMEM(gain.shape, gain.dtype),
            pltpu.VMEM(base.shape, base.dtype),
            pltpu.VMEM(rate.shape, rate.dtype),
            pltpu.VMEM(ggain.shape, ggain.dtype),
            dma((1,)),
            dma((nx,)),
            dma((tp,)),
            dma((tp,)),
            dma((1,)),
            dma((nx,)),
            dma((1,)),
            dma((tp,)),
            dma((2,)),
            dma((2, 7)),
            dma((1,)),
            dma((2,)),
            dma((4,)),
            dma((2,)),
            dma((6,)),
        ],
        compiler_params=pltpu.CompilerParams(
            collective_id=0, has_side_effects=True, vmem_limit_bytes=VMEM_LIMIT
        ),
        name="step",
    )(tok, lens, gain, base, rate, ggain, *weights, wo, state)


def put_body(mixed_ref, state_ref, out_ref, new_ref, sem):
    count = state_ref.shape[0] * 4
    part = state_ref.shape[1] // 4
    copies = [pltpu.make_async_copy(mixed_ref, out_ref, sem.at[count])]
    for i in range(count):
        span = pl.ds(i % 4 * part, part)
        copies.append(
            pltpu.make_async_copy(state_ref.at[i // 4, span], new_ref.at[i // 4, span], sem.at[i])
        )
    for copy in copies:
        copy.start()
    for copy in copies:
        copy.wait()


def put(mixed, state):
    vmem, hbm = pl.BlockSpec(memory_space=pltpu.VMEM), pl.BlockSpec(memory_space=pltpu.HBM)
    return pl.pallas_call(
        put_body,
        out_shape=(
            jax.ShapeDtypeStruct(mixed.shape, mixed.dtype),
            jax.ShapeDtypeStruct(state.shape, state.dtype),
        ),
        in_specs=[vmem, vmem],
        out_specs=(hbm, hbm),
        scratch_shapes=[pltpu.SemaphoreType.DMA((state.shape[0] * 4 + 1,))],
        compiler_params=pltpu.CompilerParams(vmem_limit_bytes=4 * 1024 * 1024),
        name="put",
    )(mixed, state)


def on_device(
    tokens,
    lengths,
    norm_gain,
    w_recept,
    w_key,
    w_value,
    w_decay,
    w_rate,
    w_gate,
    w_out,
    decay_base,
    rate_base,
    group_gain,
    state,
):
    tp, dp = lax.axis_size("tp"), lax.axis_size("dp")
    weights = [w.transpose(0, 2, 1) for w in (w_recept, w_key, w_value, w_decay, w_rate, w_gate)]
    mixed, states = step(
        tokens, lengths.reshape(1, -1), norm_gain, decay_base, rate_base, group_gain,
        weights, w_out.transpose(0, 2, 1), state, tp, dp,
    )
    return put(mixed, states)


def solution(mesh):
    columns = P(None, None, ("tp", "dp"))
    in_specs = (
        (P("dp", "tp"), P("dp"), P())
        + (columns,) * 7
        + (P(None, "tp"),) * 3
        + (P(None, "dp", "tp", None, None),)
    )
    out_specs = (P("dp", "tp"), P(None, "dp", "tp", None, None))
    return jax.shard_map(
        on_device, mesh=mesh, in_specs=in_specs, out_specs=out_specs, check_vma=False
    )
```

```python
import contextlib
import functools

import jax
import jax.numpy as jnp
from jax import lax
from jax.experimental import pallas as pl
from jax.experimental.pallas import tpu as pltpu
from jax.sharding import PartitionSpec as P

STEP = 16
RMS_EPS = 1e-06
GROUP_EPS = 0.00064
VMEM_LIMIT = 55_000_000
MESH = pl.DeviceIdType.MESH


def scope(name):
    return contextlib.nullcontext()


def dot_t(a, b):
    return lax.dot_general(a, b, (((1,), (1,)), ((), ())), preferred_element_type=jnp.float32)


def plane_offsets(tp):
    ny = 4 if tp == 16 else tp
    nz = tp // ny
    hops = lambda k, n: min(k, n - k)
    offs = [(dz, dy) for dz in range(nz) for dy in range(ny)]
    offs.sort(key=lambda o: (hops(o[0], nz) + hops(o[1], ny), o))
    return ny, nz, offs


def step_body(
    tok, lens_hbm, gain_hbm, base_hbm, rate_hbm, ggain_hbm, wr, wk, wv, wd, wa, wg, wo, state,
    mixed_ref, st,
    xg, wcat, wot, vg, mg, pieces, turned, rows_ref, acc, square,
    lens, gain, base, rate, ggain,
    ag_send, a1_recv, b1_recv, fin_recv, ex_send, ex_recv, mg_send, mg_recv,
    wo_send, wo_recv, wc_send, wc_recv, own_sem, st_sem, small_sem,
    *, tp, dp,
):
    t, d = lax.axis_index("tp"), lax.axis_index("dp")
    nx = dp // 2
    x, core = d // 2, lax.rem(d, 2)
    sibling = d + 1 - 2 * core
    ny, nz, offs = plane_offsets(tp)
    z, y = t // ny, lax.rem(t, ny)
    rows, width = tok.shape
    slim = width // dp
    feat = tp * width
    half = rows // 2
    weights = (wr, wk, wv, wd, wa, wg)

    def plane(off):
        return lax.rem(z + off[0], nz) * ny + lax.rem(y + off[1], ny)

    def xpeer(k):
        return lax.rem(x + k + nx, nx)

    def remote(src, dst, ssem, rsem, tt, dd):
        return pltpu.make_async_remote_copy(
            src_ref=src, dst_ref=dst, send_sem=ssem, recv_sem=rsem,
            device_id=(tt, dd), device_id_type=MESH,
        )

    def arrived(ref, sem):
        remote(ref, ref, ag_send.at[0], sem, t, sibling).wait_recv()

    def fetched(ref, sem):
        pltpu.make_async_copy(ref, ref, sem).wait()

    peers = [plane(o) for o in offs[1:]]
    far = peers[::-1]
    ks = [1, nx - 1] + list(range(2, nx - 1))
    xs = [xpeer(k) for k in ks]


    def fetch(src, dst, sem):
        copy = pltpu.make_async_copy(src, dst, sem)
        copy.start()
        return copy

    def wrow(q):
        return pl.ds(pl.multiple_of(q * 2 * slim + core * slim, slim), slim)

    def worow(dd, start=0, count=None):
        return pl.ds(pl.multiple_of(dd * slim + start, slim // 2), slim if count is None else count)

    def slot(tt, xx, h, count=half):
        start = tt * (nx * rows) + xx * rows + h * half
        return pl.ds(pl.multiple_of(start, half), count)

    own_tok = fetch(tok, xg.at[0, slot(t, x, 0, rows)], small_sem.at[5])
    barrier = pltpu.get_barrier_semaphore()
    everyone = [(p, d) for p in far] + [(t, 2 * o + core) for o in xs] + [(t, sibling)]
    for p in everyone:
        pl.semaphore_signal(barrier, inc=1, device_id=p, device_id_type=MESH)
    small = [
        fetch(src, dst, small_sem.at[i])
        for i, (src, dst) in enumerate(
            [(lens_hbm, lens), (gain_hbm, gain), (base_hbm, base), (rate_hbm, rate), (ggain_hbm, ggain)]
        )
    ]
    own_s = [fetch(state.at[0], st.at[0], st_sem.at[0])]
    for l in range(2):
        for q in range(6):
            fetch(weights[q].at[l], wcat.at[l, wrow(q)], own_sem.at[l])
    own_o = [fetch(wo.at[l], wot.at[l, worow(d)], own_sem.at[2 + l]) for l in range(2)]
    own_s.append(fetch(state.at[1], st.at[1], st_sem.at[1]))


    def turn(l):
        own_s[l].wait()

        def one(i, carry):
            for k in range(4):
                for p in range(nx // 2):
                    both = jnp.concatenate([st[l, i * 4 + k, 2 * p], st[l, i * 4 + k, 2 * p + 1]], axis=0)
                    turned[l, i * 4 + k, :, p * 128 : (p + 1) * 128] = both.T.astype(jnp.bfloat16)
            return carry

        lax.fori_loop(0, rows // 4, one, 0)

    with scope("barrier"):
        pl.semaphore_wait(barrier, len(everyone))
    with scope("small"):
        own_tok.wait()

    def gather_start(l):
        def send(block, rsem, tt, dd):
            remote(block, block, ag_send.at[0], rsem, tt, dd).start()

        first, second = xg.at[l, slot(t, x, 0)], xg.at[l, slot(t, x, 1)]
        for o in xs:
            send(first, a1_recv.at[x], t, 2 * o + core)
        for p in far:
            send(second, b1_recv.at[t], p, d)
        for p in far:
            send(first, fin_recv.at[t], p, d)
        for o in xs:
            send(second, fin_recv.at[t], t, 2 * o + core)
        return send

    def gather_relay(l, send):
        steps = [("b", peers[0]), ("a", xs[0])]
        steps += [("b", peers[1]), ("a", xs[1])]
        steps += [("b", p) for p in peers[2:4]] + [("a", o) for o in xs[2:]]
        steps += [("b", p) for p in peers[4:]]
        for i, (kind, o) in enumerate(steps):
            with scope(f"{kind}{l}_{i}"):
                if kind == "a":
                    block = xg.at[l, slot(t, o, 0)]
                    arrived(block, a1_recv.at[o])
                    for p in far:
                        send(block, fin_recv.at[t], p, d)
                else:
                    block = xg.at[l, slot(o, x, 1)]
                    arrived(block, b1_recv.at[o])
                    for p in xs:
                        send(block, fin_recv.at[o], t, 2 * p + core)

    def sent_all(ref, sem):
        remote(ref, ref, sem, ex_recv.at[0], t, sibling).wait_send()

    def prepare(l):
        fetched(wcat.at[l, pl.ds(0, 6 * slim)], own_sem.at[l])
        arrived(wcat.at[l, pl.ds(0, 6 * slim)], wc_recv.at[l])
        line = gain[l : l + 1, :]

        def one(i, carry):
            part = pl.ds(pl.multiple_of(i * 16, 16), 16)
            wcat[l, part, :] = (wcat[l, part, :].astype(jnp.float32) * line).astype(jnp.bfloat16)
            return carry

        lax.fori_loop(0, 12 * slim // 16, one, 0)

    def project(l, after):
        acc[...] = jnp.zeros_like(acc)
        square[...] = jnp.zeros_like(square)
        for i, o in enumerate(offs):
            tt = plane(o)
            count = (nx - 1) * half if o == (0, 0) else (2 * nx - 1) * half
            with scope(f"x{l}_{o[0]}_{o[1]}"):
                arrived(xg.at[l, pl.ds(0, count)], fin_recv.at[tt])
            if i == 3:
                after()
            block = xg[l, slot(tt, 0, 0, nx * rows), :]
            cols = pl.ds(pl.multiple_of(tt * width, width), width)
            acc[...] += dot_t(block, wcat[l, :, cols])
            values = block.astype(jnp.float32)
            values = values * values
            total = values[:, :128]
            for j in range(1, width // 128):
                total += values[:, j * 128 : (j + 1) * 128]
            square[...] += total
        factor = lax.rsqrt(jnp.sum(square[...], axis=1, keepdims=True) / feat + RMS_EPS)
        done = (acc[...] * factor).astype(jnp.bfloat16)
        for j in range(nx):
            pieces[l, j] = done[j * rows : (j + 1) * rows]
        for o in xs:
            remote(pieces.at[l, o], vg.at[l, x], ex_send.at[0], ex_recv.at[x], t, 2 * o + core).start()
        vg[l, x] = pieces[l, x]

    part = slim // 2
    up, down, across = xpeer(1), xpeer(-1), xpeer(2)

    def out_piece(l, xx, cc, piece):
        start, count = (0, slim) if piece is None else (piece * part, part)
        return wot.at[l, worow(2 * xx + cc, start, count)]

    def out_send(l, n, xx, piece, to_x, to_core):
        block = out_piece(l, xx, core, piece)
        remote(block, block, wo_send.at[l], wo_recv.at[l, n], t, 2 * to_x + to_core).start()

    def out_arrived(l, n, xx, piece):
        arrived(out_piece(l, xx, core, piece), wo_recv.at[l, n])

    def out_first(l):
        own_o[l].wait()
        out_send(l, 0, x, 0, up, core)
        out_send(l, 1, x, 1, down, core)
        out_send(l, 6, x, None, x, 1 - core)

    def out_second(l):
        out_arrived(l, 0, down, 0)
        out_send(l, 4, down, 0, up, core)
        out_send(l, 6, down, 0, x, 1 - core)
        out_arrived(l, 1, up, 1)
        out_send(l, 5, up, 1, down, core)
        out_send(l, 6, up, 1, x, 1 - core)

    def out_third(l):
        out_send(l, 2, x, 1, up, core)
        out_send(l, 3, x, 0, down, core)

    def out_fourth(l):
        out_arrived(l, 2, down, 1)
        out_send(l, 6, down, 1, x, 1 - core)
        out_arrived(l, 3, up, 0)
        out_send(l, 6, up, 0, x, 1 - core)

    def out_fifth(l):
        out_arrived(l, 4, across, 0)
        out_arrived(l, 5, across, 1)
        out_send(l, 6, across, None, x, 1 - core)

    def out_finish(l):
        arrived(wot.at[l, pl.ds(0, nx * slim)], wo_recv.at[l, 6])

    size = 2 * slim
    eight = lax.broadcasted_iota(jnp.int32, (8, 2 * size), 0)
    left = lax.broadcasted_iota(jnp.int32, (8, 2 * size), 1) < size
    left_half = lax.broadcasted_iota(jnp.int32, (half, 2 * size), 1) < size

    def paired(parts, p):
        return jnp.concatenate([parts[2 * p], parts[2 * p + 1]], axis=1)

    def by_head(values):
        one = jnp.sum(jnp.where(left_half, values, 0.0), axis=1, keepdims=True)
        two = jnp.sum(jnp.where(left_half, 0.0, values), axis=1, keepdims=True)
        return jnp.where(left_half, one, two) / size

    def recur(l):
        if l == 0:
            with scope("prepare1"):
                prepare(1)
                turn(1)
        else:
            with scope("update0"):
                update(0)
        with scope(f"exchange{l}"):
            for o in xs:
                arrived(vg.at[l, o], ex_recv.at[o])
        sub = lax.broadcasted_iota(jnp.int32, (rows, rows), 0)
        lane = lax.broadcasted_iota(jnp.int32, (rows, rows), 1)
        spread = jnp.where(sub == lane, lens[...].astype(jnp.float32), 0.0)
        live = jnp.sum(spread, axis=1, keepdims=True) > STEP
        looks, extras, gates = [], [], []
        for h in range(nx):
            part = slice(h * size, (h + 1) * size)
            recept, key, value, decay_pre, rate_pre, gate_pre = [
                vg[l, h, :, q * size : (q + 1) * size].astype(jnp.float32) for q in range(6)
            ]
            decay = jnp.exp(-jnp.exp(-jax.nn.softplus(-(base[l : l + 1, part] + decay_pre)) - 0.5))
            learn = jax.nn.sigmoid(rate[l : l + 1, part] + rate_pre)
            length = jnp.maximum(jnp.sqrt(jnp.sum(key * key, axis=1, keepdims=True)), 1e-12)
            blend = jnp.sum(key * learn * recept, axis=1, keepdims=True)
            unit = key / length
            held = value * length
            rows_ref[l, 0, h] = jnp.where(live, -unit, 0.0)
            rows_ref[l, 1, h] = jnp.where(live, held, 0.0)
            rows_ref[l, 2, h] = jnp.where(live, decay, 1.0)
            rows_ref[l, 3, h] = unit * learn
            looks.append(decay * recept - (blend / length) * unit)
            extras.append(blend * value)
            gates.append(jax.nn.sigmoid(gate_pre) * ggain[l : l + 1, part])
        gates = [paired(gates, p) for p in range(nx // 2)]
        extras = [paired(extras, p) for p in range(nx // 2)]
        for g in range(2):
            reads = [[] for p in range(nx // 2)]
            for k in range(half // 8):
                low = g * half + k * 8
                look = jnp.concatenate([v[low : low + 8] for v in looks], axis=0).astype(jnp.bfloat16)
                sums = [extras[p][low : low + 8] for p in range(nx // 2)]
                for b in range(8):
                    got = jnp.dot(look, turned[l, low + b], preferred_element_type=jnp.float32)
                    for h in range(nx):
                        p = h // 2
                        side = left if h % 2 == 0 else jnp.logical_not(left)
                        piece = got[h * 8 : (h + 1) * 8, p * 128 : (p + 1) * 128]
                        sums[p] += jnp.where((eight == b) & side, piece, 0.0)
                for p in range(nx // 2):
                    reads[p].append(sums[p])
            span = slice(g * half, (g + 1) * half)
            outs = []
            for p in range(nx // 2):
                read = jnp.concatenate(reads[p], axis=0)
                apart = read - by_head(read)
                normal = apart * lax.rsqrt(by_head(apart * apart) + GROUP_EPS) * gates[p][span]
                outs.append(jnp.where(live[span], normal, 0.0).astype(jnp.bfloat16))
            span = pl.ds(pl.multiple_of(t * rows + g * half, half), half)
            mg[l, span, :] = jnp.concatenate(outs, axis=1)
            block = mg.at[l, span]
            for p in far:
                remote(block, block, mg_send.at[0], mg_recv.at[t], p, d).start()

    eye = lax.broadcasted_iota(jnp.int32, (size, size), 0) == lax.broadcasted_iota(jnp.int32, (size, size), 1)

    def update(l):
        def one(i, carry):
            for k in range(4):
                b = i * 4 + k
                for h in range(nx):
                    neg, held, decay, rated = [rows_ref[l, q, h, pl.ds(b, 1), :] for q in range(4)]
                    old = st[l, b, h]
                    weight = jnp.sum(old * neg + jnp.where(eye, held, 0.0), axis=1, keepdims=True)
                    st[l, b, h] = old * decay + weight * rated
            return carry

        lax.fori_loop(0, rows // 4, one, 0)

    def fold(l):
        total = jnp.zeros((rows, width), jnp.float32)
        for o in offs:
            tt = plane(o)
            span = pl.ds(pl.multiple_of(tt * rows, rows), rows)
            if o != (0, 0):
                with scope(f"m{l}_{o[0]}_{o[1]}"):
                    arrived(mg.at[l, span], mg_recv.at[tt])
            cols = pl.ds(pl.multiple_of(tt * width, width), width)
            total += dot_t(mg[l, span, :], wot[l, :, cols])
        return total.astype(jnp.bfloat16)

    for l in range(2):
        with scope(f"start{l}"):
            if l == 1:
                xg[1, slot(t, x, 0, rows), :] = current
            send = gather_start(l)
            if l == 0:
                for ll in range(2):
                    for q in range(6):
                        remote(
                            weights[q].at[ll], wcat.at[ll, wrow(q)], wc_send.at[0], wc_recv.at[ll], t, sibling
                        ).start()
                out_first(0)
            else:
                out_second(1)
        if l == 0:
            with scope("turn0"):
                turn(0)
        gather_relay(l, send)
        if l == 0:
            with scope("prepare0"):
                for copy in small:
                    copy.wait()
                prepare(0)
        with scope(f"project{l}"):
            project(l, lambda: out_second(0) if l == 0 else None)
            out_third(l)
            sent_all(xg.at[l, pl.ds(0, ((nx - 1) * (tp + 1) + (tp - 1) * (nx + 1)) * half)], ag_send.at[0])
        with scope(f"recur{l}"):
            recur(l)
        with scope(f"outfourth{l}"):
            out_fourth(l)
            if l == 0:
                out_first(1)
            out_fifth(l)
        if l == 1:
            with scope("update1"):
                update(1)
        with scope(f"outfinish{l}"):
            out_finish(l)
        with scope(f"fold{l}"):
            current = fold(l)
        sent_all(pieces.at[l, pl.ds(0, nx - 1)], ex_send.at[0])
        sent_all(mg.at[l, pl.ds(0, (tp - 1) * rows)], mg_send.at[0])
        sent_all(wot.at[l, pl.ds(0, 7 * slim)], wo_send.at[l])
    mixed_ref[...] = current
    sent_all(wcat.at[0], wc_send.at[0])


def step(tok, lens, gain, base, rate, ggain, weights, wo, state, tp, dp):
    rows, width = tok.shape
    slim = width // dp
    nx = dp // 2
    feat = tp * width
    bf = jnp.bfloat16
    vmem, hbm = pl.BlockSpec(memory_space=pltpu.VMEM), pl.BlockSpec(memory_space=pltpu.HBM)
    dma = pltpu.SemaphoreType.DMA
    half = rows // 2
    return pl.pallas_call(
        functools.partial(step_body, tp=tp, dp=dp),
        out_shape=(
            pltpu.VMEM((rows, width), bf),
            pltpu.VMEM(state.shape, state.dtype),
        ),
        in_specs=[hbm] * 14,
        out_specs=(vmem, vmem),
        scratch_shapes=[
            pltpu.VMEM((2, tp * nx * rows, width), bf),
            pltpu.VMEM((2, 12 * slim, feat), bf),
            pltpu.VMEM((2, width, feat), bf),
            pltpu.VMEM((2, nx, rows, 12 * slim), bf),
            pltpu.VMEM((2, tp * rows, width), bf),
            pltpu.VMEM((2, nx, rows, 12 * slim), bf),
            pltpu.VMEM((2, rows, 2 * slim, nx * 2 * slim), bf),
            pltpu.VMEM((2, 4, nx, rows, 2 * slim), jnp.float32),
            pltpu.VMEM((nx * rows, 12 * slim), jnp.float32),
            pltpu.VMEM((nx * rows, 128), jnp.float32),
            pltpu.VMEM(lens.shape, lens.dtype),
            pltpu.VMEM(gain.shape, gain.dtype),
            pltpu.VMEM(base.shape, base.dtype),
            pltpu.VMEM(rate.shape, rate.dtype),
            pltpu.VMEM(ggain.shape, ggain.dtype),
            dma((1,)),
            dma((nx,)),
            dma((tp,)),
            dma((tp,)),
            dma((1,)),
            dma((nx,)),
            dma((1,)),
            dma((tp,)),
            dma((2,)),
            dma((2, 7)),
            dma((1,)),
            dma((2,)),
            dma((4,)),
            dma((2,)),
            dma((6,)),
        ],
        compiler_params=pltpu.CompilerParams(
            collective_id=0, has_side_effects=True, vmem_limit_bytes=VMEM_LIMIT
        ),
        name="step",
    )(tok, lens, gain, base, rate, ggain, *weights, wo, state)


def put_body(mixed_ref, state_ref, out_ref, new_ref, sem):
    count = state_ref.shape[0] * 4
    part = state_ref.shape[1] // 4
    copies = [pltpu.make_async_copy(mixed_ref, out_ref, sem.at[count])]
    for i in range(count):
        span = pl.ds(i % 4 * part, part)
        copies.append(
            pltpu.make_async_copy(state_ref.at[i // 4, span], new_ref.at[i // 4, span], sem.at[i])
        )
    for copy in copies:
        copy.start()
    for copy in copies:
        copy.wait()


def put(mixed, state):
    vmem, hbm = pl.BlockSpec(memory_space=pltpu.VMEM), pl.BlockSpec(memory_space=pltpu.HBM)
    return pl.pallas_call(
        put_body,
        out_shape=(
            jax.ShapeDtypeStruct(mixed.shape, mixed.dtype),
            jax.ShapeDtypeStruct(state.shape, state.dtype),
        ),
        in_specs=[vmem, vmem],
        out_specs=(hbm, hbm),
        scratch_shapes=[pltpu.SemaphoreType.DMA((state.shape[0] * 4 + 1,))],
        compiler_params=pltpu.CompilerParams(vmem_limit_bytes=4 * 1024 * 1024),
        name="put",
    )(mixed, state)


def on_device(
    tokens,
    lengths,
    norm_gain,
    w_recept,
    w_key,
    w_value,
    w_decay,
    w_rate,
    w_gate,
    w_out,
    decay_base,
    rate_base,
    group_gain,
    state,
):
    tp, dp = lax.axis_size("tp"), lax.axis_size("dp")
    weights = [w.transpose(0, 2, 1) for w in (w_recept, w_key, w_value, w_decay, w_rate, w_gate)]
    mixed, states = step(
        tokens, lengths.reshape(1, -1), norm_gain, decay_base, rate_base, group_gain,
        weights, w_out.transpose(0, 2, 1), state, tp, dp,
    )
    return put(mixed, states)


def solution(mesh):
    columns = P(None, None, ("tp", "dp"))
    in_specs = (
        (P("dp", "tp"), P("dp"), P())
        + (columns,) * 7
        + (P(None, "tp"),) * 3
        + (P(None, "dp", "tp", None, None),)
    )
    out_specs = (P("dp", "tp"), P(None, "dp", "tp", None, None))
    return jax.shard_map(
        on_device, mesh=mesh, in_specs=in_specs, out_specs=out_specs, check_vma=False
    )
```

```python
import contextlib
import functools

import jax
import jax.numpy as jnp
from jax import lax
from jax.experimental import pallas as pl
from jax.experimental.pallas import tpu as pltpu
from jax.sharding import PartitionSpec as P

STEP = 16
RMS_EPS = 1e-06
GROUP_EPS = 0.00064
VMEM_LIMIT = 55_000_000
MESH = pl.DeviceIdType.MESH
CUT = (16, 16)


def scope(name):
    return contextlib.nullcontext()


def dot_t(a, b):
    return lax.dot_general(a, b, (((1,), (1,)), ((), ())), preferred_element_type=jnp.float32)


def plane_offsets(tp):
    ny = 4 if tp == 16 else tp
    nz = tp // ny
    hops = lambda k, n: min(k, n - k)
    offs = [(dz, dy) for dz in range(nz) for dy in range(ny)]
    offs.sort(key=lambda o: (hops(o[0], nz) + hops(o[1], ny), o))
    return ny, nz, offs


def step_body(
    tok, lens_hbm, gain_hbm, base_hbm, rate_hbm, ggain_hbm, wr, wk, wv, wd, wa, wg, wo, state,
    mixed_ref, st,
    xg, wcat, wot, vg, mg, pieces, turned, rows_ref, acc, square,
    lens, gain, base, rate, ggain,
    ag_send, a1_recv, b1_recv, fin_recv, ex_send, ex_recv, mg_send, mg_recv,
    wo_send, wo_recv, wc_send, wc_recv, own_sem, st_sem, small_sem,
    *, tp, dp,
):
    t, d = lax.axis_index("tp"), lax.axis_index("dp")
    nx = dp // 2
    x, core = d // 2, lax.rem(d, 2)
    sibling = d + 1 - 2 * core
    ny, nz, offs = plane_offsets(tp)
    z, y = t // ny, lax.rem(t, ny)
    rows, width = tok.shape
    slim = width // dp
    feat = tp * width
    half = rows // 2
    weights = (wr, wk, wv, wd, wa, wg)

    def plane(off):
        return lax.rem(z + off[0], nz) * ny + lax.rem(y + off[1], ny)

    def xpeer(k):
        return lax.rem(x + k + nx, nx)

    def remote(src, dst, ssem, rsem, tt, dd):
        return pltpu.make_async_remote_copy(
            src_ref=src, dst_ref=dst, send_sem=ssem, recv_sem=rsem,
            device_id=(tt, dd), device_id_type=MESH,
        )

    def arrived(ref, sem):
        remote(ref, ref, ag_send.at[0], sem, t, sibling).wait_recv()

    def fetched(ref, sem):
        pltpu.make_async_copy(ref, ref, sem).wait()

    peers = [plane(o) for o in offs[1:]]
    far = peers
    ks = [1, nx - 1] + list(range(2, nx - 1))
    xs = [xpeer(k) for k in ks]
    outward = xs[::-1]


    def fetch(src, dst, sem):
        copy = pltpu.make_async_copy(src, dst, sem)
        copy.start()
        return copy

    def wrow(q):
        return pl.ds(pl.multiple_of(q * 2 * slim + core * slim, slim), slim)

    def worow(dd, start=0, count=None):
        return pl.ds(pl.multiple_of(dd * slim + start, slim // 2), slim if count is None else count)

    def slot(tt, xx, count):
        return pl.ds(pl.multiple_of(tt * (nx * rows) + xx * rows, rows), count)

    def share(l, tt, xx, h):
        start, count = (0, CUT[l]) if h == 0 else (CUT[l], rows - CUT[l])
        return pl.ds(pl.multiple_of(tt * (nx * rows) + xx * rows + start, 8), count)

    own_tok = fetch(tok, xg.at[0, slot(t, x, rows)], small_sem.at[5])
    barrier = pltpu.get_barrier_semaphore()
    everyone = [(p, d) for p in far] + [(t, 2 * o + core) for o in xs] + [(t, sibling)]
    for p in everyone:
        pl.semaphore_signal(barrier, inc=1, device_id=p, device_id_type=MESH)
    small = [
        fetch(src, dst, small_sem.at[i])
        for i, (src, dst) in enumerate(
            [(lens_hbm, lens), (gain_hbm, gain), (base_hbm, base), (rate_hbm, rate), (ggain_hbm, ggain)]
        )
    ]
    own_s = [fetch(state.at[0], st.at[0], st_sem.at[0])]
    for l in range(2):
        for q in range(6):
            fetch(weights[q].at[l], wcat.at[l, wrow(q)], own_sem.at[l])
    own_o = [fetch(wo.at[l], wot.at[l, worow(d)], own_sem.at[2 + l]) for l in range(2)]
    own_s.append(fetch(state.at[1], st.at[1], st_sem.at[1]))


    def turn(l):
        own_s[l].wait()

        def one(i, carry):
            for k in range(4):
                for p in range(nx // 2):
                    both = jnp.concatenate([st[l, i * 4 + k, 2 * p], st[l, i * 4 + k, 2 * p + 1]], axis=0)
                    turned[l, i * 4 + k, :, p * 128 : (p + 1) * 128] = both.T.astype(jnp.bfloat16)
            return carry

        lax.fori_loop(0, rows // 4, one, 0)

    with scope("barrier"):
        pl.semaphore_wait(barrier, len(everyone))
    with scope("small"):
        own_tok.wait()

    def gather_start(l):
        def send(block, rsem, tt, dd):
            remote(block, block, ag_send.at[0], rsem, tt, dd).start()

        first, second = xg.at[l, share(l, t, x, 0)], xg.at[l, share(l, t, x, 1)]
        for o in outward:
            send(first, a1_recv.at[x], t, 2 * o + core)
        for p in peers:
            send(second, b1_recv.at[t], p, d)
        for o in outward:
            send(second, fin_recv.at[t], t, 2 * o + core)
        for p in far:
            send(first, fin_recv.at[t], p, d)
        return send

    def gather_relay(l, send):
        steps = [("b", peers[0]), ("a", xs[0])]
        steps += [("b", peers[1]), ("a", xs[1])]
        steps += [("b", p) for p in peers[2:4]] + [("a", o) for o in xs[2:]]
        steps += [("b", p) for p in peers[4:]]
        for i, (kind, o) in enumerate(steps):
            with scope(f"{kind}{l}_{i}"):
                if kind == "a":
                    block = xg.at[l, share(l, t, o, 0)]
                    arrived(block, a1_recv.at[o])
                    for p in far:
                        send(block, fin_recv.at[t], p, d)
                else:
                    block = xg.at[l, share(l, o, x, 1)]
                    arrived(block, b1_recv.at[o])
                    for p in outward:
                        send(block, fin_recv.at[o], t, 2 * p + core)

    def sent_all(ref, sem):
        remote(ref, ref, sem, ex_recv.at[0], t, sibling).wait_send()

    def prepare(l):
        fetched(wcat.at[l, pl.ds(0, 6 * slim)], own_sem.at[l])
        arrived(wcat.at[l, pl.ds(0, 6 * slim)], wc_recv.at[l])
        line = gain[l : l + 1, :]

        def one(i, carry):
            part = pl.ds(pl.multiple_of(i * 16, 16), 16)
            wcat[l, part, :] = (wcat[l, part, :].astype(jnp.float32) * line).astype(jnp.bfloat16)
            return carry

        lax.fori_loop(0, 12 * slim // 16, one, 0)

    def project(l, after):
        acc[...] = jnp.zeros_like(acc)
        square[...] = jnp.zeros_like(square)
        for i, o in enumerate(offs):
            tt = plane(o)
            count = (nx - 1) * (rows - CUT[l]) + (0 if o == (0, 0) else nx * CUT[l])
            with scope(f"x{l}_{o[0]}_{o[1]}"):
                arrived(xg.at[l, pl.ds(0, count)], fin_recv.at[tt])
            if i == 3:
                after()
            block = xg[l, slot(tt, 0, nx * rows), :]
            cols = pl.ds(pl.multiple_of(tt * width, width), width)
            acc[...] += dot_t(block, wcat[l, :, cols])
            values = block.astype(jnp.float32)
            values = values * values
            total = values[:, :128]
            for j in range(1, width // 128):
                total += values[:, j * 128 : (j + 1) * 128]
            square[...] += total
        factor = lax.rsqrt(jnp.sum(square[...], axis=1, keepdims=True) / feat + RMS_EPS)
        done = (acc[...] * factor).astype(jnp.bfloat16)
        for j in range(nx):
            pieces[l, j] = done[j * rows : (j + 1) * rows]
        for o in outward:
            remote(pieces.at[l, o], vg.at[l, x], ex_send.at[0], ex_recv.at[x], t, 2 * o + core).start()
        vg[l, x] = pieces[l, x]

    part = slim // 2
    up, down, across = xpeer(1), xpeer(-1), xpeer(2)

    def out_piece(l, xx, cc, piece):
        start, count = (0, slim) if piece is None else (piece * part, part)
        return wot.at[l, worow(2 * xx + cc, start, count)]

    def out_send(l, n, xx, piece, to_x, to_core):
        block = out_piece(l, xx, core, piece)
        remote(block, block, wo_send.at[l], wo_recv.at[l, n], t, 2 * to_x + to_core).start()

    def out_arrived(l, n, xx, piece):
        arrived(out_piece(l, xx, core, piece), wo_recv.at[l, n])

    def out_first(l):
        own_o[l].wait()
        out_send(l, 0, x, 0, up, core)
        out_send(l, 1, x, 1, down, core)
        out_send(l, 6, x, None, x, 1 - core)

    def out_second(l):
        out_arrived(l, 0, down, 0)
        out_send(l, 4, down, 0, up, core)
        out_send(l, 6, down, 0, x, 1 - core)
        out_arrived(l, 1, up, 1)
        out_send(l, 5, up, 1, down, core)
        out_send(l, 6, up, 1, x, 1 - core)

    def out_third(l):
        out_send(l, 2, x, 1, up, core)
        out_send(l, 3, x, 0, down, core)

    def out_fourth(l):
        out_arrived(l, 2, down, 1)
        out_send(l, 6, down, 1, x, 1 - core)
        out_arrived(l, 3, up, 0)
        out_send(l, 6, up, 0, x, 1 - core)

    def out_fifth(l):
        out_arrived(l, 4, across, 0)
        out_arrived(l, 5, across, 1)
        out_send(l, 6, across, None, x, 1 - core)

    def out_finish(l):
        arrived(wot.at[l, pl.ds(0, nx * slim)], wo_recv.at[l, 6])

    size = 2 * slim
    eight = lax.broadcasted_iota(jnp.int32, (8, 2 * size), 0)
    left = lax.broadcasted_iota(jnp.int32, (8, 2 * size), 1) < size
    left_half = lax.broadcasted_iota(jnp.int32, (half, 2 * size), 1) < size

    def paired(parts, p):
        return jnp.concatenate([parts[2 * p], parts[2 * p + 1]], axis=1)

    def by_head(values):
        one = jnp.sum(jnp.where(left_half, values, 0.0), axis=1, keepdims=True)
        two = jnp.sum(jnp.where(left_half, 0.0, values), axis=1, keepdims=True)
        return jnp.where(left_half, one, two) / size

    def recur(l):
        if l == 0:
            with scope("prepare1"):
                prepare(1)
                turn(1)
        else:
            with scope("update0"):
                update(0)
        with scope(f"exchange{l}"):
            for o in xs:
                arrived(vg.at[l, o], ex_recv.at[o])
        sub = lax.broadcasted_iota(jnp.int32, (rows, rows), 0)
        lane = lax.broadcasted_iota(jnp.int32, (rows, rows), 1)
        spread = jnp.where(sub == lane, lens[...].astype(jnp.float32), 0.0)
        live = jnp.sum(spread, axis=1, keepdims=True) > STEP
        looks, extras, gates = [], [], []
        for h in range(nx):
            part = slice(h * size, (h + 1) * size)
            recept, key, value, decay_pre, rate_pre, gate_pre = [
                vg[l, h, :, q * size : (q + 1) * size].astype(jnp.float32) for q in range(6)
            ]
            decay = jnp.exp(-jnp.exp(-jax.nn.softplus(-(base[l : l + 1, part] + decay_pre)) - 0.5))
            learn = jax.nn.sigmoid(rate[l : l + 1, part] + rate_pre)
            length = jnp.maximum(jnp.sqrt(jnp.sum(key * key, axis=1, keepdims=True)), 1e-12)
            blend = jnp.sum(key * learn * recept, axis=1, keepdims=True)
            unit = key / length
            held = value * length
            rows_ref[l, 0, h] = jnp.where(live, -unit, 0.0)
            rows_ref[l, 1, h] = jnp.where(live, held, 0.0)
            rows_ref[l, 2, h] = jnp.where(live, decay, 1.0)
            rows_ref[l, 3, h] = unit * learn
            looks.append(decay * recept - (blend / length) * unit)
            extras.append(blend * value)
            gates.append(jax.nn.sigmoid(gate_pre) * ggain[l : l + 1, part])
        gates = [paired(gates, p) for p in range(nx // 2)]
        extras = [paired(extras, p) for p in range(nx // 2)]
        for g in range(2):
            reads = [[] for p in range(nx // 2)]
            for k in range(half // 8):
                low = g * half + k * 8
                look = jnp.concatenate([v[low : low + 8] for v in looks], axis=0).astype(jnp.bfloat16)
                sums = [extras[p][low : low + 8] for p in range(nx // 2)]
                for b in range(8):
                    got = jnp.dot(look, turned[l, low + b], preferred_element_type=jnp.float32)
                    for h in range(nx):
                        p = h // 2
                        side = left if h % 2 == 0 else jnp.logical_not(left)
                        piece = got[h * 8 : (h + 1) * 8, p * 128 : (p + 1) * 128]
                        sums[p] += jnp.where((eight == b) & side, piece, 0.0)
                for p in range(nx // 2):
                    reads[p].append(sums[p])
            span = slice(g * half, (g + 1) * half)
            outs = []
            for p in range(nx // 2):
                read = jnp.concatenate(reads[p], axis=0)
                apart = read - by_head(read)
                normal = apart * lax.rsqrt(by_head(apart * apart) + GROUP_EPS) * gates[p][span]
                outs.append(jnp.where(live[span], normal, 0.0).astype(jnp.bfloat16))
            span = pl.ds(pl.multiple_of(t * rows + g * half, half), half)
            mg[l, span, :] = jnp.concatenate(outs, axis=1)
            block = mg.at[l, span]
            for p in far:
                remote(block, block, mg_send.at[0], mg_recv.at[t], p, d).start()

    eye = lax.broadcasted_iota(jnp.int32, (size, size), 0) == lax.broadcasted_iota(jnp.int32, (size, size), 1)

    def update(l):
        def one(i, carry):
            for k in range(4):
                b = i * 4 + k
                for h in range(nx):
                    neg, held, decay, rated = [rows_ref[l, q, h, pl.ds(b, 1), :] for q in range(4)]
                    old = st[l, b, h]
                    weight = jnp.sum(old * neg + jnp.where(eye, held, 0.0), axis=1, keepdims=True)
                    st[l, b, h] = old * decay + weight * rated
            return carry

        lax.fori_loop(0, rows // 4, one, 0)

    def fold(l):
        total = jnp.zeros((rows, width), jnp.float32)
        for o in offs:
            tt = plane(o)
            span = pl.ds(pl.multiple_of(tt * rows, rows), rows)
            if o != (0, 0):
                with scope(f"m{l}_{o[0]}_{o[1]}"):
                    arrived(mg.at[l, span], mg_recv.at[tt])
            cols = pl.ds(pl.multiple_of(tt * width, width), width)
            total += dot_t(mg[l, span, :], wot[l, :, cols])
        return total.astype(jnp.bfloat16)

    for l in range(2):
        with scope(f"start{l}"):
            if l == 1:
                xg[1, slot(t, x, rows), :] = current
            send = gather_start(l)
            if l == 0:
                for ll in range(2):
                    for q in range(6):
                        remote(
                            weights[q].at[ll], wcat.at[ll, wrow(q)], wc_send.at[0], wc_recv.at[ll], t, sibling
                        ).start()
                out_first(0)
            else:
                out_second(1)
        if l == 0:
            with scope("turn0"):
                turn(0)
        gather_relay(l, send)
        if l == 0:
            with scope("prepare0"):
                for copy in small:
                    copy.wait()
                prepare(0)
        with scope(f"project{l}"):
            project(l, lambda: out_second(0) if l == 0 else None)
            out_third(l)
            count = ((nx - 1) + (tp - 1) * nx) * CUT[l] + ((tp - 1) + tp * (nx - 1)) * (rows - CUT[l])
            sent_all(xg.at[l, pl.ds(0, count)], ag_send.at[0])
        with scope(f"recur{l}"):
            recur(l)
        with scope(f"outfourth{l}"):
            out_fourth(l)
            if l == 0:
                out_first(1)
            out_fifth(l)
        if l == 1:
            with scope("update1"):
                update(1)
        with scope(f"outfinish{l}"):
            out_finish(l)
        with scope(f"fold{l}"):
            current = fold(l)
        sent_all(pieces.at[l, pl.ds(0, nx - 1)], ex_send.at[0])
        sent_all(mg.at[l, pl.ds(0, (tp - 1) * rows)], mg_send.at[0])
        sent_all(wot.at[l, pl.ds(0, 7 * slim)], wo_send.at[l])
    mixed_ref[...] = current
    sent_all(wcat.at[0], wc_send.at[0])


def step(tok, lens, gain, base, rate, ggain, weights, wo, state, tp, dp):
    rows, width = tok.shape
    slim = width // dp
    nx = dp // 2
    feat = tp * width
    bf = jnp.bfloat16
    vmem, hbm = pl.BlockSpec(memory_space=pltpu.VMEM), pl.BlockSpec(memory_space=pltpu.HBM)
    dma = pltpu.SemaphoreType.DMA
    half = rows // 2
    return pl.pallas_call(
        functools.partial(step_body, tp=tp, dp=dp),
        out_shape=(
            pltpu.VMEM((rows, width), bf),
            pltpu.VMEM(state.shape, state.dtype),
        ),
        in_specs=[hbm] * 14,
        out_specs=(vmem, vmem),
        scratch_shapes=[
            pltpu.VMEM((2, tp * nx * rows, width), bf),
            pltpu.VMEM((2, 12 * slim, feat), bf),
            pltpu.VMEM((2, width, feat), bf),
            pltpu.VMEM((2, nx, rows, 12 * slim), bf),
            pltpu.VMEM((2, tp * rows, width), bf),
            pltpu.VMEM((2, nx, rows, 12 * slim), bf),
            pltpu.VMEM((2, rows, 2 * slim, nx * 2 * slim), bf),
            pltpu.VMEM((2, 4, nx, rows, 2 * slim), jnp.float32),
            pltpu.VMEM((nx * rows, 12 * slim), jnp.float32),
            pltpu.VMEM((nx * rows, 128), jnp.float32),
            pltpu.VMEM(lens.shape, lens.dtype),
            pltpu.VMEM(gain.shape, gain.dtype),
            pltpu.VMEM(base.shape, base.dtype),
            pltpu.VMEM(rate.shape, rate.dtype),
            pltpu.VMEM(ggain.shape, ggain.dtype),
            dma((1,)),
            dma((nx,)),
            dma((tp,)),
            dma((tp,)),
            dma((1,)),
            dma((nx,)),
            dma((1,)),
            dma((tp,)),
            dma((2,)),
            dma((2, 7)),
            dma((1,)),
            dma((2,)),
            dma((4,)),
            dma((2,)),
            dma((6,)),
        ],
        compiler_params=pltpu.CompilerParams(
            collective_id=0, has_side_effects=True, vmem_limit_bytes=VMEM_LIMIT
        ),
        name="step",
    )(tok, lens, gain, base, rate, ggain, *weights, wo, state)


def put_body(mixed_ref, state_ref, out_ref, new_ref, sem):
    count = state_ref.shape[0] * 4
    part = state_ref.shape[1] // 4
    copies = [pltpu.make_async_copy(mixed_ref, out_ref, sem.at[count])]
    for i in range(count):
        span = pl.ds(i % 4 * part, part)
        copies.append(
            pltpu.make_async_copy(state_ref.at[i // 4, span], new_ref.at[i // 4, span], sem.at[i])
        )
    for copy in copies:
        copy.start()
    for copy in copies:
        copy.wait()


def put(mixed, state):
    vmem, hbm = pl.BlockSpec(memory_space=pltpu.VMEM), pl.BlockSpec(memory_space=pltpu.HBM)
    return pl.pallas_call(
        put_body,
        out_shape=(
            jax.ShapeDtypeStruct(mixed.shape, mixed.dtype),
            jax.ShapeDtypeStruct(state.shape, state.dtype),
        ),
        in_specs=[vmem, vmem],
        out_specs=(hbm, hbm),
        scratch_shapes=[pltpu.SemaphoreType.DMA((state.shape[0] * 4 + 1,))],
        compiler_params=pltpu.CompilerParams(vmem_limit_bytes=4 * 1024 * 1024),
        name="put",
    )(mixed, state)


def on_device(
    tokens,
    lengths,
    norm_gain,
    w_recept,
    w_key,
    w_value,
    w_decay,
    w_rate,
    w_gate,
    w_out,
    decay_base,
    rate_base,
    group_gain,
    state,
):
    tp, dp = lax.axis_size("tp"), lax.axis_size("dp")
    weights = [w.transpose(0, 2, 1) for w in (w_recept, w_key, w_value, w_decay, w_rate, w_gate)]
    mixed, states = step(
        tokens, lengths.reshape(1, -1), norm_gain, decay_base, rate_base, group_gain,
        weights, w_out.transpose(0, 2, 1), state, tp, dp,
    )
    return put(mixed, states)


def solution(mesh):
    columns = P(None, None, ("tp", "dp"))
    in_specs = (
        (P("dp", "tp"), P("dp"), P())
        + (columns,) * 7
        + (P(None, "tp"),) * 3
        + (P(None, "dp", "tp", None, None),)
    )
    out_specs = (P("dp", "tp"), P(None, "dp", "tp", None, None))
    return jax.shard_map(
        on_device, mesh=mesh, in_specs=in_specs, out_specs=out_specs, check_vma=False
    )
```

```python
import contextlib
import functools

import jax
import jax.numpy as jnp
from jax import lax
from jax.experimental import pallas as pl
from jax.experimental.pallas import tpu as pltpu
from jax.sharding import PartitionSpec as P

STEP = 16
RMS_EPS = 1e-06
GROUP_EPS = 0.00064
VMEM_LIMIT = 55_000_000
MESH = pl.DeviceIdType.MESH
CUT = (16, 16)


def scope(name):
    return contextlib.nullcontext()


def dot_t(a, b):
    return lax.dot_general(a, b, (((1,), (1,)), ((), ())), preferred_element_type=jnp.float32)


def plane_offsets(tp):
    ny = 4 if tp == 16 else tp
    nz = tp // ny
    hops = lambda k, n: min(k, n - k)
    offs = [(dz, dy) for dz in range(nz) for dy in range(ny)]
    offs.sort(key=lambda o: (hops(o[0], nz) + hops(o[1], ny), o))
    return ny, nz, offs


def step_body(
    tok, lens_hbm, gain_hbm, base_hbm, rate_hbm, ggain_hbm, wr, wk, wv, wd, wa, wg, wo, state,
    mixed_ref, st,
    xg, wcat, wot, vg, mg, pieces, turned, rows_ref, acc, square,
    lens, gain, base, rate, ggain,
    ag_send, a1_recv, b1_recv, fin_recv, ex_send, ex_recv, mg_send, mg_recv,
    wo_send, wo_recv, wc_send, wc_recv, own_sem, st_sem, small_sem,
    *, tp, dp,
):
    t, d = lax.axis_index("tp"), lax.axis_index("dp")
    nx = dp // 2
    x, core = d // 2, lax.rem(d, 2)
    sibling = d + 1 - 2 * core
    ny, nz, offs = plane_offsets(tp)
    z, y = t // ny, lax.rem(t, ny)
    rows, width = tok.shape
    slim = width // dp
    feat = tp * width
    half = rows // 2
    weights = (wr, wk, wv, wd, wa, wg)

    def plane(off):
        return lax.rem(z + off[0], nz) * ny + lax.rem(y + off[1], ny)

    def xpeer(k):
        return lax.rem(x + k + nx, nx)

    def remote(src, dst, ssem, rsem, tt, dd):
        return pltpu.make_async_remote_copy(
            src_ref=src, dst_ref=dst, send_sem=ssem, recv_sem=rsem,
            device_id=(tt, dd), device_id_type=MESH,
        )

    def arrived(ref, sem):
        remote(ref, ref, ag_send.at[0], sem, t, sibling).wait_recv()

    def fetched(ref, sem):
        pltpu.make_async_copy(ref, ref, sem).wait()

    peers = [plane(o) for o in offs[1:]]
    far = peers
    ks = [1, nx - 1] + list(range(2, nx - 1))
    xs = [xpeer(k) for k in ks]
    outward = xs[::-1]


    def fetch(src, dst, sem):
        copy = pltpu.make_async_copy(src, dst, sem)
        copy.start()
        return copy

    def wrow(q):
        return pl.ds(pl.multiple_of(q * 2 * slim + core * slim, slim), slim)

    def worow(dd, start=0, count=None):
        return pl.ds(pl.multiple_of(dd * slim + start, slim // 2), slim if count is None else count)

    def slot(tt, xx, count):
        return pl.ds(pl.multiple_of(tt * (nx * rows) + xx * rows, rows), count)

    def share(l, tt, xx, h):
        start, count = (0, CUT[l]) if h == 0 else (CUT[l], rows - CUT[l])
        return pl.ds(pl.multiple_of(tt * (nx * rows) + xx * rows + start, 8), count)

    own_tok = fetch(tok, xg.at[0, slot(t, x, rows)], small_sem.at[5])
    barrier = pltpu.get_barrier_semaphore()
    everyone = [(p, d) for p in far[::-1]] + [(t, 2 * o + core) for o in xs] + [(t, sibling)]
    for p in everyone:
        pl.semaphore_signal(barrier, inc=1, device_id=p, device_id_type=MESH)
    own_o = [fetch(wo.at[0], wot.at[0, worow(d)], own_sem.at[2])]
    small = [
        fetch(src, dst, small_sem.at[i])
        for i, (src, dst) in enumerate(
            [(lens_hbm, lens), (gain_hbm, gain), (base_hbm, base), (rate_hbm, rate), (ggain_hbm, ggain)]
        )
    ]
    for l in range(2):
        for q in range(6):
            fetch(weights[q].at[l], wcat.at[l, wrow(q)], own_sem.at[l])
    own_s = [fetch(state.at[0], st.at[0], st_sem.at[0])]
    own_o.append(fetch(wo.at[1], wot.at[1, worow(d)], own_sem.at[3]))
    own_s.append(fetch(state.at[1], st.at[1], st_sem.at[1]))


    def turn(l):
        own_s[l].wait()

        def one(i, carry):
            for k in range(4):
                for p in range(nx // 2):
                    both = jnp.concatenate([st[l, i * 4 + k, 2 * p], st[l, i * 4 + k, 2 * p + 1]], axis=0)
                    turned[l, i * 4 + k, :, p * 128 : (p + 1) * 128] = both.T.astype(jnp.bfloat16)
            return carry

        lax.fori_loop(0, rows // 4, one, 0)

    with scope("barrier"):
        pl.semaphore_wait(barrier, len(everyone))
    with scope("small"):
        own_tok.wait()

    def gather_start(l):
        def send(block, rsem, tt, dd):
            remote(block, block, ag_send.at[0], rsem, tt, dd).start()

        first, second = xg.at[l, share(l, t, x, 0)], xg.at[l, share(l, t, x, 1)]
        for o in outward:
            send(first, a1_recv.at[x], t, 2 * o + core)
        for p in peers:
            send(second, b1_recv.at[t], p, d)
        for o in outward:
            send(second, fin_recv.at[t], t, 2 * o + core)
        for p in far:
            send(first, fin_recv.at[t], p, d)
        return send

    def gather_relay(l, send):
        steps = [("b", peers[0]), ("a", xs[0])]
        steps += [("b", peers[1]), ("a", xs[1])]
        steps += [("b", p) for p in peers[2:4]] + [("a", o) for o in xs[2:]]
        steps += [("b", p) for p in peers[4:]]
        for i, (kind, o) in enumerate(steps):
            with scope(f"{kind}{l}_{i}"):
                if kind == "a":
                    block = xg.at[l, share(l, t, o, 0)]
                    arrived(block, a1_recv.at[o])
                    for p in far:
                        send(block, fin_recv.at[t], p, d)
                else:
                    block = xg.at[l, share(l, o, x, 1)]
                    arrived(block, b1_recv.at[o])
                    for p in outward:
                        send(block, fin_recv.at[o], t, 2 * p + core)

    def sent_all(ref, sem):
        remote(ref, ref, sem, ex_recv.at[0], t, sibling).wait_send()

    def prepare(l):
        fetched(wcat.at[l, pl.ds(0, 6 * slim)], own_sem.at[l])
        arrived(wcat.at[l, pl.ds(0, 6 * slim)], wc_recv.at[l])
        line = gain[l : l + 1, :]

        def one(i, carry):
            part = pl.ds(pl.multiple_of(i * 16, 16), 16)
            wcat[l, part, :] = (wcat[l, part, :].astype(jnp.float32) * line).astype(jnp.bfloat16)
            return carry

        lax.fori_loop(0, 12 * slim // 16, one, 0)

    def project(l, after):
        acc[...] = jnp.zeros_like(acc)
        square[...] = jnp.zeros_like(square)
        for i, o in enumerate(offs):
            tt = plane(o)
            count = (nx - 1) * (rows - CUT[l]) + (0 if o == (0, 0) else nx * CUT[l])
            with scope(f"x{l}_{o[0]}_{o[1]}"):
                arrived(xg.at[l, pl.ds(0, count)], fin_recv.at[tt])
            if i == 3:
                after()
            block = xg[l, slot(tt, 0, nx * rows), :]
            cols = pl.ds(pl.multiple_of(tt * width, width), width)
            acc[...] += dot_t(block, wcat[l, :, cols])
            values = block.astype(jnp.float32)
            values = values * values
            total = values[:, :128]
            for j in range(1, width // 128):
                total += values[:, j * 128 : (j + 1) * 128]
            square[...] += total
        factor = lax.rsqrt(jnp.sum(square[...], axis=1, keepdims=True) / feat + RMS_EPS)
        done = (acc[...] * factor).astype(jnp.bfloat16)
        for j in range(nx):
            pieces[l, j] = done[j * rows : (j + 1) * rows]
        for o in outward:
            remote(pieces.at[l, o], vg.at[l, x], ex_send.at[0], ex_recv.at[x], t, 2 * o + core).start()
        vg[l, x] = pieces[l, x]

    part = slim // 2
    up, down, across = xpeer(1), xpeer(-1), xpeer(2)

    def out_piece(l, xx, cc, piece):
        start, count = (0, slim) if piece is None else (piece * part, part)
        return wot.at[l, worow(2 * xx + cc, start, count)]

    def out_send(l, n, xx, piece, to_x, to_core):
        block = out_piece(l, xx, core, piece)
        remote(block, block, wo_send.at[l], wo_recv.at[l, n], t, 2 * to_x + to_core).start()

    def out_arrived(l, n, xx, piece):
        arrived(out_piece(l, xx, core, piece), wo_recv.at[l, n])

    def out_first(l):
        own_o[l].wait()
        out_send(l, 0, x, 0, up, core)
        out_send(l, 1, x, 1, down, core)
        out_send(l, 6, x, None, x, 1 - core)

    def out_second(l):
        out_arrived(l, 0, down, 0)
        out_send(l, 4, down, 0, up, core)
        out_send(l, 6, down, 0, x, 1 - core)
        out_arrived(l, 1, up, 1)
        out_send(l, 5, up, 1, down, core)
        out_send(l, 6, up, 1, x, 1 - core)

    def out_third(l):
        out_send(l, 2, x, 1, up, core)
        out_send(l, 3, x, 0, down, core)

    def out_fourth(l):
        out_arrived(l, 2, down, 1)
        out_send(l, 6, down, 1, x, 1 - core)
        out_arrived(l, 3, up, 0)
        out_send(l, 6, up, 0, x, 1 - core)

    def out_fifth(l):
        out_arrived(l, 4, across, 0)
        out_arrived(l, 5, across, 1)
        out_send(l, 6, across, None, x, 1 - core)

    def out_finish(l):
        arrived(wot.at[l, pl.ds(0, nx * slim)], wo_recv.at[l, 6])

    size = 2 * slim
    eight = lax.broadcasted_iota(jnp.int32, (8, 2 * size), 0)
    left = lax.broadcasted_iota(jnp.int32, (8, 2 * size), 1) < size
    left_half = lax.broadcasted_iota(jnp.int32, (half, 2 * size), 1) < size

    def paired(parts, p):
        return jnp.concatenate([parts[2 * p], parts[2 * p + 1]], axis=1)

    def by_head(values):
        one = jnp.sum(jnp.where(left_half, values, 0.0), axis=1, keepdims=True)
        two = jnp.sum(jnp.where(left_half, 0.0, values), axis=1, keepdims=True)
        return jnp.where(left_half, one, two) / size

    def recur(l):
        if l == 0:
            with scope("prepare1"):
                prepare(1)
                turn(1)
        else:
            with scope("update0"):
                update(0)
        with scope(f"exchange{l}"):
            for o in xs:
                arrived(vg.at[l, o], ex_recv.at[o])
        sub = lax.broadcasted_iota(jnp.int32, (rows, rows), 0)
        lane = lax.broadcasted_iota(jnp.int32, (rows, rows), 1)
        spread = jnp.where(sub == lane, lens[...].astype(jnp.float32), 0.0)
        live = jnp.sum(spread, axis=1, keepdims=True) > STEP
        looks, extras, gates = [], [], []
        for h in range(nx):
            part = slice(h * size, (h + 1) * size)
            recept, key, value, decay_pre, rate_pre, gate_pre = [
                vg[l, h, :, q * size : (q + 1) * size].astype(jnp.float32) for q in range(6)
            ]
            decay = jnp.exp(-jnp.exp(-jax.nn.softplus(-(base[l : l + 1, part] + decay_pre)) - 0.5))
            learn = jax.nn.sigmoid(rate[l : l + 1, part] + rate_pre)
            length = jnp.maximum(jnp.sqrt(jnp.sum(key * key, axis=1, keepdims=True)), 1e-12)
            blend = jnp.sum(key * learn * recept, axis=1, keepdims=True)
            unit = key / length
            held = value * length
            rows_ref[l, 0, h] = jnp.where(live, -unit, 0.0)
            rows_ref[l, 1, h] = jnp.where(live, held, 0.0)
            rows_ref[l, 2, h] = jnp.where(live, decay, 1.0)
            rows_ref[l, 3, h] = unit * learn
            looks.append(decay * recept - (blend / length) * unit)
            extras.append(blend * value)
            gates.append(jax.nn.sigmoid(gate_pre) * ggain[l : l + 1, part])
        gates = [paired(gates, p) for p in range(nx // 2)]
        extras = [paired(extras, p) for p in range(nx // 2)]
        for g in range(2):
            reads = [[] for p in range(nx // 2)]
            for k in range(half // 8):
                low = g * half + k * 8
                look = jnp.concatenate([v[low : low + 8] for v in looks], axis=0).astype(jnp.bfloat16)
                sums = [extras[p][low : low + 8] for p in range(nx // 2)]
                for b in range(8):
                    got = jnp.dot(look, turned[l, low + b], preferred_element_type=jnp.float32)
                    for h in range(nx):
                        p = h // 2
                        side = left if h % 2 == 0 else jnp.logical_not(left)
                        piece = got[h * 8 : (h + 1) * 8, p * 128 : (p + 1) * 128]
                        sums[p] += jnp.where((eight == b) & side, piece, 0.0)
                for p in range(nx // 2):
                    reads[p].append(sums[p])
            span = slice(g * half, (g + 1) * half)
            outs = []
            for p in range(nx // 2):
                read = jnp.concatenate(reads[p], axis=0)
                apart = read - by_head(read)
                normal = apart * lax.rsqrt(by_head(apart * apart) + GROUP_EPS) * gates[p][span]
                outs.append(jnp.where(live[span], normal, 0.0).astype(jnp.bfloat16))
            span = pl.ds(pl.multiple_of(t * rows + g * half, half), half)
            mg[l, span, :] = jnp.concatenate(outs, axis=1)
            block = mg.at[l, span]
            for p in far:
                remote(block, block, mg_send.at[0], mg_recv.at[t], p, d).start()

    eye = lax.broadcasted_iota(jnp.int32, (size, size), 0) == lax.broadcasted_iota(jnp.int32, (size, size), 1)

    def update(l):
        def one(i, carry):
            for k in range(4):
                b = i * 4 + k
                for h in range(nx):
                    neg, held, decay, rated = [rows_ref[l, q, h, pl.ds(b, 1), :] for q in range(4)]
                    old = st[l, b, h]
                    weight = jnp.sum(old * neg + jnp.where(eye, held, 0.0), axis=1, keepdims=True)
                    st[l, b, h] = old * decay + weight * rated
            return carry

        lax.fori_loop(0, rows // 4, one, 0)

    def fold(l):
        total = jnp.zeros((rows, width), jnp.float32)
        for o in offs:
            tt = plane(o)
            span = pl.ds(pl.multiple_of(tt * rows, rows), rows)
            if o != (0, 0):
                with scope(f"m{l}_{o[0]}_{o[1]}"):
                    arrived(mg.at[l, span], mg_recv.at[tt])
            cols = pl.ds(pl.multiple_of(tt * width, width), width)
            total += dot_t(mg[l, span, :], wot[l, :, cols])
        return total.astype(jnp.bfloat16)

    for l in range(2):
        with scope(f"start{l}"):
            if l == 1:
                xg[1, slot(t, x, rows), :] = current
            send = gather_start(l)
            if l == 0:
                out_first(0)
            if l == 0:
                for ll in range(1):
                    for q in range(6):
                        remote(
                            weights[q].at[ll], wcat.at[ll, wrow(q)], wc_send.at[0], wc_recv.at[ll], t, sibling
                        ).start()
            else:
                out_second(1)
        gather_relay(l, send)
        if l == 0:
            with scope("turn0"):
                turn(0)
            for q in range(6):
                remote(
                    weights[q].at[1], wcat.at[1, wrow(q)], wc_send.at[0], wc_recv.at[1], t, sibling
                ).start()
            with scope("prepare0"):
                for copy in small:
                    copy.wait()
                prepare(0)
        with scope(f"project{l}"):
            project(l, lambda: out_second(0) if l == 0 else None)
            out_third(l)
            count = ((nx - 1) + (tp - 1) * nx) * CUT[l] + ((tp - 1) + tp * (nx - 1)) * (rows - CUT[l])
            sent_all(xg.at[l, pl.ds(0, count)], ag_send.at[0])
        with scope(f"recur{l}"):
            recur(l)
        with scope(f"outfourth{l}"):
            out_fourth(l)
            if l == 0:
                out_first(1)
            out_fifth(l)
        if l == 1:
            with scope("update1"):
                update(1)
        with scope(f"outfinish{l}"):
            out_finish(l)
        with scope(f"fold{l}"):
            current = fold(l)
        sent_all(pieces.at[l, pl.ds(0, nx - 1)], ex_send.at[0])
        sent_all(mg.at[l, pl.ds(0, (tp - 1) * rows)], mg_send.at[0])
        sent_all(wot.at[l, pl.ds(0, 7 * slim)], wo_send.at[l])
    mixed_ref[...] = current
    sent_all(wcat.at[0], wc_send.at[0])


def step(tok, lens, gain, base, rate, ggain, weights, wo, state, tp, dp):
    rows, width = tok.shape
    slim = width // dp
    nx = dp // 2
    feat = tp * width
    bf = jnp.bfloat16
    vmem, hbm = pl.BlockSpec(memory_space=pltpu.VMEM), pl.BlockSpec(memory_space=pltpu.HBM)
    dma = pltpu.SemaphoreType.DMA
    half = rows // 2
    return pl.pallas_call(
        functools.partial(step_body, tp=tp, dp=dp),
        out_shape=(
            pltpu.VMEM((rows, width), bf),
            pltpu.VMEM(state.shape, state.dtype),
        ),
        in_specs=[hbm] * 14,
        out_specs=(vmem, vmem),
        scratch_shapes=[
            pltpu.VMEM((2, tp * nx * rows, width), bf),
            pltpu.VMEM((2, 12 * slim, feat), bf),
            pltpu.VMEM((2, width, feat), bf),
            pltpu.VMEM((2, nx, rows, 12 * slim), bf),
            pltpu.VMEM((2, tp * rows, width), bf),
            pltpu.VMEM((2, nx, rows, 12 * slim), bf),
            pltpu.VMEM((2, rows, 2 * slim, nx * 2 * slim), bf),
            pltpu.VMEM((2, 4, nx, rows, 2 * slim), jnp.float32),
            pltpu.VMEM((nx * rows, 12 * slim), jnp.float32),
            pltpu.VMEM((nx * rows, 128), jnp.float32),
            pltpu.VMEM(lens.shape, lens.dtype),
            pltpu.VMEM(gain.shape, gain.dtype),
            pltpu.VMEM(base.shape, base.dtype),
            pltpu.VMEM(rate.shape, rate.dtype),
            pltpu.VMEM(ggain.shape, ggain.dtype),
            dma((1,)),
            dma((nx,)),
            dma((tp,)),
            dma((tp,)),
            dma((1,)),
            dma((nx,)),
            dma((1,)),
            dma((tp,)),
            dma((2,)),
            dma((2, 7)),
            dma((1,)),
            dma((2,)),
            dma((4,)),
            dma((2,)),
            dma((6,)),
        ],
        compiler_params=pltpu.CompilerParams(
            collective_id=0, has_side_effects=True, vmem_limit_bytes=VMEM_LIMIT
        ),
        name="step",
    )(tok, lens, gain, base, rate, ggain, *weights, wo, state)


def put_body(mixed_ref, state_ref, out_ref, new_ref, sem):
    count = state_ref.shape[0] * 4
    part = state_ref.shape[1] // 4
    copies = [pltpu.make_async_copy(mixed_ref, out_ref, sem.at[count])]
    for i in range(count):
        span = pl.ds(i % 4 * part, part)
        copies.append(
            pltpu.make_async_copy(state_ref.at[i // 4, span], new_ref.at[i // 4, span], sem.at[i])
        )
    for copy in copies:
        copy.start()
    for copy in copies:
        copy.wait()


def put(mixed, state):
    vmem, hbm = pl.BlockSpec(memory_space=pltpu.VMEM), pl.BlockSpec(memory_space=pltpu.HBM)
    return pl.pallas_call(
        put_body,
        out_shape=(
            jax.ShapeDtypeStruct(mixed.shape, mixed.dtype),
            jax.ShapeDtypeStruct(state.shape, state.dtype),
        ),
        in_specs=[vmem, vmem],
        out_specs=(hbm, hbm),
        scratch_shapes=[pltpu.SemaphoreType.DMA((state.shape[0] * 4 + 1,))],
        compiler_params=pltpu.CompilerParams(vmem_limit_bytes=4 * 1024 * 1024),
        name="put",
    )(mixed, state)


def on_device(
    tokens,
    lengths,
    norm_gain,
    w_recept,
    w_key,
    w_value,
    w_decay,
    w_rate,
    w_gate,
    w_out,
    decay_base,
    rate_base,
    group_gain,
    state,
):
    tp, dp = lax.axis_size("tp"), lax.axis_size("dp")
    weights = [w.transpose(0, 2, 1) for w in (w_recept, w_key, w_value, w_decay, w_rate, w_gate)]
    mixed, states = step(
        tokens, lengths.reshape(1, -1), norm_gain, decay_base, rate_base, group_gain,
        weights, w_out.transpose(0, 2, 1), state, tp, dp,
    )
    return put(mixed, states)


def solution(mesh):
    columns = P(None, None, ("tp", "dp"))
    in_specs = (
        (P("dp", "tp"), P("dp"), P())
        + (columns,) * 7
        + (P(None, "tp"),) * 3
        + (P(None, "dp", "tp", None, None),)
    )
    out_specs = (P("dp", "tp"), P(None, "dp", "tp", None, None))
    return jax.shard_map(
        on_device, mesh=mesh, in_specs=in_specs, out_specs=out_specs, check_vma=False
    )
```

```python
import contextlib
import functools

import jax
import jax.numpy as jnp
from jax import lax
from jax.experimental import pallas as pl
from jax.experimental.pallas import tpu as pltpu
from jax.sharding import PartitionSpec as P

STEP = 16
RMS_EPS = 1e-06
GROUP_EPS = 0.00064
VMEM_LIMIT = 55_000_000
MESH = pl.DeviceIdType.MESH
CUT = (16, 16)


def scope(name):
    return contextlib.nullcontext()


def dot_t(a, b):
    return lax.dot_general(a, b, (((1,), (1,)), ((), ())), preferred_element_type=jnp.float32)


def plane_offsets(tp):
    ny = 4 if tp == 16 else tp
    nz = tp // ny
    hops = lambda k, n: min(k, n - k)
    offs = [(dz, dy) for dz in range(nz) for dy in range(ny)]
    offs.sort(key=lambda o: (hops(o[0], nz) + hops(o[1], ny), o))
    return ny, nz, offs


def step_body(
    tok, lens_hbm, gain_hbm, base_hbm, rate_hbm, ggain_hbm, wr, wk, wv, wd, wa, wg, wo, state,
    mixed_ref, st,
    xg, wcat, wot, vg, mg, pieces, turned, rows_ref, acc, square,
    lens, gain, base, rate, ggain,
    ag_send, a1_recv, b1_recv, fin_recv, ex_send, ex_recv, mg_send, mg_recv,
    wo_send, wo_recv, wc_send, wc_recv, own_sem, st_sem, small_sem,
    *, tp, dp,
):
    t, d = lax.axis_index("tp"), lax.axis_index("dp")
    nx = dp // 2
    x, core = d // 2, lax.rem(d, 2)
    sibling = d + 1 - 2 * core
    ny, nz, offs = plane_offsets(tp)
    z, y = t // ny, lax.rem(t, ny)
    rows, width = tok.shape
    slim = width // dp
    feat = tp * width
    half = rows // 2
    weights = (wr, wk, wv, wd, wa, wg)

    def plane(off):
        return lax.rem(z + off[0], nz) * ny + lax.rem(y + off[1], ny)

    def xpeer(k):
        return lax.rem(x + k + nx, nx)

    def remote(src, dst, ssem, rsem, tt, dd):
        return pltpu.make_async_remote_copy(
            src_ref=src, dst_ref=dst, send_sem=ssem, recv_sem=rsem,
            device_id=(tt, dd), device_id_type=MESH,
        )

    def arrived(ref, sem):
        remote(ref, ref, ag_send.at[0], sem, t, sibling).wait_recv()

    def fetched(ref, sem):
        pltpu.make_async_copy(ref, ref, sem).wait()

    peers = [plane(o) for o in offs[1:]]
    far = peers
    ks = [1, nx - 1] + list(range(2, nx - 1))
    xs = [xpeer(k) for k in ks]
    outward = xs[::-1]


    def fetch(src, dst, sem):
        copy = pltpu.make_async_copy(src, dst, sem)
        copy.start()
        return copy

    def wrow(q):
        return pl.ds(pl.multiple_of(q * 2 * slim + core * slim, slim), slim)

    def worow(dd, start=0, count=None):
        return pl.ds(pl.multiple_of(dd * slim + start, slim // 2), slim if count is None else count)

    def slot(tt, xx, count):
        return pl.ds(pl.multiple_of(tt * (nx * rows) + xx * rows, rows), count)

    def share(l, tt, xx, h):
        start, count = (0, CUT[l]) if h == 0 else (CUT[l], rows - CUT[l])
        return pl.ds(pl.multiple_of(tt * (nx * rows) + xx * rows + start, 8), count)

    own_tok = fetch(tok, xg.at[0, slot(t, x, rows)], small_sem.at[5])
    barrier = pltpu.get_barrier_semaphore()
    everyone = [(p, d) for p in far[::-1]] + [(t, 2 * o + core) for o in xs] + [(t, sibling)]
    for p in everyone:
        pl.semaphore_signal(barrier, inc=1, device_id=p, device_id_type=MESH)
    own_o = [fetch(wo.at[0], wot.at[0, worow(d)], own_sem.at[2])]
    small = [
        fetch(src, dst, small_sem.at[i])
        for i, (src, dst) in enumerate(
            [(lens_hbm, lens), (gain_hbm, gain), (base_hbm, base), (rate_hbm, rate), (ggain_hbm, ggain)]
        )
    ]
    for l in range(2):
        for q in range(6):
            fetch(weights[q].at[l], wcat.at[l, wrow(q)], own_sem.at[l])
    own_s = [fetch(state.at[0], st.at[0], st_sem.at[0])]
    own_o.append(fetch(wo.at[1], wot.at[1, worow(d)], own_sem.at[3]))
    own_s.append(fetch(state.at[1], st.at[1], st_sem.at[1]))


    def turn(l):
        own_s[l].wait()

        def one(i, carry):
            for k in range(4):
                for p in range(nx // 2):
                    both = jnp.concatenate([st[l, i * 4 + k, 2 * p], st[l, i * 4 + k, 2 * p + 1]], axis=0)
                    turned[l, i * 4 + k, :, p * 128 : (p + 1) * 128] = both.T.astype(jnp.bfloat16)
            return carry

        lax.fori_loop(0, rows // 4, one, 0)

    with scope("barrier"):
        pl.semaphore_wait(barrier, len(everyone))
    with scope("small"):
        own_tok.wait()

    def gather_start(l):
        def send(block, rsem, tt, dd):
            remote(block, block, ag_send.at[0], rsem, tt, dd).start()

        first, second = xg.at[l, share(l, t, x, 0)], xg.at[l, share(l, t, x, 1)]
        for o in outward:
            send(first, a1_recv.at[x], t, 2 * o + core)
        for p in peers:
            send(second, b1_recv.at[t], p, d)
        for o in outward:
            send(second, fin_recv.at[t], t, 2 * o + core)
        for p in far:
            send(first, fin_recv.at[t], p, d)
        return send

    def gather_relay(l, send):
        steps = [("b", peers[0]), ("a", xs[0])]
        steps += [("b", peers[1]), ("a", xs[1])]
        steps += [("b", p) for p in peers[2:4]] + [("a", o) for o in xs[2:]]
        steps += [("b", p) for p in peers[4:]]
        for i, (kind, o) in enumerate(steps):
            with scope(f"{kind}{l}_{i}"):
                if kind == "a":
                    block = xg.at[l, share(l, t, o, 0)]
                    arrived(block, a1_recv.at[o])
                    for p in far:
                        send(block, fin_recv.at[t], p, d)
                else:
                    block = xg.at[l, share(l, o, x, 1)]
                    arrived(block, b1_recv.at[o])
                    for p in outward:
                        send(block, fin_recv.at[o], t, 2 * p + core)

    def sent_all(ref, sem):
        remote(ref, ref, sem, ex_recv.at[0], t, sibling).wait_send()

    def prepare(l):
        fetched(wcat.at[l, pl.ds(0, 6 * slim)], own_sem.at[l])
        arrived(wcat.at[l, pl.ds(0, 6 * slim)], wc_recv.at[l])
        line = gain[l : l + 1, :]

        def one(i, carry):
            part = pl.ds(pl.multiple_of(i * 16, 16), 16)
            wcat[l, part, :] = (wcat[l, part, :].astype(jnp.float32) * line).astype(jnp.bfloat16)
            return carry

        lax.fori_loop(0, 12 * slim // 16, one, 0)

    def project(l, after):
        acc[...] = jnp.zeros_like(acc)
        square[...] = jnp.zeros_like(square)
        for i, o in enumerate(offs):
            tt = plane(o)
            count = (nx - 1) * (rows - CUT[l]) + (0 if o == (0, 0) else nx * CUT[l])
            with scope(f"x{l}_{o[0]}_{o[1]}"):
                arrived(xg.at[l, pl.ds(0, count)], fin_recv.at[tt])
            if i == 2:
                after()
            block = xg[l, slot(tt, 0, nx * rows), :]
            cols = pl.ds(pl.multiple_of(tt * width, width), width)
            acc[...] += dot_t(block, wcat[l, :, cols])
            values = block.astype(jnp.float32)
            values = values * values
            total = values[:, :128]
            for j in range(1, width // 128):
                total += values[:, j * 128 : (j + 1) * 128]
            square[...] += total
        factor = lax.rsqrt(jnp.sum(square[...], axis=1, keepdims=True) / feat + RMS_EPS)
        done = (acc[...] * factor).astype(jnp.bfloat16)
        for j in range(nx):
            pieces[l, j] = done[j * rows : (j + 1) * rows]
        for o in outward:
            remote(pieces.at[l, o], vg.at[l, x], ex_send.at[0], ex_recv.at[x], t, 2 * o + core).start()
        vg[l, x] = pieces[l, x]

    part = slim // 2
    up, down, across = xpeer(1), xpeer(-1), xpeer(2)

    def out_piece(l, xx, cc, piece):
        start, count = (0, slim) if piece is None else (piece * part, part)
        return wot.at[l, worow(2 * xx + cc, start, count)]

    def out_send(l, n, xx, piece, to_x, to_core):
        block = out_piece(l, xx, core, piece)
        remote(block, block, wo_send.at[l], wo_recv.at[l, n], t, 2 * to_x + to_core).start()

    def out_arrived(l, n, xx, piece):
        arrived(out_piece(l, xx, core, piece), wo_recv.at[l, n])

    def out_first(l):
        own_o[l].wait()
        out_send(l, 0, x, 0, up, core)
        out_send(l, 1, x, 1, down, core)
        out_send(l, 6, x, None, x, 1 - core)

    def out_second(l):
        out_arrived(l, 0, down, 0)
        out_send(l, 4, down, 0, up, core)
        out_send(l, 6, down, 0, x, 1 - core)
        out_arrived(l, 1, up, 1)
        out_send(l, 5, up, 1, down, core)
        out_send(l, 6, up, 1, x, 1 - core)

    def out_third(l):
        out_send(l, 2, x, 1, up, core)
        out_send(l, 3, x, 0, down, core)

    def out_fourth(l):
        out_arrived(l, 2, down, 1)
        out_send(l, 6, down, 1, x, 1 - core)
        out_arrived(l, 3, up, 0)
        out_send(l, 6, up, 0, x, 1 - core)

    def out_fifth(l):
        out_arrived(l, 4, across, 0)
        out_arrived(l, 5, across, 1)
        out_send(l, 6, across, None, x, 1 - core)

    def out_finish(l):
        arrived(wot.at[l, pl.ds(0, nx * slim)], wo_recv.at[l, 6])

    size = 2 * slim
    eight = lax.broadcasted_iota(jnp.int32, (8, 2 * size), 0)
    left = lax.broadcasted_iota(jnp.int32, (8, 2 * size), 1) < size
    left_half = lax.broadcasted_iota(jnp.int32, (half, 2 * size), 1) < size

    def paired(parts, p):
        return jnp.concatenate([parts[2 * p], parts[2 * p + 1]], axis=1)

    def by_head(values):
        one = jnp.sum(jnp.where(left_half, values, 0.0), axis=1, keepdims=True)
        two = jnp.sum(jnp.where(left_half, 0.0, values), axis=1, keepdims=True)
        return jnp.where(left_half, one, two) / size

    def recur(l):
        if l == 0:
            with scope("prepare1"):
                prepare(1)
                turn(1)
        else:
            with scope("update0"):
                update(0)
        with scope(f"exchange{l}"):
            for o in xs:
                arrived(vg.at[l, o], ex_recv.at[o])
        sub = lax.broadcasted_iota(jnp.int32, (rows, rows), 0)
        lane = lax.broadcasted_iota(jnp.int32, (rows, rows), 1)
        spread = jnp.where(sub == lane, lens[...].astype(jnp.float32), 0.0)
        live = jnp.sum(spread, axis=1, keepdims=True) > STEP
        looks, extras, gates = [], [], []
        for h in range(nx):
            part = slice(h * size, (h + 1) * size)
            recept, key, value, decay_pre, rate_pre, gate_pre = [
                vg[l, h, :, q * size : (q + 1) * size].astype(jnp.float32) for q in range(6)
            ]
            decay = jnp.exp(-jnp.exp(-jax.nn.softplus(-(base[l : l + 1, part] + decay_pre)) - 0.5))
            learn = jax.nn.sigmoid(rate[l : l + 1, part] + rate_pre)
            length = jnp.maximum(jnp.sqrt(jnp.sum(key * key, axis=1, keepdims=True)), 1e-12)
            blend = jnp.sum(key * learn * recept, axis=1, keepdims=True)
            unit = key / length
            held = value * length
            rows_ref[l, 0, h] = jnp.where(live, -unit, 0.0)
            rows_ref[l, 1, h] = jnp.where(live, held, 0.0)
            rows_ref[l, 2, h] = jnp.where(live, decay, 1.0)
            rows_ref[l, 3, h] = unit * learn
            looks.append(decay * recept - (blend / length) * unit)
            extras.append(blend * value)
            gates.append(jax.nn.sigmoid(gate_pre) * ggain[l : l + 1, part])
        gates = [paired(gates, p) for p in range(nx // 2)]
        extras = [paired(extras, p) for p in range(nx // 2)]
        for g in range(2):
            reads = [[] for p in range(nx // 2)]
            for k in range(half // 8):
                low = g * half + k * 8
                look = jnp.concatenate([v[low : low + 8] for v in looks], axis=0).astype(jnp.bfloat16)
                sums = [extras[p][low : low + 8] for p in range(nx // 2)]
                for b in range(8):
                    got = jnp.dot(look, turned[l, low + b], preferred_element_type=jnp.float32)
                    for h in range(nx):
                        p = h // 2
                        side = left if h % 2 == 0 else jnp.logical_not(left)
                        piece = got[h * 8 : (h + 1) * 8, p * 128 : (p + 1) * 128]
                        sums[p] += jnp.where((eight == b) & side, piece, 0.0)
                for p in range(nx // 2):
                    reads[p].append(sums[p])
            span = slice(g * half, (g + 1) * half)
            outs = []
            for p in range(nx // 2):
                read = jnp.concatenate(reads[p], axis=0)
                apart = read - by_head(read)
                normal = apart * lax.rsqrt(by_head(apart * apart) + GROUP_EPS) * gates[p][span]
                outs.append(jnp.where(live[span], normal, 0.0).astype(jnp.bfloat16))
            span = pl.ds(pl.multiple_of(t * rows + g * half, half), half)
            mg[l, span, :] = jnp.concatenate(outs, axis=1)
            block = mg.at[l, span]
            for p in far:
                remote(block, block, mg_send.at[0], mg_recv.at[t], p, d).start()

    eye = lax.broadcasted_iota(jnp.int32, (size, size), 0) == lax.broadcasted_iota(jnp.int32, (size, size), 1)

    def update(l):
        def one(i, carry):
            for k in range(4):
                b = i * 4 + k
                for h in range(nx):
                    neg, held, decay, rated = [rows_ref[l, q, h, pl.ds(b, 1), :] for q in range(4)]
                    old = st[l, b, h]
                    weight = jnp.sum(old * neg + jnp.where(eye, held, 0.0), axis=1, keepdims=True)
                    st[l, b, h] = old * decay + weight * rated
            return carry

        lax.fori_loop(0, rows // 4, one, 0)

    def fold(l):
        total = jnp.zeros((rows, width), jnp.float32)
        for o in offs:
            tt = plane(o)
            span = pl.ds(pl.multiple_of(tt * rows, rows), rows)
            if o != (0, 0):
                with scope(f"m{l}_{o[0]}_{o[1]}"):
                    arrived(mg.at[l, span], mg_recv.at[tt])
            cols = pl.ds(pl.multiple_of(tt * width, width), width)
            total += dot_t(mg[l, span, :], wot[l, :, cols])
        return total.astype(jnp.bfloat16)

    for l in range(2):
        with scope(f"start{l}"):
            if l == 1:
                xg[1, slot(t, x, rows), :] = current
            send = gather_start(l)
            if l == 0:
                out_first(0)
            if l == 0:
                for ll in range(1):
                    for q in range(6):
                        remote(
                            weights[q].at[ll], wcat.at[ll, wrow(q)], wc_send.at[0], wc_recv.at[ll], t, sibling
                        ).start()
            else:
                out_second(1)
        gather_relay(l, send)
        if l == 0:
            with scope("turn0"):
                turn(0)
            for q in range(6):
                remote(
                    weights[q].at[1], wcat.at[1, wrow(q)], wc_send.at[0], wc_recv.at[1], t, sibling
                ).start()
            with scope("prepare0"):
                for copy in small:
                    copy.wait()
                prepare(0)
        with scope(f"project{l}"):
            project(l, lambda: out_second(0) if l == 0 else None)
            out_third(l)
            count = ((nx - 1) + (tp - 1) * nx) * CUT[l] + ((tp - 1) + tp * (nx - 1)) * (rows - CUT[l])
            sent_all(xg.at[l, pl.ds(0, count)], ag_send.at[0])
        with scope(f"recur{l}"):
            recur(l)
        with scope(f"outfourth{l}"):
            out_fourth(l)
            if l == 0:
                out_first(1)
            out_fifth(l)
        if l == 1:
            with scope("update1"):
                update(1)
        with scope(f"outfinish{l}"):
            out_finish(l)
        with scope(f"fold{l}"):
            current = fold(l)
        sent_all(pieces.at[l, pl.ds(0, nx - 1)], ex_send.at[0])
        sent_all(mg.at[l, pl.ds(0, (tp - 1) * rows)], mg_send.at[0])
        sent_all(wot.at[l, pl.ds(0, 7 * slim)], wo_send.at[l])
    mixed_ref[...] = current
    sent_all(wcat.at[0], wc_send.at[0])


def step(tok, lens, gain, base, rate, ggain, weights, wo, state, tp, dp):
    rows, width = tok.shape
    slim = width // dp
    nx = dp // 2
    feat = tp * width
    bf = jnp.bfloat16
    vmem, hbm = pl.BlockSpec(memory_space=pltpu.VMEM), pl.BlockSpec(memory_space=pltpu.HBM)
    dma = pltpu.SemaphoreType.DMA
    half = rows // 2
    return pl.pallas_call(
        functools.partial(step_body, tp=tp, dp=dp),
        out_shape=(
            pltpu.VMEM((rows, width), bf),
            pltpu.VMEM(state.shape, state.dtype),
        ),
        in_specs=[hbm] * 14,
        out_specs=(vmem, vmem),
        scratch_shapes=[
            pltpu.VMEM((2, tp * nx * rows, width), bf),
            pltpu.VMEM((2, 12 * slim, feat), bf),
            pltpu.VMEM((2, width, feat), bf),
            pltpu.VMEM((2, nx, rows, 12 * slim), bf),
            pltpu.VMEM((2, tp * rows, width), bf),
            pltpu.VMEM((2, nx, rows, 12 * slim), bf),
            pltpu.VMEM((2, rows, 2 * slim, nx * 2 * slim), bf),
            pltpu.VMEM((2, 4, nx, rows, 2 * slim), jnp.float32),
            pltpu.VMEM((nx * rows, 12 * slim), jnp.float32),
            pltpu.VMEM((nx * rows, 128), jnp.float32),
            pltpu.VMEM(lens.shape, lens.dtype),
            pltpu.VMEM(gain.shape, gain.dtype),
            pltpu.VMEM(base.shape, base.dtype),
            pltpu.VMEM(rate.shape, rate.dtype),
            pltpu.VMEM(ggain.shape, ggain.dtype),
            dma((1,)),
            dma((nx,)),
            dma((tp,)),
            dma((tp,)),
            dma((1,)),
            dma((nx,)),
            dma((1,)),
            dma((tp,)),
            dma((2,)),
            dma((2, 7)),
            dma((1,)),
            dma((2,)),
            dma((4,)),
            dma((2,)),
            dma((6,)),
        ],
        compiler_params=pltpu.CompilerParams(
            collective_id=0, has_side_effects=True, vmem_limit_bytes=VMEM_LIMIT
        ),
        name="step",
    )(tok, lens, gain, base, rate, ggain, *weights, wo, state)


def put_body(mixed_ref, state_ref, out_ref, new_ref, sem):
    count = state_ref.shape[0] * 4
    part = state_ref.shape[1] // 4
    copies = [pltpu.make_async_copy(mixed_ref, out_ref, sem.at[count])]
    for i in range(count):
        span = pl.ds(i % 4 * part, part)
        copies.append(
            pltpu.make_async_copy(state_ref.at[i // 4, span], new_ref.at[i // 4, span], sem.at[i])
        )
    for copy in copies:
        copy.start()
    for copy in copies:
        copy.wait()


def put(mixed, state):
    vmem, hbm = pl.BlockSpec(memory_space=pltpu.VMEM), pl.BlockSpec(memory_space=pltpu.HBM)
    return pl.pallas_call(
        put_body,
        out_shape=(
            jax.ShapeDtypeStruct(mixed.shape, mixed.dtype),
            jax.ShapeDtypeStruct(state.shape, state.dtype),
        ),
        in_specs=[vmem, vmem],
        out_specs=(hbm, hbm),
        scratch_shapes=[pltpu.SemaphoreType.DMA((state.shape[0] * 4 + 1,))],
        compiler_params=pltpu.CompilerParams(vmem_limit_bytes=4 * 1024 * 1024),
        name="put",
    )(mixed, state)


def on_device(
    tokens,
    lengths,
    norm_gain,
    w_recept,
    w_key,
    w_value,
    w_decay,
    w_rate,
    w_gate,
    w_out,
    decay_base,
    rate_base,
    group_gain,
    state,
):
    tp, dp = lax.axis_size("tp"), lax.axis_size("dp")
    weights = [w.transpose(0, 2, 1) for w in (w_recept, w_key, w_value, w_decay, w_rate, w_gate)]
    mixed, states = step(
        tokens, lengths.reshape(1, -1), norm_gain, decay_base, rate_base, group_gain,
        weights, w_out.transpose(0, 2, 1), state, tp, dp,
    )
    return put(mixed, states)


def solution(mesh):
    columns = P(None, None, ("tp", "dp"))
    in_specs = (
        (P("dp", "tp"), P("dp"), P())
        + (columns,) * 7
        + (P(None, "tp"),) * 3
        + (P(None, "dp", "tp", None, None),)
    )
    out_specs = (P("dp", "tp"), P(None, "dp", "tp", None, None))
    return jax.shard_map(
        on_device, mesh=mesh, in_specs=in_specs, out_specs=out_specs, check_vma=False
    )
```
